128 devices in a mesh: ep: 32 (over z, y, core), tp: 4 (over x).
Axes of the slice: x: 4, y: 4, z: 4, core: 2. Of those that a mesh axis runs over, the one named last changes fastest.
Arguments:
- queries: bfloat16 [32768, 1024], P('ep', 'tp'), may hold values from -6 to 6
- key_rows: bfloat16 [32768, 256], P('ep', 'tp'), may hold values from -6 to 6
- values: bfloat16 [32768, 256], P('ep', 'tp'), may hold values from -6 to 6
- sink_logit: float32 [16], P('tp'), may hold values from 3 to 7
- out_weight: bfloat16 [1024, 2048], P('tp'), may hold values from -0.1875 to 0.1875
- out_gain: float32 [2048], replicated, may hold values from 0.1 to 1.9
- routed_tokens: bfloat16 [65536, 2048], P(('ep', 'tp')), may hold values from -6 to 6
- expert_ids: int32 [65536, 2], P(('ep', 'tp')), may hold values from 0 to 31, as said below
- route_weight: float32 [65536, 2], P(('ep', 'tp')), may hold values from 0.1 to 1
- routed_gain: float32 [2048], replicated, may hold values from 0.1 to 1.9
- expert_gate: bfloat16 [32, 2048, 1024], P('ep', None, 'tp'), may hold values from -0.125 to 0.125
- expert_up: bfloat16 [32, 2048, 1024], P('ep', None, 'tp'), may hold values from -0.125 to 0.125
- expert_down: bfloat16 [32, 2048, 1024], P('ep', None, 'tp'), may hold values from -0.1875 to 0.1875
Outputs:
- mixer_out: bfloat16 [32768, 2048], P(('ep', 'tp'))
- experts_out: bfloat16 [65536, 2048], P(('ep', 'tp'))
The draws below stay inside these ranges and needn't reach their ends.
Inputs may be any that keep to these rules, and one draw needn't show every extreme that they name: `expert_ids`: both experts of a row lie in one group (equal id // 8); the 512 rows of one device name every group exactly 512 / 4 times; the rows of one device name no expert more than 64 times; in every device's rows some expert of each group is named exactly 64 times, and one expert is named exactly 64 times by the rows of every device.
All inputs are finite; a program needn't handle non-finite values.
Results may differ from the reference program's by a relative error of at most 0.0071.
Values may be sent and summed in bfloat16 or wider, within the bound.
No kernel may reach another device: no remote copies, remote signals or barrier semaphores. Data moves between devices by JAX's collectives and lax.ppermute only.
A program may use at most 128 MiB of HBM per device.

```python
import math
import jax
import jax.numpy as jnp
from jax import lax

D = 2048
HEADS = 16
KV_HEADS = 4
HEAD_DIM = 64
WINDOW = 128
QBLOCK = 512
EXPERTS = 32
GROUPS = 4
EPG = 8
TOP = 2
EXPERT_FF = 1024
TB = 512
CAP = 64
SEQ_A = 32768
TOKENS_B = 65536
N_EP = 32
N_TP = 4


def draw_queries(key, part):
    drawn = jax.random.normal(jax.random.fold_in(key, 12), (SEQ_A, HEADS * HEAD_DIM), jnp.float32)
    return jnp.clip(drawn, -4.0, 4.0).astype(jnp.bfloat16)


def draw_key_rows(key, part):
    drawn = jax.random.normal(jax.random.fold_in(key, 22), (SEQ_A, KV_HEADS * HEAD_DIM), jnp.float32)
    return jnp.clip(drawn, -4.0, 4.0).astype(jnp.bfloat16)


def draw_expert_ids(key, part):
    block_total = TOKENS_B // TB
    half_group = TB // (2 * GROUPS)
    common_hot = jax.random.randint(jax.random.fold_in(key, 101), (), 0, EPG)

    def one_block(block_index):
        block_key = jax.random.fold_in(jax.random.fold_in(key, 202), block_index)
        order_key, hot_key, rest_key = jax.random.split(block_key, 3)
        order = jax.random.permutation(order_key, TB)
        hottest = jax.random.randint(hot_key, (GROUPS,), 0, EPG).at[0].set(common_hot)
        others = jax.vmap(lambda inner: jax.random.permutation(inner, EPG - 1))(jax.random.split(rest_key, GROUPS))
        group = order % GROUPS
        rank = order // GROUPS
        hot_token = hottest[group]
        rest_token = others[group]
        stride = 1 + rank // (EPG - 1) % (EPG - 2)
        first_other = jnp.take_along_axis(rest_token, (rank % (EPG - 1))[:, None], axis=1)[:, 0]
        second_other = jnp.take_along_axis(rest_token, ((rank + stride) % (EPG - 1))[:, None], axis=1)[:, 0]
        other_one = (hot_token + 1 + first_other) % EPG
        other_two = (hot_token + 1 + second_other) % EPG
        leading = jnp.where(rank < half_group, hot_token, other_one)
        trailing = jnp.where(rank < half_group, other_one, other_two)
        return jnp.stack([group * EPG + leading, group * EPG + trailing], axis=-1)
    chosen = jax.vmap(one_block)(jnp.arange(block_total))
    return chosen.reshape(TOKENS_B, TOP).astype(jnp.int32)


def block_scale(rng, dims, shards, least, high):
    gain = 1.0
    for dim, blocks in shards:
        steps = jax.random.uniform(jax.random.fold_in(jax.random.fold_in(rng, 6), dim), (blocks,), jnp.float32, least / len(shards), high / len(shards))
        gain = gain * jnp.repeat(jnp.exp(steps), dims[dim] // blocks).reshape((-1,) + (1,) * (len(dims) - 1 - dim))
    return gain


def gaussian(rng, shape, deviation, most, cuts=(), kind=jnp.bfloat16):
    level = block_scale(rng, shape, cuts, -0.22, 0.18) if cuts else 1.0
    values = jax.random.normal(rng, shape, jnp.float32) * deviation * level
    return jnp.minimum(jnp.maximum(values, -most), most).astype(kind)


def setup_inputs(seed: int = 0) -> dict:
    seeds = jax.random.split(jax.random.key(seed), 14)
    queries = draw_queries(jax.random.fold_in(seeds[13], 71), 0)
    key_rows = draw_key_rows(jax.random.fold_in(seeds[13], 71), 0)
    values = gaussian(seeds[2], (SEQ_A, KV_HEADS * HEAD_DIM), 1.0, 6.0, ((0, 32), (1, 4)))
    sink_logit = jnp.clip(3.0 + 4.0 * jax.random.uniform(seeds[3], (HEADS,), jnp.float32) ** block_scale(seeds[3], (HEADS,), ((0, 4),), -0.2, 0.2), 3.0, 7.0)
    out_weight = gaussian(seeds[4], (HEADS * HEAD_DIM, D), (HEADS * HEAD_DIM) ** -0.5, 0.1875, ((0, 4),))
    out_gain = jnp.clip(1.0 + 0.18 * jax.random.normal(seeds[5], (D,), jnp.float32), 0.1, 1.9)
    routed_tokens = gaussian(seeds[6], (TOKENS_B, D), 1.0, 6.0, ((0, 128),))
    expert_ids = draw_expert_ids(jax.random.fold_in(seeds[13], 71), 0)
    route_weight = jnp.clip(jnp.exp(math.log(1.0) - 2.3025851 * jax.random.uniform(seeds[8], (TOKENS_B, TOP), jnp.float32) ** block_scale(seeds[8], (TOKENS_B, TOP), ((0, 128),), -0.2, 0.2)), 0.1, 1.0)
    routed_gain = jnp.clip(1.0 + 0.18 * jax.random.normal(seeds[9], (D,), jnp.float32), 0.1, 1.9)
    expert_gate = gaussian(seeds[10], (EXPERTS, D, EXPERT_FF), D ** -0.5, 0.125, ((0, 32), (2, 4)))
    expert_up = gaussian(seeds[11], (EXPERTS, D, EXPERT_FF), D ** -0.5, 0.125, ((0, 32), (2, 4)))
    expert_down = gaussian(seeds[12], (EXPERTS, D, EXPERT_FF), EXPERT_FF ** -0.5, 0.1875, ((0, 32), (2, 4)))
    return dict(queries=queries, key_rows=key_rows, values=values, sink_logit=sink_logit, out_weight=out_weight, out_gain=out_gain, routed_tokens=routed_tokens, expert_ids=expert_ids, route_weight=route_weight, routed_gain=routed_gain, expert_gate=expert_gate, expert_up=expert_up, expert_down=expert_down)


epsilon = 1e-06
far_below = -1e+30

def window_block(block_index, grouped, padded_keys, padded_values, sink_logit, seq_total):
    start_row = block_index * QBLOCK
    span_keys = QBLOCK + 2 * WINDOW
    query_block = lax.dynamic_slice_in_dim(grouped, start_row, QBLOCK, 0).astype(jnp.float32)
    key_block = lax.dynamic_slice_in_dim(padded_keys, start_row, span_keys, 0).astype(jnp.float32)
    value_block = lax.dynamic_slice_in_dim(padded_values, start_row, span_keys, 0).astype(jnp.float32)
    scores = jnp.einsum('qhgd,khd->hgqk', query_block, key_block) * HEAD_DIM ** (-0.5)
    query_pos = start_row + jnp.arange(QBLOCK, dtype=jnp.int32)
    key_pos = start_row - WINDOW + jnp.arange(span_keys, dtype=jnp.int32)
    valid = (jnp.abs(key_pos[None, :] - query_pos[:, None]) <= WINDOW) & (key_pos[None, :] >= 0) & (key_pos[None, :] < seq_total)
    sinks = sink_logit.reshape(KV_HEADS, HEADS // KV_HEADS)[:, :, None, None]
    masked = jnp.where(valid, scores, far_below)
    largest = jnp.maximum(lax.optimization_barrier(jnp.max(masked, axis=-1, keepdims=True)), sinks)
    raised = jnp.where(valid, jnp.exp(masked - largest), 0.0)
    denominator = lax.optimization_barrier(jnp.sum(raised, axis=-1, keepdims=True)) + jnp.exp(sinks - largest)
    weights = (raised / denominator).astype(jnp.bfloat16)
    attended = jnp.einsum('hgqk,khd->qhgd', weights.astype(jnp.float32), value_block)
    return attended.astype(jnp.bfloat16).reshape(QBLOCK, HEADS * HEAD_DIM)

def reference(queries, key_rows, values, sink_logit, out_weight, out_gain, routed_tokens, expert_ids, route_weight, routed_gain, expert_gate, expert_up, expert_down):
    seq_total = queries.shape[0]
    grouped = queries.reshape(seq_total, KV_HEADS, HEADS // KV_HEADS, HEAD_DIM)
    padding = ((WINDOW, WINDOW), (0, 0), (0, 0))
    padded_keys = jnp.pad(key_rows.reshape(seq_total, KV_HEADS, HEAD_DIM), padding)
    padded_values = jnp.pad(values.reshape(seq_total, KV_HEADS, HEAD_DIM), padding)
    block_ids = jnp.arange(seq_total // QBLOCK, dtype=jnp.int32)
    attended = lax.map(lambda block_index: window_block(block_index, grouped, padded_keys, padded_values, sink_logit, seq_total), block_ids)
    attended = attended.reshape(seq_total, HEADS * HEAD_DIM)
    mixed = jnp.dot(attended, out_weight, preferred_element_type=jnp.float32)
    mixer_out = (mixed * lax.rsqrt(lax.optimization_barrier(jnp.mean(mixed * mixed, axis=-1, keepdims=True)) + epsilon) * out_gain).astype(jnp.bfloat16)
    token_total = routed_tokens.shape[0]
    inputs = routed_tokens.astype(jnp.float32)
    normed = (inputs * lax.rsqrt(lax.optimization_barrier(jnp.mean(inputs * inputs, axis=-1, keepdims=True)) + epsilon) * routed_gain).astype(jnp.bfloat16)
    flat_ids = expert_ids.reshape(-1)
    most_rows = CAP * N_EP * N_TP
    empty = jnp.zeros((token_total * TOP, normed.shape[1]), jnp.bfloat16)

    def one_expert(results, expert):
        picked = jnp.nonzero(flat_ids == expert, size=most_rows, fill_value=token_total * TOP)[0]
        rows_in = jnp.take(normed, picked // TOP, axis=0, mode='fill', fill_value=0)
        gate = jnp.dot(rows_in, expert_gate[expert], preferred_element_type=jnp.float32)
        upward = jnp.dot(rows_in, expert_up[expert], preferred_element_type=jnp.float32)
        hidden = (jax.nn.silu(gate) * upward).astype(jnp.bfloat16)
        produced = jnp.dot(hidden, expert_down[expert].T, preferred_element_type=jnp.float32).astype(jnp.bfloat16)
        return (results.at[picked].set(produced, mode='drop'), None)
    results, unused = lax.scan(one_expert, empty, jnp.arange(EXPERTS, dtype=jnp.int32))
    results = results.reshape(token_total, TOP, normed.shape[1]).astype(jnp.float32)
    experts_out = lax.optimization_barrier(jnp.sum(results * route_weight[:, :, None], axis=1)).astype(jnp.bfloat16)
    return (mixer_out, experts_out)
```

```python
import functools

import jax
import jax.numpy as jnp
from jax import lax
from jax.experimental import pallas as pl
from jax.experimental.pallas import tpu as pltpu
from jax.sharding import Mesh, PartitionSpec as P

HEAD_DIM = 64
WINDOW = 128
QBLOCK = 512
CAP = 64
GROUPS = 4
META = 128
STEP_BLOCKS = 8

epsilon = 1e-06
f32 = jnp.float32
bf16 = jnp.bfloat16
NT = (((1,), (1,)), ((), ()))
TN = (((0,), (0,)), ((), ()))
VMEM_LIMIT = 60 * 1024 * 1024


def shifted(size, shift):
    return [(i, (i + shift) % size) for i in range(size)]


def iota(shape, dim, kind=jnp.int32):
    return lax.broadcasted_iota(jnp.int32, shape, dim).astype(kind)


def prep_kernel(place, tok, ids_t, weight_t, gain, first, second, third, fourth, order):
    count = tok.shape[0]
    each = count // GROUPS
    inputs = tok[...].astype(f32)
    scale = lax.rsqrt(jnp.mean(inputs * inputs, axis=-1, keepdims=True) + epsilon)
    normed = (inputs * scale * gain[...]).astype(bf16)
    ids = ids_t[...]
    group = lax.shift_right_logical(ids[0:1, :], 3)
    relative = lax.bitwise_and(group - place[0] + GROUPS, GROUPS - 1)
    member = (iota((16, count), 0) == relative).astype(f32)
    before = (iota((count, count), 0) < iota((count, count), 1)).astype(f32).astype(bf16)
    earlier = jnp.dot(member.astype(bf16), before, preferred_element_type=f32)
    rank = jnp.sum(earlier * member, axis=0, keepdims=True)
    slot = (relative * each).astype(f32) + rank
    permute = (iota((count, count), 0, f32) == slot).astype(f32).astype(bf16)
    order[...] = permute
    rows = jnp.dot(permute, normed, preferred_element_type=f32).astype(bf16)
    line = iota((META, count), 0)
    meta = jnp.where(line == 0, ids[0:1, :].astype(f32), 0.0)
    meta = jnp.where(line == 1, ids[1:2, :].astype(f32), meta)
    for k in range(2):
        rest = weight_t[k : k + 1, :]
        for part in range(3):
            piece = rest.astype(bf16).astype(f32)
            meta = jnp.where(line == 2 + 3 * k + part, piece, meta)
            rest = rest - piece
    tags = lax.dot_general(permute, meta.astype(bf16), NT, preferred_element_type=f32).astype(bf16)
    width = tok.shape[1]
    for index, out in enumerate((first, second, third, fourth)):
        out[:, :width] = rows[index * each : (index + 1) * each]
        out[:, width:] = tags[index * each : (index + 1) * each]


def prepare(place, tokens, ids, weights, gain):
    count, width = tokens.shape
    chunk = jax.ShapeDtypeStruct((count // GROUPS, width + META), bf16)
    vmem = pl.BlockSpec(memory_space=pltpu.VMEM)
    return pl.pallas_call(
        prep_kernel,
        out_shape=(chunk, chunk, chunk, chunk, jax.ShapeDtypeStruct((count, count), bf16)),
        in_specs=[pl.BlockSpec(memory_space=pltpu.SMEM)] + [vmem] * 4,
        out_specs=(vmem,) * 5,
        compiler_params=pltpu.CompilerParams(vmem_limit_bytes=VMEM_LIMIT),
        cost_estimate=pl.CostEstimate(flops=6_000_000_000, bytes_accessed=6_000_000, transcendentals=512),
        name="prep",
    )(place, tokens, ids.T, weights.T, gain.reshape(1, width))


def choices(tags, expert):
    blocks = tags.shape[0]
    size = tags.shape[1]
    lines = [jnp.transpose(tags[b].astype(f32)) for b in range(blocks)]
    hits = [tuple((t[k : k + 1] == expert).astype(f32) for k in range(2)) for t in lines]
    row = iota((16, size), 0)
    counts = jnp.zeros((16, size), f32)
    for b in range(blocks):
        counts = jnp.where(row == b, hits[b][0] + hits[b][1], counts)
    before = (iota((size, size), 0) < iota((size, size), 1)).astype(f32).astype(bf16)
    earlier = jnp.dot(counts.astype(bf16), before, preferred_element_type=f32)
    place = iota((2 * CAP, size), 0, f32)
    found = []
    for pair in range(blocks // 2):
        halves = []
        weight = jnp.zeros((2 * CAP, size), f32)
        for j in range(2):
            b = 2 * pair + j
            slot = earlier[b : b + 1] + float(CAP * j)
            one = jnp.where(place == slot, hits[b][0], 0.0)
            two = jnp.where(place == slot + hits[b][0], hits[b][1], 0.0)
            halves.append(one + two)
            t = lines[b]
            weight = weight + one * (t[2:3] + t[3:4] + t[4:5]) + two * (t[5:6] + t[6:7] + t[7:8])
        pick = jnp.concatenate(halves, axis=1).astype(bf16)
        found.append((pick, jnp.sum(weight, axis=1, keepdims=True)))
    return found


def hidden_kernel(place, tok, *refs):
    gates, ups, out, rows = refs[:4], refs[4:8], refs[8], refs[9]
    width = gates[0].shape[0]
    expert = place[1].astype(f32)
    size = tok.shape[1]
    for pair, (pick, _) in enumerate(choices(tok[:, :, width:], expert)):
        both = tok[2 * pair : 2 * pair + 2, :, :width].reshape(2 * size, width)
        rows[2 * CAP * pair : 2 * CAP * (pair + 1)] = jnp.dot(pick, both, preferred_element_type=f32).astype(bf16)
    inputs = rows[...]
    wide = gates[0].shape[1]
    for s in range(4):
        gate = jnp.dot(inputs, gates[s][...], preferred_element_type=f32)
        up = jnp.dot(inputs, ups[s][...], preferred_element_type=f32)
        out[:, s * wide : (s + 1) * wide] = (gate / (1.0 + jnp.exp(-gate)) * up).astype(bf16)


def hidden_units(place, tokens, gates, ups):
    blocks, size, full = tokens.shape
    width, wide = gates[0].shape
    steps = blocks // STEP_BLOCKS
    rows = STEP_BLOCKS * CAP
    weight = pl.BlockSpec((width, wide), lambda i: (0, 0))
    return pl.pallas_call(
        hidden_kernel,
        grid=(steps,),
        out_shape=jax.ShapeDtypeStruct((blocks * CAP, 4 * wide), bf16),
        in_specs=[
            pl.BlockSpec(memory_space=pltpu.SMEM),
            pl.BlockSpec((STEP_BLOCKS, size, full), lambda i: (i, 0, 0)),
        ]
        + [weight] * 8,
        out_specs=pl.BlockSpec((rows, 4 * wide), lambda i: (i, 0)),
        scratch_shapes=[pltpu.VMEM((rows, width), bf16)],
        compiler_params=pltpu.CompilerParams(vmem_limit_bytes=VMEM_LIMIT),
        cost_estimate=pl.CostEstimate(
            flops=blocks * CAP * width * wide * 16, bytes_accessed=blocks * size * full * 2 + 8_000_000, transcendentals=0
        ),
        name="hidden",
    )(place, tokens, *gates, *ups)


def result_kernel(place, tags, hidden, *refs):
    downs, out = refs[:5], refs[5]
    wide = downs[0].shape[1]
    size = tags.shape[1]
    expert = place[1].astype(f32)
    half = downs[3].shape[0]
    found = choices(tags[...], expert)
    units = [hidden[:, s * wide : (s + 1) * wide] for s in range(4)]
    for part in range(2):
        cols = slice(part * half, (part + 1) * half)
        total = lax.dot_general(units[3], downs[3 + part][...], NT, preferred_element_type=f32)
        for s in range(3):
            total = total + lax.dot_general(units[s], downs[s][cols, :], NT, preferred_element_type=f32)
        result = total.astype(bf16).astype(f32)
        for pair, (pick, weight) in enumerate(found):
            scaled = (result[2 * CAP * pair : 2 * CAP * (pair + 1)] * weight).astype(bf16)
            spread = lax.dot_general(pick, scaled, TN, preferred_element_type=f32)
            out[2 * size * pair : 2 * size * (pair + 1), cols] = spread.astype(bf16)


def results(place, tokens, hidden, downs):
    blocks, size, full = tokens.shape
    wide = downs[0].shape[1]
    width = downs[0].shape[0]
    steps = blocks // STEP_BLOCKS
    rows = STEP_BLOCKS * CAP
    return pl.pallas_call(
        result_kernel,
        grid=(steps,),
        out_shape=jax.ShapeDtypeStruct((blocks * size, width), bf16),
        in_specs=[
            pl.BlockSpec(memory_space=pltpu.SMEM),
            pl.BlockSpec((STEP_BLOCKS, size, META), lambda i: (i, 0, width // META)),
            pl.BlockSpec((rows, 4 * wide), lambda i: (i, 0)),
        ]
        + [pl.BlockSpec(d.shape, lambda i: (0, 0)) for d in downs],
        out_specs=pl.BlockSpec((STEP_BLOCKS * size, width), lambda i: (i, 0)),
        compiler_params=pltpu.CompilerParams(vmem_limit_bytes=VMEM_LIMIT),
        cost_estimate=pl.CostEstimate(
            flops=blocks * CAP * width * wide * 12, bytes_accessed=blocks * size * width * 2 + 8_000_000, transcendentals=0
        ),
        name="result",
    )(place, tokens, hidden, *downs)


def finish_kernel(order, first, second, third, fourth, out):
    each = first.shape[0]
    total = jnp.zeros(out.shape, f32)
    for index, piece in enumerate((first, second, third, fourth)):
        total = total + lax.dot_general(
            order[index * each : (index + 1) * each, :], piece[...], TN, preferred_element_type=f32
        )
    out[...] = total.astype(bf16)


def finish(order, pieces):
    count = order.shape[0]
    width = pieces[0].shape[1]
    vmem = pl.BlockSpec(memory_space=pltpu.VMEM)
    return pl.pallas_call(
        finish_kernel,
        out_shape=jax.ShapeDtypeStruct((count, width), bf16),
        in_specs=[vmem] * 5,
        out_specs=vmem,
        compiler_params=pltpu.CompilerParams(vmem_limit_bytes=VMEM_LIMIT),
        cost_estimate=pl.CostEstimate(flops=2_000_000_000, bytes_accessed=5_000_000, transcendentals=0),
        name="finish",
    )(order, *pieces)


def ring_weights(gate, up, down):
    right = lambda v: lax.ppermute(v, "x", shifted(4, 1))
    left = lambda v: lax.ppermute(v, "x", shifted(4, -1))
    half = down.shape[0] // 2
    gate_low, up_low = right(gate), right(up)
    gate_high, up_high = left(gate), left(up)
    down_low, down_high = right(down), left(down)
    gate_far = right(gate_low)
    up_far = left(up_high)
    down_far = right(down_low[:half]), left(down_high[half:])
    return (
        (gate, gate_low, gate_high, gate_far),
        (up, up_low, up_high, up_far),
        (down, down_low, down_high) + down_far,
    )


def padded(block, width):
    axes = ("z", "y", "c")
    count = 1
    for axis in axes:
        count *= lax.axis_size(axis)
    forward = [(i, i + 1) for i in range(count - 1)]
    backward = [(target, source) for source, target in forward]
    low = lax.ppermute(block[-width:], axes, forward)
    high = lax.ppermute(block[:width], axes, backward)
    return jnp.concatenate([low, block, high], axis=0)


def attention(queries, key_rows, values, sink_logit, offset, seq_total):
    row_count = queries.shape[0]
    heads_here = queries.shape[1] // HEAD_DIM
    kv_here = key_rows.shape[1] // HEAD_DIM
    group_size = heads_here // kv_here
    extended = padded(jnp.concatenate((key_rows, values), axis=1), WINDOW)
    grouped = queries.reshape(row_count, kv_here, group_size, HEAD_DIM)
    sinks = sink_logit.reshape(kv_here, group_size)[:, :, None, None]
    span_keys = QBLOCK + 2 * WINDOW

    def attend_block(block_index):
        start_row = block_index * QBLOCK
        query_block = lax.dynamic_slice_in_dim(grouped, start_row, QBLOCK, 0)
        band = lax.dynamic_slice_in_dim(extended, start_row, span_keys, 0)
        key_block = band[:, : kv_here * HEAD_DIM].reshape(span_keys, kv_here, HEAD_DIM)
        value_block = band[:, kv_here * HEAD_DIM :].reshape(span_keys, kv_here, HEAD_DIM)
        scores = jnp.einsum("qhgd,khd->hgqk", query_block, key_block, preferred_element_type=f32) * HEAD_DIM ** (-0.5)
        query_pos = offset + start_row + jnp.arange(QBLOCK, dtype=jnp.int32)
        key_pos = offset + start_row - WINDOW + jnp.arange(span_keys, dtype=jnp.int32)
        valid = (
            (jnp.abs(key_pos[None, :] - query_pos[:, None]) <= WINDOW)
            & (key_pos[None, :] >= 0)
            & (key_pos[None, :] < seq_total)
        )
        masked = jnp.where(valid, scores, -1e30)
        largest = jnp.maximum(jnp.max(masked, axis=-1, keepdims=True), sinks)
        raised = jnp.where(valid, jnp.exp(masked - largest), 0.0)
        denominator = jnp.sum(raised, axis=-1, keepdims=True) + jnp.exp(sinks - largest)
        weights = (raised / denominator).astype(bf16)
        attended = jnp.einsum("hgqk,khd->qhgd", weights, value_block, preferred_element_type=f32)
        return attended.astype(bf16).reshape(QBLOCK, heads_here * HEAD_DIM)

    attended = lax.map(attend_block, jnp.arange(row_count // QBLOCK, dtype=jnp.int32))
    return attended.reshape(row_count, heads_here * HEAD_DIM)


def local(
    queries,
    key_rows,
    values,
    sink_logit,
    out_weight,
    out_gain,
    routed_tokens,
    expert_ids,
    route_weight,
    routed_gain,
    expert_gate,
    expert_up,
    expert_down,
):
    row_count = queries.shape[0]
    z, y, c = lax.axis_index("z"), lax.axis_index("y"), lax.axis_index("c")
    expert = (z * 4 + y) * 2 + c
    place = jnp.stack([z, expert]).astype(jnp.int32)
    plane = ("y", "c")
    gates, ups, downs = ring_weights(expert_gate[0], expert_up[0], expert_down[0])

    chunks = prepare(place, routed_tokens, expert_ids, route_weight, routed_gain)
    own, order = chunks[0], chunks[4]
    moved = [lax.ppermute(chunks[s], "z", shifted(4, s)) for s in (1, 3, 2)]
    near = lax.all_gather(own, plane, axis=0, tiled=False)
    far = lax.all_gather(jnp.concatenate(moved, axis=0), plane, axis=0, tiled=False)
    size, full = own.shape
    near = near.reshape(8, size, full)
    far = far.reshape(24, size, full)

    attended = attention(queries, key_rows, values, sink_logit, expert * row_count, row_count * 32)
    quarter = row_count // 4
    heads = attended.shape[1]
    crossed = lax.all_to_all(attended.reshape(4, quarter, heads), "x", 0, 0)
    low = lax.ppermute(out_weight, "x", shifted(4, 1))
    high = lax.ppermute(out_weight, "x", shifted(4, -1))
    half = heads // 2
    across = lax.ppermute(low[:half], "x", shifted(4, 1)), lax.ppermute(high[half:], "x", shifted(4, -1))
    across = jnp.concatenate(across, axis=0)
    x = lax.axis_index("x")
    mixed = jnp.zeros((quarter, out_weight.shape[1]), f32)
    for shift, piece in ((0, out_weight), (3, low), (1, high), (2, across)):
        part = lax.dynamic_index_in_dim(crossed, (x + shift) % 4, 0, keepdims=False)
        mixed = mixed + jnp.dot(part, piece, preferred_element_type=f32)
    mixer_out = (
        mixed * lax.rsqrt(jnp.mean(mixed * mixed, axis=-1, keepdims=True) + epsilon) * out_gain
    ).astype(bf16)

    near_hidden = hidden_units(place, near, gates, ups)
    far_hidden = hidden_units(place, far, gates, ups)
    far_part = results(place, far, far_hidden, downs)
    near_part = results(place, near, near_hidden, downs)
    far_sum = lax.psum_scatter(far_part, plane, scatter_dimension=0, tiled=True)
    near_sum = lax.psum_scatter(near_part, plane, scatter_dimension=0, tiled=True)
    back = {0: near_sum}
    for index, s in enumerate((1, 3, 2)):
        back[s] = lax.ppermute(far_sum[index * size : (index + 1) * size], "z", shifted(4, -s))
    experts_out = finish(order, [back[s] for s in range(4)])
    return (mixer_out, experts_out)


def solution(mesh):
    split = Mesh(mesh.devices.reshape(4, 4, 2, 4), ("z", "y", "c", "x"))
    ep = ("z", "y", "c")
    placed = (
        P(ep, "x"),
        P(ep, "x"),
        P(ep, "x"),
        P("x"),
        P("x", None),
        P(),
        P(ep + ("x",), None),
        P(ep + ("x",), None),
        P(ep + ("x",), None),
        P(),
        P(ep, None, "x"),
        P(ep, None, "x"),
        P(ep, None, "x"),
    )
    return jax.shard_map(
        local,
        mesh=split,
        in_specs=placed,
        out_specs=(P(ep + ("x",), None), P(ep + ("x",), None)),
        check_vma=False,
    )
```

```python
import jax
import jax.numpy as jnp
from jax import lax
from jax.experimental import pallas as pl
from jax.experimental.pallas import tpu as pltpu
from jax.sharding import Mesh, PartitionSpec as P


HEAD_DIM = 64
WINDOW = 128
QBLOCK = 512
CAP = 64
GROUPS = 4
META = 128
SET_BLOCKS = 8

epsilon = 1e-06
f32 = jnp.float32
bf16 = jnp.bfloat16
NT = (((1,), (1,)), ((), ()))
TN = (((0,), (0,)), ((), ()))
VMEM_LIMIT = 60 * 1024 * 1024


def shifted(size, shift):
    return [(i, (i + shift) % size) for i in range(size)]


def iota(shape, dim, kind=jnp.int32):
    return lax.broadcasted_iota(jnp.int32, shape, dim).astype(kind)


def prep_kernel(place, tok, ids_t, weight_t, gain, first, second, third, fourth, order):
    count = tok.shape[0]
    each = count // GROUPS
    inputs = tok[...].astype(f32)
    scale = lax.rsqrt(jnp.mean(inputs * inputs, axis=-1, keepdims=True) + epsilon)
    normed = (inputs * scale * gain[...]).astype(bf16)
    ids = ids_t[...]
    group = lax.shift_right_logical(ids[0:1, :], 3)
    relative = lax.bitwise_and(group - place[0] + GROUPS, GROUPS - 1)
    member = (iota((16, count), 0) == relative).astype(f32)
    before = (iota((count, count), 0) < iota((count, count), 1)).astype(f32).astype(bf16)
    earlier = jnp.dot(member.astype(bf16), before, preferred_element_type=f32)
    rank = jnp.sum(earlier * member, axis=0, keepdims=True)
    slot = (relative * each).astype(f32) + rank
    permute = (iota((count, count), 0, f32) == slot).astype(f32).astype(bf16)
    order[...] = permute
    rows = jnp.dot(permute, normed, preferred_element_type=f32).astype(bf16)
    line = iota((META, count), 0)
    meta = jnp.where(line == 0, ids[0:1, :].astype(f32), 0.0)
    meta = jnp.where(line == 1, ids[1:2, :].astype(f32), meta)
    for k in range(2):
        rest = weight_t[k : k + 1, :]
        for part in range(3):
            piece = rest.astype(bf16).astype(f32)
            meta = jnp.where(line == 2 + 3 * k + part, piece, meta)
            rest = rest - piece
    tags = lax.dot_general(permute, meta.astype(bf16), NT, preferred_element_type=f32).astype(bf16)
    width = tok.shape[1]
    for index, out in enumerate((first, second, third, fourth)):
        out[:, :width] = rows[index * each : (index + 1) * each]
        out[:, width:] = tags[index * each : (index + 1) * each]


def prepare(place, tokens, ids, weights, gain):
    count, width = tokens.shape
    chunk = jax.ShapeDtypeStruct((count // GROUPS, width + META), bf16)
    vmem = pl.BlockSpec(memory_space=pltpu.VMEM)
    return pl.pallas_call(
        prep_kernel,
        out_shape=(chunk, chunk, chunk, chunk, jax.ShapeDtypeStruct((count, count), bf16)),
        in_specs=[pl.BlockSpec(memory_space=pltpu.SMEM)] + [vmem] * 4,
        out_specs=(vmem,) * 5,
        compiler_params=pltpu.CompilerParams(vmem_limit_bytes=VMEM_LIMIT),
        cost_estimate=pl.CostEstimate(flops=6_000_000_000, bytes_accessed=6_000_000, transcendentals=512),
        name="prep",
    )(place, tokens, ids.T, weights.T, gain.reshape(1, width))


def choices(tags, experts):
    blocks = len(tags)
    size = tags[0].shape[0]
    lines = [jnp.transpose(t.astype(f32)) for t in tags]
    hits = [[tuple((t[k : k + 1] == e).astype(f32) for k in range(2)) for t in lines] for e in experts]
    row = iota((2 * blocks, size), 0)
    counts = jnp.zeros((2 * blocks, size), f32)
    for e in range(2):
        for b in range(blocks):
            counts = jnp.where(row == e * blocks + b, hits[e][b][0] + hits[e][b][1], counts)
    before = (iota((size, size), 0) < iota((size, size), 1)).astype(f32).astype(bf16)
    earlier = jnp.dot(counts.astype(bf16), before, preferred_element_type=f32)
    place = iota((2 * CAP, size), 0, f32)
    found = []
    for pair in range(blocks // 2):
        picks = []
        weights = []
        for e in range(2):
            halves = []
            weight = jnp.zeros((2 * CAP, size), f32)
            for j in range(2):
                b = 2 * pair + j
                hit = hits[e][b]
                slot = earlier[e * blocks + b : e * blocks + b + 1] + float(CAP * j)
                one = jnp.where(place == slot, hit[0], 0.0)
                two = jnp.where(place == slot + hit[0], hit[1], 0.0)
                halves.append(one + two)
                t = lines[b]
                weight = weight + one * (t[2:3] + t[3:4] + t[4:5]) + two * (t[5:6] + t[6:7] + t[7:8])
            picks.append(jnp.concatenate(halves, axis=1))
            weights.append(jnp.sum(weight, axis=1, keepdims=True))
        found.append((jnp.concatenate(picks, axis=0).astype(bf16), jnp.concatenate(weights, axis=0)))
    return found


def stage_kernel(place, *refs):
    tokens, weights = refs[:SET_BLOCKS], refs[SET_BLOCKS : SET_BLOCKS + 12]
    rows_out, hidden_out, pick_out, scale_out = refs[SET_BLOCKS + 12 : SET_BLOCKS + 16]
    tok, held, rows, units, pick_v, scale_v, tok_sem, held_sem, out_sem = refs[SET_BLOCKS + 16 :]
    width = rows.shape[-1]
    part = weights[0].shape[0]
    wide = weights[0].shape[1]
    size = tokens[0].shape[0]
    arrivals = [pltpu.make_async_copy(tokens[b], tok.at[b], tok_sem.at[b]) for b in range(SET_BLOCKS)]
    fetches = []
    for i in range(6):
        first, second = weights[2 * i], weights[2 * i + 1]
        fetches.append(pltpu.make_async_copy(first, held.at[i, pl.ds(0, part)], held_sem.at[2 * i]))
        fetches.append(
            pltpu.make_async_copy(
                second.at[pl.ds(0, 2 * width - part)], held.at[i, pl.ds(part, 2 * width - part)], held_sem.at[2 * i + 1]
            )
        )
    for copy in arrivals + fetches:
        copy.start()
    experts = (place[1].astype(f32), place[2].astype(f32))
    for copy in arrivals:
        copy.wait()
    for pair, (pick, scale) in enumerate(choices([tok[b, :, width:] for b in range(SET_BLOCKS)], experts)):
        pick_v[pair] = pick
        scale_v[pair] = jnp.broadcast_to(scale, scale_v.shape[1:])
        both = tok[2 * pair : 2 * pair + 2, :, :width].reshape(2 * size, width)
        chosen = jnp.dot(pick, both, preferred_element_type=f32).astype(bf16)
        for e in range(2):
            rows[e, 2 * CAP * pair : 2 * CAP * (pair + 1)] = chosen[2 * CAP * e : 2 * CAP * (e + 1)]
    sent = [
        pltpu.make_async_copy(rows, rows_out, out_sem.at[0]),
        pltpu.make_async_copy(pick_v, pick_out, out_sem.at[1]),
        pltpu.make_async_copy(scale_v, scale_out, out_sem.at[2]),
    ]
    for copy in sent:
        copy.start()
    for copy in fetches:
        copy.wait()

    def one_expert(e, _):
        for shard in range(3):
            gate = jnp.dot(rows[e], held[e * 3 + shard, :width], preferred_element_type=f32)
            up = jnp.dot(rows[e], held[e * 3 + shard, width:], preferred_element_type=f32)
            units[e, :, shard * wide : (shard + 1) * wide] = (gate / (1.0 + jnp.exp(-gate)) * up).astype(bf16)
        return 0

    lax.fori_loop(0, 2, one_expert, 0)
    last = pltpu.make_async_copy(units, hidden_out, out_sem.at[3])
    last.start()
    for copy in sent + [last]:
        copy.wait()


def stage(place, tokens, weights):
    size, full = tokens[0].shape
    width = full - META
    _, wide = weights[0].shape
    rows = SET_BLOCKS * CAP
    shapes = (
        ((2, rows, width), bf16),
        ((2, rows, 3 * wide), bf16),
        ((SET_BLOCKS // 2, 4 * CAP, 2 * size), bf16),
        ((SET_BLOCKS // 2, 4 * CAP, 128), f32),
    )
    anywhere = pl.BlockSpec(memory_space=pl.ANY)
    return pl.pallas_call(
        stage_kernel,
        out_shape=tuple(jax.ShapeDtypeStruct(*s) for s in shapes),
        in_specs=[pl.BlockSpec(memory_space=pltpu.SMEM)] + [anywhere] * (SET_BLOCKS + 12),
        out_specs=(anywhere,) * 4,
        scratch_shapes=[
            pltpu.VMEM((SET_BLOCKS, size, full), bf16),
            pltpu.VMEM((6, 2 * width, wide), bf16),
        ]
        + [pltpu.VMEM(*s) for s in shapes]
        + [
            pltpu.SemaphoreType.DMA((SET_BLOCKS,)),
            pltpu.SemaphoreType.DMA((12,)),
            pltpu.SemaphoreType.DMA((4,)),
        ],
        compiler_params=pltpu.CompilerParams(vmem_limit_bytes=VMEM_LIMIT),
        cost_estimate=pl.CostEstimate(flops=10_000_000_000, bytes_accessed=24_000_000, transcendentals=0),
    )(place, *tokens, *weights)


def result_kernel(rows_in, hidden_in, pick_in, scale_in, *refs):
    far, downs = refs[:4], refs[4:10]
    outs = refs[10:18]
    rows, units, pick_v, scale_v, held, down_v, sem = refs[18:]
    width = rows.shape[-1]
    part, wide = far[0].shape
    rest = 2 * width - part
    first = []
    for e in range(2):
        first += [
            pltpu.make_async_copy(rows_in.at[e], rows.at[e], sem.at[3 * e]),
            pltpu.make_async_copy(far[2 * e], held.at[e, pl.ds(0, part)], sem.at[3 * e + 1]),
            pltpu.make_async_copy(far[2 * e + 1].at[pl.ds(0, rest)], held.at[e, pl.ds(part, rest)], sem.at[3 * e + 2]),
        ]
    second = [
        pltpu.make_async_copy(hidden_in.at[e], units.at[e, :, pl.ds(0, 3 * wide)], sem.at[6 + e]) for e in range(2)
    ]
    for e in range(2):
        for shard in range(4):
            source = far[2 * e + 1] if shard == 3 else downs[3 * e + shard]
            second.append(
                pltpu.make_async_copy(
                    source.at[pl.ds(rest, width)], down_v.at[e, :, pl.ds(shard * wide, wide)], sem.at[8 + 4 * e + shard]
                )
            )
    second.append(pltpu.make_async_copy(pick_in, pick_v, sem.at[16]))
    second.append(pltpu.make_async_copy(scale_in, scale_v, sem.at[17]))
    for copy in first + second:
        copy.start()
    for e in range(2):
        for copy in first[3 * e : 3 * e + 3]:
            copy.wait()
        gate = jnp.dot(rows[e], held[e, :width], preferred_element_type=f32)
        up = jnp.dot(rows[e], held[e, width:], preferred_element_type=f32)
        units[e, :, 3 * wide :] = (gate / (1.0 + jnp.exp(-gate)) * up).astype(bf16)
    for copy in second:
        copy.wait()
    size = outs[0].shape[0]
    half = width // 2

    def one_half(h, _):
        cols = pl.ds(pl.multiple_of(h * half, half), half)
        made = [
            lax.dot_general(units[e], down_v[e, cols, :], NT, preferred_element_type=f32).astype(bf16).astype(f32)
            for e in range(2)
        ]
        for pair in range(SET_BLOCKS // 2):
            lines = slice(2 * CAP * pair, 2 * CAP * (pair + 1))
            result = jnp.concatenate([made[0][lines], made[1][lines]], axis=0)
            scaled = (result * scale_v[pair, :, 0:1]).astype(bf16)
            spread = lax.dot_general(pick_v[pair], scaled, TN, preferred_element_type=f32).astype(bf16)
            outs[2 * pair][:, cols] = spread[:size]
            outs[2 * pair + 1][:, cols] = spread[size:]
        return 0

    lax.fori_loop(0, 2, one_half, 0)


def results(staged, far, downs, size):
    rows, hidden, picks, scales = staged
    width = rows.shape[-1]
    _, wide = far[0].shape
    anywhere = pl.BlockSpec(memory_space=pl.ANY)
    vmem = pl.BlockSpec(memory_space=pltpu.VMEM)
    return pl.pallas_call(
        result_kernel,
        out_shape=(jax.ShapeDtypeStruct((size, width), bf16),) * SET_BLOCKS,
        in_specs=[anywhere] * 14,
        out_specs=(vmem,) * SET_BLOCKS,
        scratch_shapes=[
            pltpu.VMEM(rows.shape, bf16),
            pltpu.VMEM((2, rows.shape[1], 4 * wide), bf16),
            pltpu.VMEM(picks.shape, bf16),
            pltpu.VMEM(scales.shape, f32),
            pltpu.VMEM((2, 2 * width, wide), bf16),
            pltpu.VMEM((2, width, 4 * wide), bf16),
            pltpu.SemaphoreType.DMA((18,)),
        ],
        compiler_params=pltpu.CompilerParams(vmem_limit_bytes=VMEM_LIMIT),
        cost_estimate=pl.CostEstimate(flops=8_000_000_000, bytes_accessed=24_000_000, transcendentals=0),
    )(rows, hidden, picks, scales, *far, *downs)


def finish_kernel(order, first, second, third, fourth, out):
    each = first.shape[0]
    total = jnp.zeros(out.shape, f32)
    for index, piece in enumerate((first, second, third, fourth)):
        total = total + lax.dot_general(
            order[index * each : (index + 1) * each, :], piece[...], TN, preferred_element_type=f32
        )
    out[...] = total.astype(bf16)


def finish(order, pieces):
    count = order.shape[0]
    width = pieces[0].shape[1]
    vmem = pl.BlockSpec(memory_space=pltpu.VMEM)
    return pl.pallas_call(
        finish_kernel,
        out_shape=jax.ShapeDtypeStruct((count, width), bf16),
        in_specs=[vmem] * 5,
        out_specs=vmem,
        compiler_params=pltpu.CompilerParams(vmem_limit_bytes=VMEM_LIMIT),
        cost_estimate=pl.CostEstimate(flops=2_000_000_000, bytes_accessed=5_000_000, transcendentals=0),
        name="finish",
    )(order, *pieces)


def padded(block, width):
    axes = ("z", "y", "c")
    count = 1
    for axis in axes:
        count *= lax.axis_size(axis)
    forward = [(i, i + 1) for i in range(count - 1)]
    backward = [(target, source) for source, target in forward]
    low = lax.ppermute(block[-width:], axes, forward)
    high = lax.ppermute(block[:width], axes, backward)
    return jnp.concatenate([low, block, high], axis=0)


def attention(queries, extended, sink_logit, offset, seq_total):
    row_count = queries.shape[0]
    heads_here = queries.shape[1] // HEAD_DIM
    kv_here = extended.shape[1] // (2 * HEAD_DIM)
    group_size = heads_here // kv_here
    grouped = queries.reshape(row_count, kv_here, group_size, HEAD_DIM)
    sinks = sink_logit.reshape(kv_here, group_size)[:, :, None, None]
    span_keys = QBLOCK + 2 * WINDOW

    def attend_block(block_index):
        start_row = block_index * QBLOCK
        query_block = lax.dynamic_slice_in_dim(grouped, start_row, QBLOCK, 0)
        band = lax.dynamic_slice_in_dim(extended, start_row, span_keys, 0)
        key_block = band[:, : kv_here * HEAD_DIM].reshape(span_keys, kv_here, HEAD_DIM)
        value_block = band[:, kv_here * HEAD_DIM :].reshape(span_keys, kv_here, HEAD_DIM)
        scores = jnp.einsum("qhgd,khd->hgqk", query_block, key_block, preferred_element_type=f32) * HEAD_DIM ** (-0.5)
        query_pos = offset + start_row + jnp.arange(QBLOCK, dtype=jnp.int32)
        key_pos = offset + start_row - WINDOW + jnp.arange(span_keys, dtype=jnp.int32)
        valid = (
            (jnp.abs(key_pos[None, :] - query_pos[:, None]) <= WINDOW)
            & (key_pos[None, :] >= 0)
            & (key_pos[None, :] < seq_total)
        )
        masked = jnp.where(valid, scores, -1e30)
        largest = jnp.maximum(jnp.max(masked, axis=-1, keepdims=True), sinks)
        raised = jnp.where(valid, jnp.exp(masked - largest), 0.0)
        denominator = jnp.sum(raised, axis=-1, keepdims=True) + jnp.exp(sinks - largest)
        weights = (raised / denominator).astype(bf16)
        attended = jnp.einsum("hgqk,khd->qhgd", weights, value_block, preferred_element_type=f32)
        return attended.astype(bf16).reshape(QBLOCK, heads_here * HEAD_DIM)

    attended = lax.map(attend_block, jnp.arange(row_count // QBLOCK, dtype=jnp.int32))
    return attended.reshape(row_count, heads_here * HEAD_DIM)


def move(value, axis, shift):
    return lax.ppermute(value, axis, shifted(lax.axis_size(axis), shift))


def after(value, *others):
    return lax.optimization_barrier((value,) + others)[0]


def local(
    queries,
    key_rows,
    values,
    sink_logit,
    out_weight,
    out_gain,
    routed_tokens,
    expert_ids,
    route_weight,
    routed_gain,
    expert_gate,
    expert_up,
    expert_down,
):
    row_count = queries.shape[0]
    z, y, c, x = (lax.axis_index(axis) for axis in ("z", "y", "c", "x"))
    expert = (z * 4 + y) * 2 + c
    place = jnp.stack([z, expert, expert + 1 - 2 * c]).astype(jnp.int32)

    split = expert_up.shape[1] // 2
    part_a = jnp.concatenate((expert_gate[0], expert_up[0, :split]), axis=0)
    part_b = jnp.concatenate((expert_up[0, split:], expert_down[0]), axis=0)
    low_a = move(part_a, "x", 1)
    high_b = move(part_b, "x", -1)
    low_b = move(part_b, "x", 1)
    high_a = move(part_a, "x", -1)
    far_a = move(low_a, "x", 1)
    far_b = move(high_b, "x", -1)
    mine = (part_a, part_b, low_a, low_b, high_a, high_b, far_a, far_b)
    theirs = tuple(move(v, "c", 1) for v in mine)

    prepared = prepare(place, routed_tokens, expert_ids, route_weight, routed_gain)
    chunks = {0: prepared[0]}
    order = prepared[4]
    for s in (1, 3, 2):
        chunks[s] = move(prepared[s], "z", s)
    blocks = {}
    for s in (0, 1, 3, 2):
        low = move(chunks[s], "y", 1)
        high = move(chunks[s], "y", -1)
        far = move(low, "y", 1) if s in (0, 3) else move(high, "y", -1)
        blocks[s] = (chunks[s], low, high, far)
    sets = ((2, 3), (1, 0))
    staged = []
    for pair in sets:
        staged.append(stage(place, [block for s in pair for block in blocks[s]], mine[:6] + theirs[:6]))

    far = (mine[6], mine[7], theirs[6], theirs[7])
    downs = mine[1:6:2] + theirs[1:6:2]
    size = blocks[0][0].shape[0]
    made = []
    for which in range(2):
        made.append(results(staged[which], far, downs, size))
    back = {}
    merges = {}
    for which, pair in enumerate(sets):
        for index, s in enumerate(pair):
            way = 1 if index == 0 else -1
            p_own, p_low, p_high, p_far = made[which][4 * index : 4 * index + 4]
            straight, through = (p_low, p_high) if way == 1 else (p_high, p_low)
            began = move(p_far, "y", way)
            direct = move(straight, "y", -way)
            merged = (began.astype(f32) + through.astype(f32)).astype(bf16)
            merges[s] = merged
            ended = move(merged, "y", way)
            total = (p_own.astype(f32) + direct.astype(f32) + ended.astype(f32)).astype(bf16)
            back[s] = move(total, "z", -s) if s else total
    experts_out = finish(order, [back[s] for s in range(4)])

    extended = padded(jnp.concatenate((key_rows, values), axis=1), WINDOW)
    queries = after(queries, made[1][0])
    attended = attention(queries, extended, sink_logit, expert * row_count, row_count * 32)
    quarter = row_count // 4
    heads = attended.shape[1]
    attended = after(attended, merges[0], merges[1])
    crossed = lax.all_to_all(attended.reshape(4, quarter, heads), "x", 0, 0)
    late = after(out_weight, made[1][0])
    low = move(late, "x", 1)
    high = move(late, "x", -1)
    half = heads // 2
    across = jnp.concatenate((move(low[:half], "x", 1), move(high[half:], "x", -1)), axis=0)
    mixed = jnp.zeros((quarter, out_weight.shape[1]), f32)
    for shift, piece in ((0, out_weight), (3, low), (1, high), (2, across)):
        part = lax.dynamic_index_in_dim(crossed, lax.bitwise_and(x + shift, 3), 0, keepdims=False)
        mixed = mixed + jnp.dot(part, piece, preferred_element_type=f32)
    mixer_out = (
        mixed * lax.rsqrt(jnp.mean(mixed * mixed, axis=-1, keepdims=True) + epsilon) * out_gain
    ).astype(bf16)
    return (mixer_out, experts_out)


def solution(mesh):
    split = Mesh(mesh.devices.reshape(4, 4, 2, 4), ("z", "y", "c", "x"))
    ep = ("z", "y", "c")
    placed = (
        P(ep, "x"),
        P(ep, "x"),
        P(ep, "x"),
        P("x"),
        P("x", None),
        P(),
        P(ep + ("x",), None),
        P(ep + ("x",), None),
        P(ep + ("x",), None),
        P(),
        P(ep, None, "x"),
        P(ep, None, "x"),
        P(ep, None, "x"),
    )

    return jax.shard_map(
        local,
        mesh=split,
        in_specs=placed,
        out_specs=(P(ep + ("x",), None), P(ep + ("x",), None)),
        check_vma=False,
    )
```

```python
import jax
import jax.numpy as jnp
from jax import lax
from jax.experimental import pallas as pl
from jax.experimental.pallas import tpu as pltpu
from jax.sharding import Mesh, PartitionSpec as P


HEAD_DIM = 64
WINDOW = 128
CAP = 64
GROUPS = 4
META = 128
SET_BLOCKS = 8

epsilon = 1e-06
f32 = jnp.float32
bf16 = jnp.bfloat16
NT = (((1,), (1,)), ((), ()))
TN = (((0,), (0,)), ((), ()))
VMEM_LIMIT = 60 * 1024 * 1024


def shifted(size, shift):
    return [(i, (i + shift) % size) for i in range(size)]


def iota(shape, dim, kind=jnp.int32):
    return lax.broadcasted_iota(jnp.int32, shape, dim).astype(kind)


def prep_kernel(place, tok, ids_t, weight_t, gain, first, second, third, fourth, order):
    count = tok.shape[0]
    each = count // GROUPS
    inputs = tok[...].astype(f32)
    scale = lax.rsqrt(jnp.mean(inputs * inputs, axis=-1, keepdims=True) + epsilon)
    normed = (inputs * scale * gain[...]).astype(bf16)
    ids = ids_t[...]
    group = lax.shift_right_logical(ids[0:1, :], 3)
    relative = lax.bitwise_and(group - place[0] + GROUPS, GROUPS - 1)
    member = (iota((16, count), 0) == relative).astype(f32)
    before = (iota((count, count), 0) < iota((count, count), 1)).astype(f32).astype(bf16)
    earlier = jnp.dot(member.astype(bf16), before, preferred_element_type=f32)
    rank = jnp.sum(earlier * member, axis=0, keepdims=True)
    slot = (relative * each).astype(f32) + rank
    permute = (iota((count, count), 0, f32) == slot).astype(f32).astype(bf16)
    order[...] = permute
    rows = jnp.dot(permute, normed, preferred_element_type=f32).astype(bf16)
    line = iota((META, count), 0)
    meta = jnp.where(line == 0, ids[0:1, :].astype(f32), 0.0)
    meta = jnp.where(line == 1, ids[1:2, :].astype(f32), meta)
    for k in range(2):
        rest = weight_t[k : k + 1, :]
        for part in range(3):
            piece = rest.astype(bf16).astype(f32)
            meta = jnp.where(line == 2 + 3 * k + part, piece, meta)
            rest = rest - piece
    tags = lax.dot_general(permute, meta.astype(bf16), NT, preferred_element_type=f32).astype(bf16)
    width = tok.shape[1]
    for index, out in enumerate((first, second, third, fourth)):
        out[:, :width] = rows[index * each : (index + 1) * each]
        out[:, width:] = tags[index * each : (index + 1) * each]


def prepare(place, tokens, ids, weights, gain):
    count, width = tokens.shape
    chunk = jax.ShapeDtypeStruct((count // GROUPS, width + META), bf16)
    vmem = pl.BlockSpec(memory_space=pltpu.VMEM)
    return pl.pallas_call(
        prep_kernel,
        out_shape=(chunk, chunk, chunk, chunk, jax.ShapeDtypeStruct((count, count), bf16)),
        in_specs=[pl.BlockSpec(memory_space=pltpu.SMEM)] + [vmem] * 4,
        out_specs=(vmem,) * 5,
        compiler_params=pltpu.CompilerParams(vmem_limit_bytes=VMEM_LIMIT),
        cost_estimate=pl.CostEstimate(flops=6_000_000_000, bytes_accessed=6_000_000, transcendentals=512),
        name="prep",
    )(place, tokens, ids.T, weights.T, gain.reshape(1, width))


def choices(tags, experts):
    blocks = len(tags)
    size = tags[0].shape[0]
    lines = [jnp.transpose(t.astype(f32)) for t in tags]
    hits = [[tuple((t[k : k + 1] == e).astype(f32) for k in range(2)) for t in lines] for e in experts]
    row = iota((2 * blocks, size), 0)
    counts = jnp.zeros((2 * blocks, size), f32)
    for e in range(2):
        for b in range(blocks):
            counts = jnp.where(row == e * blocks + b, hits[e][b][0] + hits[e][b][1], counts)
    before = (iota((size, size), 0) < iota((size, size), 1)).astype(f32).astype(bf16)
    earlier = jnp.dot(counts.astype(bf16), before, preferred_element_type=f32)
    place = iota((2 * CAP, size), 0, f32)
    found = []
    for pair in range(blocks // 2):
        picks = []
        weights = []
        for e in range(2):
            halves = []
            weight = jnp.zeros((2 * CAP, size), f32)
            for j in range(2):
                b = 2 * pair + j
                hit = hits[e][b]
                slot = earlier[e * blocks + b : e * blocks + b + 1] + float(CAP * j)
                one = jnp.where(place == slot, hit[0], 0.0)
                two = jnp.where(place == slot + hit[0], hit[1], 0.0)
                halves.append(one + two)
                t = lines[b]
                weight = weight + one * (t[2:3] + t[3:4] + t[4:5]) + two * (t[5:6] + t[6:7] + t[7:8])
            picks.append(jnp.concatenate(halves, axis=1))
            weights.append(jnp.sum(weight, axis=1, keepdims=True))
        found.append((jnp.concatenate(picks, axis=0).astype(bf16), jnp.concatenate(weights, axis=0)))
    return found


def stage_kernel(place, *refs):
    sources, weights = refs[:8], refs[8:14]
    rows_out, hidden_out, pick_out, scale_out = refs[14:18]
    tok, held, rows, units, pick_v, scale_v, tok_sem, held_sem, out_sem = refs[18:]
    width = rows.shape[-1]
    wide = weights[0].shape[1]
    size = tok.shape[1]
    arrivals = []
    for b in range(SET_BLOCKS):
        source = sources[b]
        if source.shape[0] > size:
            source = source.at[pl.ds(b // 4 * size, size)]
        arrivals.append(pltpu.make_async_copy(source, tok.at[b], tok_sem.at[b]))
    both_parts = pl.ds(0, 2 * width)
    fetches = [pltpu.make_async_copy(weights[i].at[both_parts], held.at[i], held_sem.at[i]) for i in range(6)]
    for copy in arrivals + fetches:
        copy.start()
    experts = (place[1].astype(f32), place[2].astype(f32))
    for copy in arrivals:
        copy.wait()
    for pair, (pick, scale) in enumerate(choices([tok[b, :, width:] for b in range(SET_BLOCKS)], experts)):
        pick_v[pair] = pick
        scale_v[pair] = jnp.broadcast_to(scale, scale_v.shape[1:])
        both = tok[2 * pair : 2 * pair + 2, :, :width].reshape(2 * size, width)
        chosen = jnp.dot(pick, both, preferred_element_type=f32).astype(bf16)
        for e in range(2):
            rows[e, 2 * CAP * pair : 2 * CAP * (pair + 1)] = chosen[2 * CAP * e : 2 * CAP * (e + 1)]
    sent = [
        pltpu.make_async_copy(rows, rows_out, out_sem.at[0]),
        pltpu.make_async_copy(pick_v, pick_out, out_sem.at[1]),
        pltpu.make_async_copy(scale_v, scale_out, out_sem.at[2]),
    ]
    for copy in sent:
        copy.start()
    for i in range(6):
        e, shard = i // 3, i % 3
        fetches[i].wait()
        gate = jnp.dot(rows[e], held[i, :width], preferred_element_type=f32)
        up = jnp.dot(rows[e], held[i, width:], preferred_element_type=f32)
        units[e, :, shard * wide : (shard + 1) * wide] = (gate / (1.0 + jnp.exp(-gate)) * up).astype(bf16)
        if shard == 2:
            sent.append(pltpu.make_async_copy(units.at[e], hidden_out.at[e], out_sem.at[3 + e]))
            sent[-1].start()
    for copy in sent:
        copy.wait()


def stage(place, blocks, weights):
    size = min(b.shape[0] for b in blocks)
    size = size if size < 256 else size // 2
    full = blocks[0].shape[1]
    width = full - META
    wide = weights[0].shape[1]
    rows = SET_BLOCKS * CAP
    shapes = (
        ((2, rows, width), bf16),
        ((2, rows, 3 * wide), bf16),
        ((SET_BLOCKS // 2, 4 * CAP, 2 * size), bf16),
        ((SET_BLOCKS // 2, 4 * CAP, 128), f32),
    )
    held = pl.BlockSpec(memory_space=pltpu.HBM)
    return pl.pallas_call(
        stage_kernel,
        out_shape=tuple(jax.ShapeDtypeStruct(*s) for s in shapes),
        in_specs=[pl.BlockSpec(memory_space=pltpu.SMEM)] + [held] * 14,
        out_specs=(held,) * 4,
        scratch_shapes=[
            pltpu.VMEM((SET_BLOCKS, size, full), bf16),
            pltpu.VMEM((6, 2 * width, wide), bf16),
        ]
        + [pltpu.VMEM(*s) for s in shapes]
        + [
            pltpu.SemaphoreType.DMA((SET_BLOCKS,)),
            pltpu.SemaphoreType.DMA((6,)),
            pltpu.SemaphoreType.DMA((5,)),
        ],
        compiler_params=pltpu.CompilerParams(vmem_limit_bytes=VMEM_LIMIT),
        cost_estimate=pl.CostEstimate(flops=10_000_000_000, bytes_accessed=24_000_000, transcendentals=0),
    )(place, *blocks, *weights)


def result_kernel(halves, *refs):
    staged, far, downs = (refs[:4], refs[4:8]), refs[8:12], refs[12:18]
    outs = refs[18:26]
    rows, units, pick_v, scale_v, held, down_v, sem = refs[26:]
    width = rows.shape[-1]
    part, wide = far[0].shape
    rest = 2 * width - part
    each = rows.shape[1] // 2
    first, second = [], []
    for e in range(2):
        for j in range(2):
            source = staged[j][0].at[e, pl.ds(halves[j] * each, each)]
            first.append(pltpu.make_async_copy(source, rows.at[e, pl.ds(j * each, each)], sem.at[4 * e + j]))
        first.append(pltpu.make_async_copy(far[2 * e], held.at[e, pl.ds(0, part)], sem.at[4 * e + 2]))
        first.append(pltpu.make_async_copy(far[2 * e + 1].at[pl.ds(0, rest)], held.at[e, pl.ds(part, rest)], sem.at[4 * e + 3]))
    for e in range(2):
        for j in range(2):
            source = staged[j][1].at[e, pl.ds(halves[j] * each, each)]
            target = units.at[e, pl.ds(j * each, each), pl.ds(0, 3 * wide)]
            second.append(pltpu.make_async_copy(source, target, sem.at[8 + 2 * e + j]))
    for e in range(2):
        for shard in range(4):
            source = far[2 * e + 1].at[pl.ds(rest, width)] if shard == 3 else downs[3 * e + shard].at[pl.ds(2 * width, width)]
            target = down_v.at[e, :, pl.ds(shard * wide, wide)]
            second.append(pltpu.make_async_copy(source, target, sem.at[12 + 4 * e + shard]))
    for j in range(2):
        pairs, place = pl.ds(2 * halves[j], 2), pl.ds(2 * j, 2)
        second.append(pltpu.make_async_copy(staged[j][2].at[pairs], pick_v.at[place], sem.at[20 + j]))
        second.append(pltpu.make_async_copy(staged[j][3].at[pairs], scale_v.at[place], sem.at[22 + j]))
    for copy in first + second:
        copy.start()
    for e in range(2):
        for copy in first[4 * e : 4 * e + 4]:
            copy.wait()
        gate = jnp.dot(rows[e], held[e, :width], preferred_element_type=f32)
        up = jnp.dot(rows[e], held[e, width:], preferred_element_type=f32)
        units[e, :, 3 * wide :] = (gate / (1.0 + jnp.exp(-gate)) * up).astype(bf16)
    for copy in second:
        copy.wait()
    size = outs[0].shape[0]
    half = width // 2

    def one_half(h, _):
        cols = pl.ds(pl.multiple_of(h * half, half), half)
        made = [
            lax.dot_general(units[e], down_v[e, cols, :], NT, preferred_element_type=f32).astype(bf16).astype(f32)
            for e in range(2)
        ]
        for pair in range(SET_BLOCKS // 2):
            lines = slice(2 * CAP * pair, 2 * CAP * (pair + 1))
            result = jnp.concatenate([made[0][lines], made[1][lines]], axis=0)
            scaled = (result * scale_v[pair, :, 0:1]).astype(bf16)
            spread = lax.dot_general(pick_v[pair], scaled, TN, preferred_element_type=f32).astype(bf16)
            outs[2 * pair][:, cols] = spread[:size]
            outs[2 * pair + 1][:, cols] = spread[size:]
        return 0

    lax.fori_loop(0, 2, one_half, 0)


def results(staged, halves, far, downs, size):
    rows, _, picks, scales = staged[0]
    width = rows.shape[-1]
    wide = far[0].shape[1]
    held = pl.BlockSpec(memory_space=pltpu.HBM)
    vmem = pl.BlockSpec(memory_space=pltpu.VMEM)
    return pl.pallas_call(
        lambda *refs: result_kernel(halves, *refs),
        out_shape=(jax.ShapeDtypeStruct((size, width), bf16),) * SET_BLOCKS,
        in_specs=[held] * 18,
        out_specs=(vmem,) * SET_BLOCKS,
        scratch_shapes=[
            pltpu.VMEM(rows.shape, bf16),
            pltpu.VMEM((2, rows.shape[1], 4 * wide), bf16),
            pltpu.VMEM(picks.shape, bf16),
            pltpu.VMEM(scales.shape, f32),
            pltpu.VMEM((2, 2 * width, wide), bf16),
            pltpu.VMEM((2, width, 4 * wide), bf16),
            pltpu.SemaphoreType.DMA((24,)),
        ],
        compiler_params=pltpu.CompilerParams(vmem_limit_bytes=VMEM_LIMIT),
        cost_estimate=pl.CostEstimate(flops=8_000_000_000, bytes_accessed=24_000_000, transcendentals=0),
    )(*staged[0], *staged[1], *far, *downs)


def finish_kernel(order, first, second, third, fourth, out):
    each = first.shape[0]
    total = jnp.zeros(out.shape, f32)
    for index, piece in enumerate((first, second, third, fourth)):
        total = total + lax.dot_general(
            order[index * each : (index + 1) * each, :], piece[...], TN, preferred_element_type=f32
        )
    out[...] = total.astype(bf16)


def finish(order, pieces):
    count = order.shape[0]
    width = pieces[0].shape[1]
    vmem = pl.BlockSpec(memory_space=pltpu.VMEM)
    return pl.pallas_call(
        finish_kernel,
        out_shape=jax.ShapeDtypeStruct((count, width), bf16),
        in_specs=[vmem] * 5,
        out_specs=vmem,
        compiler_params=pltpu.CompilerParams(vmem_limit_bytes=VMEM_LIMIT),
        cost_estimate=pl.CostEstimate(flops=2_000_000_000, bytes_accessed=5_000_000, transcendentals=0),
        name="finish",
    )(order, *pieces)


def padded(block, width):
    axes = ("z", "y", "c")
    count = 1
    for axis in axes:
        count *= lax.axis_size(axis)
    forward = [(i, i + 1) for i in range(count - 1)]
    backward = [(target, source) for source, target in forward]
    low = lax.ppermute(block[-width:], axes, forward)
    high = lax.ppermute(block[:width], axes, backward)
    return jnp.concatenate([low, block, high], axis=0)


def attention_kernel(bounds, sinks, queries, extended, out):
    heads = queries.shape[1] // HEAD_DIM
    total = bounds[1]
    span = 3 * WINDOW
    lines = heads * WINDOW
    row = iota((lines, span), 0)
    col = iota((lines, span), 1)
    away = col - lax.bitwise_and(row, WINDOW - 1)
    near = (away >= 0) & (away <= 2 * WINDOW)
    head = lax.shift_right_logical(iota((lines, 1), 0), 7)
    sink = jnp.zeros((lines, 1), f32)
    for h in range(heads):
        sink = jnp.where(head == h, sinks[h], sink)

    def one_block(block, _):
        start = pl.multiple_of(block * WINDOW, WINDOW)
        asked = queries[pl.ds(start, WINDOW), :]
        stacked = jnp.concatenate([asked[:, h * HEAD_DIM : (h + 1) * HEAD_DIM] for h in range(heads)], axis=0)
        band = extended[pl.ds(start, span), :]
        keys, held = band[:, :HEAD_DIM], band[:, HEAD_DIM:]
        scores = lax.dot_general(stacked, keys, NT, preferred_element_type=f32) * HEAD_DIM ** (-0.5)
        place = bounds[0] + start - WINDOW + col
        masked = jnp.where(near & (place >= 0) & (place < total), scores, -1e30)
        largest = jnp.maximum(jnp.max(masked, axis=-1, keepdims=True), sink)
        raised = jnp.exp(masked - largest)
        denominator = jnp.sum(raised, axis=-1, keepdims=True) + jnp.exp(sink - largest)
        weights = (raised * (1.0 / denominator)).astype(bf16)
        made = jnp.dot(weights, held, preferred_element_type=f32).astype(bf16)
        pieces = [made[h * WINDOW : (h + 1) * WINDOW] for h in range(heads)]
        out[pl.ds(start, WINDOW), :] = jnp.concatenate(pieces, axis=1)
        return 0

    lax.fori_loop(0, queries.shape[0] // WINDOW, one_block, 0)


def attention(queries, extended, sink_logit, offset, seq_total):
    smem = pl.BlockSpec(memory_space=pltpu.SMEM)
    vmem = pl.BlockSpec(memory_space=pltpu.VMEM)
    bounds = jnp.stack([offset, jnp.int32(seq_total)]).astype(jnp.int32)
    return pl.pallas_call(
        attention_kernel,
        out_shape=jax.ShapeDtypeStruct(queries.shape, bf16),
        in_specs=[smem, smem, vmem, vmem],
        out_specs=vmem,
        compiler_params=pltpu.CompilerParams(vmem_limit_bytes=VMEM_LIMIT // 2),
        cost_estimate=pl.CostEstimate(flops=6_000_000_000, bytes_accessed=1_500_000, transcendentals=1_600_000),
        name="attention",
    )(bounds, sink_logit, queries, extended)


def move(value, axis, shift):
    return lax.ppermute(value, axis, shifted(lax.axis_size(axis), shift))


def after(value, *others):
    return lax.optimization_barrier((value,) + others)[0]


def local(
    queries,
    key_rows,
    values,
    sink_logit,
    out_weight,
    out_gain,
    routed_tokens,
    expert_ids,
    route_weight,
    routed_gain,
    expert_gate,
    expert_up,
    expert_down,
):
    row_count = queries.shape[0]
    z, y, c, x = (lax.axis_index(axis) for axis in ("z", "y", "c", "x"))
    expert = (z * 4 + y) * 2 + c
    place = jnp.stack([z, expert, expert + 1 - 2 * c]).astype(jnp.int32)

    packed = jnp.concatenate((expert_gate[0], expert_up[0], expert_down[0]), axis=0)
    middle = packed.shape[0] // 2
    low = move(packed, "x", 1)
    high = move(packed, "x", -1)
    pass_a, pass_b = low[:middle], high[middle:]
    far_a = move(pass_a, "x", 1)
    far_b = move(pass_b, "x", -1)
    mine = (packed, low, high, far_a, far_b)
    theirs = tuple(move(v, "c", 1) for v in mine)

    prepared = prepare(place, routed_tokens, expert_ids, route_weight, routed_gain)
    own, order = prepared[0], prepared[4]
    size = own.shape[0]
    out = {s: move(prepared[s], "z", s) for s in (1, 3, 2)}
    joined = jnp.concatenate((out[1], out[3]), axis=0)
    groups = {"0": own, "13": joined, "2": out[2]}
    blocks = {}
    for name, chunk in groups.items():
        near_low = move(chunk, "y", 1)
        near_high = move(chunk, "y", -1)
        beyond = move(near_low, "y", 1) if name == "13" else move(near_high, "y", -1)
        blocks[name] = (chunk, near_low, near_high, beyond)
    staged_a = stage(place, blocks["13"] * 2, mine[:3] + theirs[:3])
    staged_b = stage(place, blocks["0"] + blocks["2"], mine[:3] + theirs[:3])

    extended = padded(jnp.concatenate((key_rows, values), axis=1), WINDOW)
    attended = attention(queries, extended, sink_logit, expert * row_count, row_count * 32)

    far = mine[3:] + theirs[3:]
    downs = mine[:3] + theirs[:3]
    sets = ((2, 3), (1, 0))
    made = []
    for which, halves in enumerate(((1, 1), (0, 0))):
        parts = (staged_b, staged_a) if which == 0 else (staged_a, staged_b)
        made.append(results(parts, halves, far, downs, size))
    back = {}
    merges = {}
    for which, pair in enumerate(sets):
        for index, s in enumerate(pair):
            way = 1 if index == 0 else -1
            p_own, p_low, p_high, p_far = made[which][4 * index : 4 * index + 4]
            straight, through = (p_low, p_high) if way == 1 else (p_high, p_low)
            began = move(p_far, "y", way)
            direct = move(straight, "y", -way)
            merged = (began.astype(f32) + through.astype(f32)).astype(bf16)
            merges[s] = merged
            ended = move(merged, "y", way)
            total = (p_own.astype(f32) + direct.astype(f32) + ended.astype(f32)).astype(bf16)
            back[s] = move(total, "z", -s) if s else total
    experts_out = finish(order, [back[s] for s in range(4)])

    quarter = row_count // 4
    heads = attended.shape[1]
    attended = after(attended, merges[0], merges[1])
    crossed = lax.all_to_all(attended.reshape(4, quarter, heads), "x", 0, 0)
    late = after(out_weight, made[1][0])
    low = move(late, "x", 1)
    high = move(late, "x", -1)
    half = heads // 2
    across = jnp.concatenate((move(low[:half], "x", 1), move(high[half:], "x", -1)), axis=0)
    mixed = jnp.zeros((quarter, out_weight.shape[1]), f32)
    for shift, piece in ((0, out_weight), (3, low), (1, high), (2, across)):
        part = lax.dynamic_index_in_dim(crossed, lax.bitwise_and(x + shift, 3), 0, keepdims=False)
        mixed = mixed + jnp.dot(part, piece, preferred_element_type=f32)
    mixer_out = (
        mixed * lax.rsqrt(jnp.mean(mixed * mixed, axis=-1, keepdims=True) + epsilon) * out_gain
    ).astype(bf16)
    return (mixer_out, experts_out)


def solution(mesh):
    split = Mesh(mesh.devices.reshape(4, 4, 2, 4), ("z", "y", "c", "x"))
    ep = ("z", "y", "c")
    placed = (
        P(ep, "x"),
        P(ep, "x"),
        P(ep, "x"),
        P("x"),
        P("x", None),
        P(),
        P(ep + ("x",), None),
        P(ep + ("x",), None),
        P(ep + ("x",), None),
        P(),
        P(ep, None, "x"),
        P(ep, None, "x"),
        P(ep, None, "x"),
    )

    return jax.shard_map(
        local,
        mesh=split,
        in_specs=placed,
        out_specs=(P(ep + ("x",), None), P(ep + ("x",), None)),
        check_vma=False,
    )
```

```python
import jax
import jax.numpy as jnp
from jax import lax
from jax.experimental import pallas as pl
from jax.experimental.pallas import tpu as pltpu
from jax.sharding import Mesh, PartitionSpec as P


HEAD_DIM = 64
WINDOW = 128
CAP = 64
GROUPS = 4
META = 128
SET_BLOCKS = 8

epsilon = 1e-06
f32 = jnp.float32
bf16 = jnp.bfloat16
NT = (((1,), (1,)), ((), ()))
TN = (((0,), (0,)), ((), ()))
VMEM_LIMIT = 60 * 1024 * 1024


def shifted(size, shift):
    return [(i, (i + shift) % size) for i in range(size)]


def iota(shape, dim, kind=jnp.int32):
    return lax.broadcasted_iota(jnp.int32, shape, dim).astype(kind)


def prep_kernel(place, tok, ids_t, weight_t, gain, first, second, third, fourth, order):
    count, width = tok.shape
    each = count // GROUPS
    inputs = tok[...].astype(f32)
    scale = lax.rsqrt(jnp.mean(inputs * inputs, axis=-1, keepdims=True) + epsilon)
    ids = ids_t[...]
    group = lax.shift_right_logical(ids[0:1, :], 3)
    relative = lax.bitwise_and(group - place[0] + GROUPS, GROUPS - 1)
    member = (iota((16, count), 0) == relative).astype(f32)
    before = (iota((count, count), 0) < iota((count, count), 1)).astype(f32).astype(bf16)
    earlier = jnp.dot(member.astype(bf16), before, preferred_element_type=f32)
    rank = jnp.sum(earlier * member, axis=0, keepdims=True)
    slot = (relative * each).astype(f32) + rank
    order[...] = (iota((count, count), 0, f32) == slot).astype(f32).astype(bf16)
    outs = (first, second, third, fourth)
    line = iota((META, count), 0)
    meta = jnp.where(line == 0, ids[0:1, :].astype(f32), 0.0)
    meta = jnp.where(line == 1, ids[1:2, :].astype(f32), meta)
    for k in range(2):
        rest = weight_t[k : k + 1, :]
        for part in range(3):
            piece = rest.astype(bf16).astype(f32)
            meta = jnp.where(line == 2 + 3 * k + part, piece, meta)
            rest = rest - piece
    tags = lax.dot_general(order[...], meta.astype(bf16), NT, preferred_element_type=f32).astype(bf16)
    for index, out in enumerate(outs):
        out[:, width:] = tags[index * each : (index + 1) * each]
    wide = width // 4

    def columns(i, _):
        cols = pl.ds(pl.multiple_of(i * wide, wide), wide)
        normed = (tok[:, cols].astype(f32) * scale * gain[:, cols]).astype(bf16)
        rows = jnp.dot(order[...], normed, preferred_element_type=f32).astype(bf16)
        for index, out in enumerate(outs):
            out[:, cols] = rows[index * each : (index + 1) * each]
        return 0

    lax.fori_loop(0, 4, columns, 0)


def prepare(place, tokens, ids, weights, gain):
    count, width = tokens.shape
    chunk = jax.ShapeDtypeStruct((count // GROUPS, width + META), bf16)
    vmem = pl.BlockSpec(memory_space=pltpu.VMEM)
    return pl.pallas_call(
        prep_kernel,
        out_shape=(chunk, chunk, chunk, chunk, jax.ShapeDtypeStruct((count, count), bf16)),
        in_specs=[pl.BlockSpec(memory_space=pltpu.SMEM)] + [vmem] * 4,
        out_specs=(vmem,) * 5,
        compiler_params=pltpu.CompilerParams(vmem_limit_bytes=VMEM_LIMIT),
        cost_estimate=pl.CostEstimate(flops=6_000_000_000, bytes_accessed=6_000_000, transcendentals=512),
        name="prep",
    )(place, tokens, ids.T, weights.T, gain.reshape(1, width))


def choices(tags, experts):
    blocks = len(tags)
    size = tags[0].shape[0]
    lines = [jnp.transpose(t.astype(f32)) for t in tags]
    hits = [[tuple((t[k : k + 1] == e).astype(f32) for k in range(2)) for t in lines] for e in experts]
    row = iota((2 * blocks, size), 0)
    counts = jnp.zeros((2 * blocks, size), f32)
    for e in range(2):
        for b in range(blocks):
            counts = jnp.where(row == e * blocks + b, hits[e][b][0] + hits[e][b][1], counts)
    before = (iota((size, size), 0) < iota((size, size), 1)).astype(f32).astype(bf16)
    earlier = jnp.dot(counts.astype(bf16), before, preferred_element_type=f32)
    place = iota((2 * CAP, size), 0, f32)
    found = []
    for pair in range(blocks // 2):
        picks = []
        weights = []
        for e in range(2):
            halves = []
            weight = jnp.zeros((2 * CAP, size), f32)
            for j in range(2):
                b = 2 * pair + j
                hit = hits[e][b]
                slot = earlier[e * blocks + b : e * blocks + b + 1] + float(CAP * j)
                one = jnp.where(place == slot, hit[0], 0.0)
                two = jnp.where(place == slot + hit[0], hit[1], 0.0)
                halves.append(one + two)
                t = lines[b]
                weight = weight + one * (t[2:3] + t[3:4] + t[4:5]) + two * (t[5:6] + t[6:7] + t[7:8])
            picks.append(jnp.concatenate(halves, axis=1))
            weights.append(jnp.sum(weight, axis=1, keepdims=True))
        found.append((jnp.concatenate(picks, axis=0).astype(bf16), jnp.concatenate(weights, axis=0)))
    return found


def stage_kernel(place, *refs):
    sources, weights = refs[:8], refs[8:20]
    rows_out, hidden_out, pick_out, scale_out = refs[20:24]
    tok, held, rows, units, pick_v, scale_v, tok_sem, held_sem, out_sem = refs[24:]
    width = rows.shape[-1]
    part, wide = weights[0].shape
    rest = 2 * width - part
    size = tok.shape[1]
    arrivals = []
    for b in range(SET_BLOCKS):
        source = sources[b]
        if source.shape[0] > size:
            source = source.at[pl.ds(b // 4 * size, size)]
        arrivals.append(pltpu.make_async_copy(source, tok.at[b], tok_sem.at[b]))
    fetches = []
    for i in range(6):
        fetches.append(
            (
                pltpu.make_async_copy(weights[2 * i], held.at[i, pl.ds(0, part)], held_sem.at[0, i]),
                pltpu.make_async_copy(
                    weights[2 * i + 1].at[pl.ds(0, rest)], held.at[i, pl.ds(part, rest)], held_sem.at[1, i]
                ),
            )
        )
    for copy in arrivals:
        copy.start()
    for copy in fetches[0]:
        copy.start()
    experts = (place[1].astype(f32), place[2].astype(f32))
    for copy in arrivals:
        copy.wait()
    for pair_of in fetches[1:]:
        for copy in pair_of:
            copy.start()
    for pair, (pick, scale) in enumerate(choices([tok[b, :, width:] for b in range(SET_BLOCKS)], experts)):
        pick_v[pair] = pick
        scale_v[pair] = jnp.broadcast_to(scale, scale_v.shape[1:])
        both = tok[2 * pair : 2 * pair + 2, :, :width].reshape(2 * size, width)
        chosen = jnp.dot(pick, both, preferred_element_type=f32).astype(bf16)
        for e in range(2):
            rows[e, 2 * CAP * pair : 2 * CAP * (pair + 1)] = chosen[2 * CAP * e : 2 * CAP * (e + 1)]
    sent = [
        pltpu.make_async_copy(rows, rows_out, out_sem.at[0]),
        pltpu.make_async_copy(pick_v, pick_out, out_sem.at[1]),
        pltpu.make_async_copy(scale_v, scale_out, out_sem.at[2]),
    ]
    for copy in sent:
        copy.start()

    def one_shard(i, _):
        e = i // 3
        shard = i - 3 * e
        pltpu.make_async_copy(weights[0], held.at[i, pl.ds(0, part)], held_sem.at[0, i]).wait()
        pltpu.make_async_copy(weights[1].at[pl.ds(0, rest)], held.at[i, pl.ds(part, rest)], held_sem.at[1, i]).wait()
        gate = jnp.dot(rows[e], held[i, :width], preferred_element_type=f32)
        up = jnp.dot(rows[e], held[i, width:], preferred_element_type=f32)
        columns = pl.ds(pl.multiple_of(shard * wide, wide), wide)
        units[e, :, columns] = (gate / (1.0 + jnp.exp(-gate)) * up).astype(bf16)
        return 0

    lax.fori_loop(0, 6, one_shard, 0)
    sent.append(pltpu.make_async_copy(units, hidden_out, out_sem.at[3]))
    sent[-1].start()
    for copy in sent:
        copy.wait()


def stage(place, blocks, weights):
    size = min(b.shape[0] for b in blocks)
    size = size if size < 256 else size // 2
    full = blocks[0].shape[1]
    width = full - META
    wide = weights[0].shape[1]
    rows = SET_BLOCKS * CAP
    shapes = (
        ((2, rows, width), bf16),
        ((2, rows, 3 * wide), bf16),
        ((SET_BLOCKS // 2, 4 * CAP, 2 * size), bf16),
        ((SET_BLOCKS // 2, 4 * CAP, 128), f32),
    )
    held = pl.BlockSpec(memory_space=pltpu.HBM)
    return pl.pallas_call(
        stage_kernel,
        out_shape=tuple(jax.ShapeDtypeStruct(*s) for s in shapes),
        in_specs=[pl.BlockSpec(memory_space=pltpu.SMEM)] + [held] * 20,
        out_specs=(held,) * 4,
        scratch_shapes=[
            pltpu.VMEM((SET_BLOCKS, size, full), bf16),
            pltpu.VMEM((6, 2 * width, wide), bf16),
        ]
        + [pltpu.VMEM(*s) for s in shapes]
        + [
            pltpu.SemaphoreType.DMA((SET_BLOCKS,)),
            pltpu.SemaphoreType.DMA((2, 6)),
            pltpu.SemaphoreType.DMA((4,)),
        ],
        compiler_params=pltpu.CompilerParams(vmem_limit_bytes=VMEM_LIMIT),
        cost_estimate=pl.CostEstimate(flops=10_000_000_000, bytes_accessed=24_000_000, transcendentals=0),
    )(place, *blocks, *weights)


def result_kernel(halves, *refs):
    staged, far, downs = (refs[:4], refs[4:8]), refs[8:12], refs[12:18]
    outs = refs[18:26]
    rows, units, pick_v, scale_v, held, down_v, made, sem = refs[26:]
    width = rows.shape[-1]
    part, wide = far[0].shape
    rest = 2 * width - part
    each = rows.shape[1] // 2
    first, second = [], []
    for e in range(2):
        for j in range(2):
            source = staged[j][0].at[e, pl.ds(halves[j] * each, each)]
            first.append(pltpu.make_async_copy(source, rows.at[e, pl.ds(j * each, each)], sem.at[4 * e + j]))
        first.append(pltpu.make_async_copy(far[2 * e], held.at[e, pl.ds(0, part)], sem.at[4 * e + 2]))
        first.append(pltpu.make_async_copy(far[2 * e + 1].at[pl.ds(0, rest)], held.at[e, pl.ds(part, rest)], sem.at[4 * e + 3]))
    for e in range(2):
        for j in range(2):
            source = staged[j][1].at[e, pl.ds(halves[j] * each, each)]
            target = units.at[e, pl.ds(j * each, each), pl.ds(0, 3 * wide)]
            second.append(pltpu.make_async_copy(source, target, sem.at[8 + 6 * e + j]))
        for shard in range(4):
            source = (far[2 * e + 1] if shard == 3 else downs[3 * e + shard]).at[pl.ds(rest, width)]
            target = down_v.at[e, :, pl.ds(shard * wide, wide)]
            second.append(pltpu.make_async_copy(source, target, sem.at[10 + 6 * e + shard]))
    third = []
    for j in range(2):
        pairs, place = pl.ds(2 * halves[j], 2), pl.ds(2 * j, 2)
        third.append(pltpu.make_async_copy(staged[j][2].at[pairs], pick_v.at[place], sem.at[20 + j]))
        third.append(pltpu.make_async_copy(staged[j][3].at[pairs], scale_v.at[place], sem.at[22 + j]))
    stages = [first[:4], first[4:], second[:6], second[6:] + third]

    def begin(group):
        for copy in stages[group]:
            copy.start()

    def arrive(group):
        for copy in stages[group]:
            copy.wait()

    def far_units(e):
        gate = jnp.dot(rows[e], held[e, :width], preferred_element_type=f32)
        up = jnp.dot(rows[e], held[e, width:], preferred_element_type=f32)
        units[e, :, 3 * wide :] = (gate / (1.0 + jnp.exp(-gate)) * up).astype(bf16)

    quarter = width // 4

    def project(e):
        def columns(i, _):
            cols = pl.ds(pl.multiple_of(i * quarter, quarter), quarter)
            made[e, :, cols] = lax.dot_general(
                units[e], down_v[e, cols, :], NT, preferred_element_type=f32
            ).astype(bf16)
            return 0

        lax.fori_loop(0, 4, columns, 0)

    begin(0)
    begin(1)
    arrive(0)
    begin(2)

    def both(e, _):
        @pl.when(e == 1)
        def _():
            arrive(1)
            begin(3)

        far_units(e)
        return 0

    lax.fori_loop(0, 2, both, 0)

    def down(e, _):
        @pl.when(e == 0)
        def _():
            arrive(2)

        @pl.when(e == 1)
        def _():
            arrive(3)

        project(e)
        return 0

    lax.fori_loop(0, 2, down, 0)
    size = outs[0].shape[0]

    def columns(i, _):
        cols = pl.ds(pl.multiple_of(i * quarter, quarter), quarter)
        for pair in range(SET_BLOCKS // 2):
            lines = slice(2 * CAP * pair, 2 * CAP * (pair + 1))
            result = jnp.concatenate([made[0, lines, cols], made[1, lines, cols]], axis=0).astype(f32)
            scaled = (result * scale_v[pair, :, 0:1]).astype(bf16)
            spread = lax.dot_general(pick_v[pair], scaled, TN, preferred_element_type=f32).astype(bf16)
            outs[2 * pair][:, cols] = spread[:size]
            outs[2 * pair + 1][:, cols] = spread[size:]
        return 0

    lax.fori_loop(0, 4, columns, 0)


def results(staged, halves, far, downs, size):
    rows, _, picks, scales = staged[0]
    width = rows.shape[-1]
    wide = far[0].shape[1]
    held = pl.BlockSpec(memory_space=pltpu.HBM)
    vmem = pl.BlockSpec(memory_space=pltpu.VMEM)
    return pl.pallas_call(
        lambda *refs: result_kernel(halves, *refs),
        out_shape=(jax.ShapeDtypeStruct((size, width), bf16),) * SET_BLOCKS,
        in_specs=[held] * 18,
        out_specs=(vmem,) * SET_BLOCKS,
        scratch_shapes=[
            pltpu.VMEM(rows.shape, bf16),
            pltpu.VMEM((2, rows.shape[1], 4 * wide), bf16),
            pltpu.VMEM(picks.shape, bf16),
            pltpu.VMEM(scales.shape, f32),
            pltpu.VMEM((2, 2 * width, wide), bf16),
            pltpu.VMEM((2, width, 4 * wide), bf16),
            pltpu.VMEM(rows.shape, bf16),
            pltpu.SemaphoreType.DMA((24,)),
        ],
        compiler_params=pltpu.CompilerParams(vmem_limit_bytes=VMEM_LIMIT),
        cost_estimate=pl.CostEstimate(flops=8_000_000_000, bytes_accessed=24_000_000, transcendentals=0),
    )(*staged[0], *staged[1], *far, *downs)


def finish_kernel(order, first, second, third, fourth, out):
    _, width = first.shape
    wide = width // 4

    def columns(i, _):
        cols = pl.ds(pl.multiple_of(i * wide, wide), wide)
        rows = jnp.concatenate([piece[:, cols] for piece in (first, second, third, fourth)], axis=0)
        out[:, cols] = lax.dot_general(order[...], rows, TN, preferred_element_type=f32).astype(bf16)
        return 0

    lax.fori_loop(0, 4, columns, 0)


def finish(order, pieces):
    count = order.shape[0]
    width = pieces[0].shape[1]
    vmem = pl.BlockSpec(memory_space=pltpu.VMEM)
    return pl.pallas_call(
        finish_kernel,
        out_shape=jax.ShapeDtypeStruct((count, width), bf16),
        in_specs=[vmem] * 5,
        out_specs=vmem,
        compiler_params=pltpu.CompilerParams(vmem_limit_bytes=VMEM_LIMIT),
        cost_estimate=pl.CostEstimate(flops=2_000_000_000, bytes_accessed=5_000_000, transcendentals=0),
        name="finish",
    )(order, *pieces)


def padded(block, width):
    axes = ("z", "y", "c")
    count = 1
    for axis in axes:
        count *= lax.axis_size(axis)
    forward = [(i, i + 1) for i in range(count - 1)]
    backward = [(target, source) for source, target in forward]
    low = lax.ppermute(block[-width:], axes, forward)
    high = lax.ppermute(block[:width], axes, backward)
    return jnp.concatenate([low, block, high], axis=0)


def attention_kernel(bounds, sinks, queries, extended, out):
    heads = queries.shape[1] // HEAD_DIM
    total = bounds[1]
    span = 3 * WINDOW
    lines = heads * WINDOW
    row = iota((lines, span), 0)
    col = iota((lines, span), 1)
    away = col - lax.bitwise_and(row, WINDOW - 1)
    near = (away >= 0) & (away <= 2 * WINDOW)
    head = lax.shift_right_logical(iota((lines, 1), 0), 7)
    sink = jnp.zeros((lines, 1), f32)
    for h in range(heads):
        sink = jnp.where(head == h, sinks[h], sink)

    blocks = queries.shape[0] // WINDOW

    def one_block(index, _):
        block = lax.bitwise_and(index + bounds[2], blocks - 1)
        start = pl.multiple_of(block * WINDOW, WINDOW)
        asked = queries[pl.ds(start, WINDOW), :]
        stacked = jnp.concatenate([asked[:, h * HEAD_DIM : (h + 1) * HEAD_DIM] for h in range(heads)], axis=0)
        band = extended[pl.ds(start, span), :]
        keys, held = band[:, :HEAD_DIM], band[:, HEAD_DIM:]
        scores = lax.dot_general(stacked, keys, NT, preferred_element_type=f32) * HEAD_DIM ** (-0.5)
        place = bounds[0] + start - WINDOW + col
        masked = jnp.where(near & (place >= 0) & (place < total), scores, -1e30)
        largest = jnp.maximum(jnp.max(masked, axis=-1, keepdims=True), sink)
        raised = jnp.exp(masked - largest)
        denominator = jnp.sum(raised, axis=-1, keepdims=True) + jnp.exp(sink - largest)
        weights = (raised * (1.0 / denominator)).astype(bf16)
        made = jnp.dot(weights, held, preferred_element_type=f32).astype(bf16)
        pieces = [made[h * WINDOW : (h + 1) * WINDOW] for h in range(heads)]
        out[pl.ds(pl.multiple_of(index * WINDOW, WINDOW), WINDOW), :] = jnp.concatenate(pieces, axis=1)
        return 0

    lax.fori_loop(0, blocks, one_block, 0)


def attention(queries, extended, sink_logit, offset, seq_total, turn):
    smem = pl.BlockSpec(memory_space=pltpu.SMEM)
    vmem = pl.BlockSpec(memory_space=pltpu.VMEM)
    bounds = jnp.stack([offset, jnp.int32(seq_total), turn]).astype(jnp.int32)
    return pl.pallas_call(
        attention_kernel,
        out_shape=jax.ShapeDtypeStruct(queries.shape, bf16),
        in_specs=[smem, smem, vmem, vmem],
        out_specs=vmem,
        compiler_params=pltpu.CompilerParams(vmem_limit_bytes=VMEM_LIMIT // 2),
        cost_estimate=pl.CostEstimate(flops=6_000_000_000, bytes_accessed=1_500_000, transcendentals=1_600_000),
        name="attention",
    )(bounds, sink_logit, queries, extended)


def move(value, axis, shift):
    return lax.ppermute(value, axis, shifted(lax.axis_size(axis), shift))


def after(value, *others):
    return lax.optimization_barrier((value,) + others)[0]


def local(
    queries,
    key_rows,
    values,
    sink_logit,
    out_weight,
    out_gain,
    routed_tokens,
    expert_ids,
    route_weight,
    routed_gain,
    expert_gate,
    expert_up,
    expert_down,
):
    row_count = queries.shape[0]
    z, y, c, x = (lax.axis_index(axis) for axis in ("z", "y", "c", "x"))
    expert = (z * 4 + y) * 2 + c
    place = jnp.stack([z, expert, expert + 1 - 2 * c]).astype(jnp.int32)

    split = expert_up.shape[1] // 2
    part_a = jnp.concatenate((expert_gate[0], expert_up[0, :split]), axis=0)
    part_b = jnp.concatenate((expert_up[0, split:], expert_down[0]), axis=0)
    low_a = move(part_a, "x", 1)
    high_b = move(part_b, "x", -1)
    low_b = move(part_b, "x", 1)
    high_a = move(part_a, "x", -1)
    far_a = move(low_a, "x", 1)
    far_b = move(high_b, "x", -1)
    mine = (part_a, part_b, low_a, low_b, high_a, high_b, far_a, far_b)
    prepared = prepare(place, routed_tokens, expert_ids, route_weight, routed_gain)
    own, order = prepared[0], prepared[4]
    size = own.shape[0]
    out = {s: move(prepared[s], "z", s) for s in (1, 3, 2)}
    joined = jnp.concatenate((out[1], out[3]), axis=0)
    groups = {"0": own, "13": joined, "2": out[2]}
    blocks = {}
    for name, chunk in groups.items():
        near_low = move(chunk, "y", 1)
        near_high = move(chunk, "y", -1)
        beyond = move(near_low, "y", 1) if name == "13" else move(near_high, "y", -1)
        blocks[name] = (chunk, near_low, near_high, beyond)

    extended = padded(jnp.concatenate((key_rows, values), axis=1), WINDOW)
    attended = attention(queries, extended, sink_logit, expert * row_count, row_count * 32, 2 * x)
    quarter = row_count // 4
    theirs = tuple(move(v, "c", 1) for v in mine)

    staged_a = stage(place, blocks["13"] * 2, mine[:6] + theirs[:6])
    staged_b = stage(place, blocks["0"] + blocks["2"], mine[:6] + theirs[:6])

    far = mine[6:] + theirs[6:]
    downs = mine[1:6:2] + theirs[1:6:2]
    sets = ((2, 3), (1, 0))
    made = []
    for which, halves in enumerate(((1, 1), (0, 0))):
        parts = (staged_b, staged_a) if which == 0 else (staged_a, staged_b)
        made.append(results(parts, halves, far, downs, size))
    back = {}
    for which, pair in enumerate(sets):
        for index, s in enumerate(pair):
            way = 1 if index == 0 else -1
            p_own, p_low, p_high, p_far = made[which][4 * index : 4 * index + 4]
            straight, through = (p_low, p_high) if way == 1 else (p_high, p_low)
            began = move(p_far, "y", way)
            direct = move(straight, "y", -way)
            merged = (began.astype(f32) + through.astype(f32)).astype(bf16)
            ended = move(merged, "y", way)
            total = (p_own.astype(f32) + direct.astype(f32) + ended.astype(f32)).astype(bf16)
            back[s] = move(total, "z", -s) if s else total
    experts_out = finish(order, [back[s] for s in range(4)])

    crossed = {0: attended[:quarter]}
    for shift in (1, 2, 3):
        crossed[shift] = move(attended[shift * quarter : (shift + 1) * quarter], "x", shift)
    late = after(out_weight, made[0][0])
    low = move(late, "x", 1)
    high = move(late, "x", -1)
    half = attended.shape[1] // 2
    across = jnp.concatenate((move(low[:half], "x", 1), move(high[half:], "x", -1)), axis=0)
    mixed = jnp.zeros((quarter, out_weight.shape[1]), f32)
    for shift, piece in ((0, out_weight), (1, low), (3, high), (2, across)):
        mixed = mixed + jnp.dot(crossed[shift], piece, preferred_element_type=f32)
    mixer_out = (
        mixed * lax.rsqrt(jnp.mean(mixed * mixed, axis=-1, keepdims=True) + epsilon) * out_gain
    ).astype(bf16)
    return (mixer_out, experts_out)


def solution(mesh):
    split = Mesh(mesh.devices.reshape(4, 4, 2, 4), ("z", "y", "c", "x"))
    ep = ("z", "y", "c")
    placed = (
        P(ep, "x"),
        P(ep, "x"),
        P(ep, "x"),
        P("x"),
        P("x", None),
        P(),
        P(ep + ("x",), None),
        P(ep + ("x",), None),
        P(ep + ("x",), None),
        P(),
        P(ep, None, "x"),
        P(ep, None, "x"),
        P(ep, None, "x"),
    )

    return jax.shard_map(
        local,
        mesh=split,
        in_specs=placed,
        out_specs=(P(ep + ("x",), None), P(ep + ("x",), None)),
        check_vma=False,
    )
```

```python
import jax
import jax.numpy as jnp
from jax import lax
from jax.experimental import pallas as pl
from jax.experimental.pallas import tpu as pltpu
from jax.sharding import Mesh, PartitionSpec as P


HEAD_DIM = 64
WINDOW = 128
CAP = 64
GROUPS = 4
META = 128
SET_BLOCKS = 8

epsilon = 1e-06
f32 = jnp.float32
bf16 = jnp.bfloat16
NT = (((1,), (1,)), ((), ()))
TN = (((0,), (0,)), ((), ()))
VMEM_LIMIT = 60 * 1024 * 1024


def shifted(size, shift):
    return [(i, (i + shift) % size) for i in range(size)]


def iota(shape, dim, kind=jnp.int32):
    return lax.broadcasted_iota(jnp.int32, shape, dim).astype(kind)


def prep_kernel(place, tok, ids_t, weight_t, gain, first, second, third, fourth, order):
    count, width = tok.shape
    each = count // GROUPS
    inputs = tok[...].astype(f32)
    scale = lax.rsqrt(jnp.mean(inputs * inputs, axis=-1, keepdims=True) + epsilon)
    ids = ids_t[...]
    group = lax.shift_right_logical(ids[0:1, :], 3)
    relative = lax.bitwise_and(group - place[0] + GROUPS, GROUPS - 1)
    member = (iota((16, count), 0) == relative).astype(f32)
    before = (iota((count, count), 0) < iota((count, count), 1)).astype(f32).astype(bf16)
    earlier = jnp.dot(member.astype(bf16), before, preferred_element_type=f32)
    rank = jnp.sum(earlier * member, axis=0, keepdims=True)
    slot = (relative * each).astype(f32) + rank
    order[...] = (iota((count, count), 0, f32) == slot).astype(f32).astype(bf16)
    outs = (first, second, third, fourth)
    line = iota((META, count), 0)
    meta = jnp.where(line == 0, ids[0:1, :].astype(f32), 0.0)
    meta = jnp.where(line == 1, ids[1:2, :].astype(f32), meta)
    for k in range(2):
        rest = weight_t[k : k + 1, :]
        for part in range(3):
            piece = rest.astype(bf16).astype(f32)
            meta = jnp.where(line == 2 + 3 * k + part, piece, meta)
            rest = rest - piece
    tags = lax.dot_general(order[...], meta.astype(bf16), NT, preferred_element_type=f32).astype(bf16)
    for index, out in enumerate(outs):
        out[:, width:] = tags[index * each : (index + 1) * each]
    wide = width // 4

    def columns(i, _):
        cols = pl.ds(pl.multiple_of(i * wide, wide), wide)
        normed = (tok[:, cols].astype(f32) * scale * gain[:, cols]).astype(bf16)
        rows = jnp.dot(order[...], normed, preferred_element_type=f32).astype(bf16)
        for index, out in enumerate(outs):
            out[:, cols] = rows[index * each : (index + 1) * each]
        return 0

    lax.fori_loop(0, 4, columns, 0)


def prepare(place, tokens, ids, weights, gain):
    count, width = tokens.shape
    chunk = jax.ShapeDtypeStruct((count // GROUPS, width + META), bf16)
    vmem = pl.BlockSpec(memory_space=pltpu.VMEM)
    return pl.pallas_call(
        prep_kernel,
        out_shape=(chunk, chunk, chunk, chunk, jax.ShapeDtypeStruct((count, count), bf16)),
        in_specs=[pl.BlockSpec(memory_space=pltpu.SMEM)] + [vmem] * 4,
        out_specs=(vmem,) * 5,
        compiler_params=pltpu.CompilerParams(vmem_limit_bytes=VMEM_LIMIT),
        cost_estimate=pl.CostEstimate(flops=6_000_000_000, bytes_accessed=6_000_000, transcendentals=512),
        name="prep",
    )(place, tokens, ids.T, weights.T, gain.reshape(1, width))


def choices(tags, experts):
    blocks = len(tags)
    size = tags[0].shape[0]
    lines = [jnp.transpose(t.astype(f32)) for t in tags]
    hits = [[tuple((t[k : k + 1] == e).astype(f32) for k in range(2)) for t in lines] for e in experts]
    row = iota((2 * blocks, size), 0)
    counts = jnp.zeros((2 * blocks, size), f32)
    for e in range(2):
        for b in range(blocks):
            counts = jnp.where(row == e * blocks + b, hits[e][b][0] + hits[e][b][1], counts)
    before = (iota((size, size), 0) < iota((size, size), 1)).astype(f32).astype(bf16)
    earlier = jnp.dot(counts.astype(bf16), before, preferred_element_type=f32)
    place = iota((2 * CAP, size), 0, f32)
    found = []
    for pair in range(blocks // 2):
        picks = []
        weights = []
        for e in range(2):
            halves = []
            weight = jnp.zeros((2 * CAP, size), f32)
            for j in range(2):
                b = 2 * pair + j
                hit = hits[e][b]
                slot = earlier[e * blocks + b : e * blocks + b + 1] + float(CAP * j)
                one = jnp.where(place == slot, hit[0], 0.0)
                two = jnp.where(place == slot + hit[0], hit[1], 0.0)
                halves.append(one + two)
                t = lines[b]
                weight = weight + one * (t[2:3] + t[3:4] + t[4:5]) + two * (t[5:6] + t[6:7] + t[7:8])
            picks.append(jnp.concatenate(halves, axis=1))
            weights.append(jnp.sum(weight, axis=1, keepdims=True))
        found.append((jnp.concatenate(picks, axis=0).astype(bf16), jnp.concatenate(weights, axis=0)))
    return found


def stage_kernel(place, *refs):
    sources, weights = refs[:8], refs[8:20]
    rows_out, hidden_out, pick_out, scale_out = refs[20:24]
    tok, held, rows, units, pick_v, scale_v, tok_sem, held_sem, out_sem = refs[24:]
    width = rows.shape[-1]
    part, wide = weights[0].shape
    rest = 2 * width - part
    size = tok.shape[1]
    arrivals = []
    for b in range(SET_BLOCKS):
        source = sources[b]
        if source.shape[0] > size:
            source = source.at[pl.ds(b // 4 * size, size)]
        arrivals.append(pltpu.make_async_copy(source, tok.at[b], tok_sem.at[b]))
    fetches = []
    for i in range(6):
        fetches.append(
            (
                pltpu.make_async_copy(weights[2 * i], held.at[i, pl.ds(0, part)], held_sem.at[0, i]),
                pltpu.make_async_copy(
                    weights[2 * i + 1].at[pl.ds(0, rest)], held.at[i, pl.ds(part, rest)], held_sem.at[1, i]
                ),
            )
        )
    for copy in arrivals:
        copy.start()
    for copy in fetches[0]:
        copy.start()
    experts = (place[1].astype(f32), place[2].astype(f32))
    for copy in arrivals:
        copy.wait()
    for pair_of in fetches[1:]:
        for copy in pair_of:
            copy.start()
    for pair, (pick, scale) in enumerate(choices([tok[b, :, width:] for b in range(SET_BLOCKS)], experts)):
        pick_v[pair] = pick
        scale_v[pair] = jnp.broadcast_to(scale, scale_v.shape[1:])
        both = tok[2 * pair : 2 * pair + 2, :, :width].reshape(2 * size, width)
        chosen = jnp.dot(pick, both, preferred_element_type=f32).astype(bf16)
        for e in range(2):
            rows[e, 2 * CAP * pair : 2 * CAP * (pair + 1)] = chosen[2 * CAP * e : 2 * CAP * (e + 1)]
    sent = [
        pltpu.make_async_copy(rows, rows_out, out_sem.at[0]),
        pltpu.make_async_copy(pick_v, pick_out, out_sem.at[1]),
        pltpu.make_async_copy(scale_v, scale_out, out_sem.at[2]),
    ]
    for copy in sent:
        copy.start()

    def one_shard(i, _):
        e = i // 3
        shard = i - 3 * e
        pltpu.make_async_copy(weights[0], held.at[i, pl.ds(0, part)], held_sem.at[0, i]).wait()
        pltpu.make_async_copy(weights[1].at[pl.ds(0, rest)], held.at[i, pl.ds(part, rest)], held_sem.at[1, i]).wait()
        gate = jnp.dot(rows[e], held[i, :width], preferred_element_type=f32)
        up = jnp.dot(rows[e], held[i, width:], preferred_element_type=f32)
        columns = pl.ds(pl.multiple_of(shard * wide, wide), wide)
        units[e, :, columns] = (gate / (1.0 + jnp.exp(-gate)) * up).astype(bf16)
        return 0

    lax.fori_loop(0, 6, one_shard, 0)
    sent.append(pltpu.make_async_copy(units, hidden_out, out_sem.at[3]))
    sent[-1].start()
    for copy in sent:
        copy.wait()


def stage(place, blocks, weights):
    size = min(b.shape[0] for b in blocks)
    size = size if size < 256 else size // 2
    full = blocks[0].shape[1]
    width = full - META
    wide = weights[0].shape[1]
    rows = SET_BLOCKS * CAP
    shapes = (
        ((2, rows, width), bf16),
        ((2, rows, 3 * wide), bf16),
        ((SET_BLOCKS // 2, 4 * CAP, 2 * size), bf16),
        ((SET_BLOCKS // 2, 4 * CAP, 128), f32),
    )
    held = pl.BlockSpec(memory_space=pltpu.HBM)
    return pl.pallas_call(
        stage_kernel,
        out_shape=tuple(jax.ShapeDtypeStruct(*s) for s in shapes),
        in_specs=[pl.BlockSpec(memory_space=pltpu.SMEM)] + [held] * 20,
        out_specs=(held,) * 4,
        scratch_shapes=[
            pltpu.VMEM((SET_BLOCKS, size, full), bf16),
            pltpu.VMEM((6, 2 * width, wide), bf16),
        ]
        + [pltpu.VMEM(*s) for s in shapes]
        + [
            pltpu.SemaphoreType.DMA((SET_BLOCKS,)),
            pltpu.SemaphoreType.DMA((2, 6)),
            pltpu.SemaphoreType.DMA((4,)),
        ],
        compiler_params=pltpu.CompilerParams(vmem_limit_bytes=VMEM_LIMIT),
        cost_estimate=pl.CostEstimate(flops=10_000_000_000, bytes_accessed=24_000_000, transcendentals=0),
    )(place, *blocks, *weights)


def result_kernel(halves, *refs):
    staged, far, downs = (refs[:4], refs[4:8]), refs[8:12], refs[12:18]
    outs = refs[18:26]
    rows, units, pick_v, scale_v, held, down_v, made, spread_v, sem, out_sem = refs[26:]
    width = rows.shape[-1]
    part, wide = far[0].shape
    rest = 2 * width - part
    each = rows.shape[1] // 2
    first, second = [], []
    for e in range(2):
        for j in range(2):
            source = staged[j][0].at[e, pl.ds(halves[j] * each, each)]
            first.append(pltpu.make_async_copy(source, rows.at[e, pl.ds(j * each, each)], sem.at[4 * e + j]))
        first.append(pltpu.make_async_copy(far[2 * e], held.at[e, pl.ds(0, part)], sem.at[4 * e + 2]))
        first.append(pltpu.make_async_copy(far[2 * e + 1].at[pl.ds(0, rest)], held.at[e, pl.ds(part, rest)], sem.at[4 * e + 3]))
    for e in range(2):
        for j in range(2):
            source = staged[j][1].at[e, pl.ds(halves[j] * each, each)]
            target = units.at[e, pl.ds(j * each, each), pl.ds(0, 3 * wide)]
            second.append(pltpu.make_async_copy(source, target, sem.at[8 + 6 * e + j]))
        for shard in range(4):
            source = (far[2 * e + 1] if shard == 3 else downs[3 * e + shard]).at[pl.ds(rest, width)]
            target = down_v.at[e, :, pl.ds(shard * wide, wide)]
            second.append(pltpu.make_async_copy(source, target, sem.at[10 + 6 * e + shard]))
    third = []
    for j in range(2):
        pairs, place = pl.ds(2 * halves[j], 2), pl.ds(2 * j, 2)
        third.append(pltpu.make_async_copy(staged[j][2].at[pairs], pick_v.at[place], sem.at[20 + j]))
        third.append(pltpu.make_async_copy(staged[j][3].at[pairs], scale_v.at[place], sem.at[22 + j]))
    stages = [first[:4], first[4:], second[:6], second[6:] + third]

    def begin(group):
        for copy in stages[group]:
            copy.start()

    def arrive(group):
        for copy in stages[group]:
            copy.wait()

    def far_units(e):
        gate = jnp.dot(rows[e], held[e, :width], preferred_element_type=f32)
        up = jnp.dot(rows[e], held[e, width:], preferred_element_type=f32)
        units[e, :, 3 * wide :] = (gate / (1.0 + jnp.exp(-gate)) * up).astype(bf16)

    quarter = width // 4

    def project(e, cols):
        return lax.dot_general(units[e], down_v[e, cols, :], NT, preferred_element_type=f32).astype(bf16)

    begin(0)
    begin(1)
    arrive(0)
    begin(2)

    def both(e, _):
        @pl.when(e == 1)
        def _():
            arrive(1)
            begin(3)

        far_units(e)
        return 0

    lax.fori_loop(0, 2, both, 0)
    arrive(2)

    def first_expert(i, _):
        cols = pl.ds(pl.multiple_of(i * quarter, quarter), quarter)
        made[:, cols] = project(0, cols)
        return 0

    lax.fori_loop(0, 4, first_expert, 0)
    arrive(3)
    size = outs[0].shape[0]

    def leave(i, b):
        cols = pl.ds(pl.multiple_of(i * quarter, quarter), quarter)
        return pltpu.make_async_copy(spread_v.at[b, :, cols], outs[b].at[:, cols], out_sem.at[i, b])

    def columns(i, _):
        cols = pl.ds(pl.multiple_of(i * quarter, quarter), quarter)
        other = project(1, cols)
        for pair in range(SET_BLOCKS // 2):
            lines = slice(2 * CAP * pair, 2 * CAP * (pair + 1))
            result = jnp.concatenate([made[lines, cols], other[lines]], axis=0).astype(f32)
            scaled = (result * scale_v[pair, :, 0:1]).astype(bf16)
            spread = lax.dot_general(pick_v[pair], scaled, TN, preferred_element_type=f32).astype(bf16)
            spread_v[2 * pair, :, cols] = spread[:size]
            spread_v[2 * pair + 1, :, cols] = spread[size:]
        for b in range(SET_BLOCKS):
            leave(i, b).start()
        return 0

    lax.fori_loop(0, 4, columns, 0)

    def settle(i, _):
        for b in range(SET_BLOCKS):
            leave(i, b).wait()
        return 0

    lax.fori_loop(0, 4, settle, 0)


def results(staged, halves, far, downs, size):
    rows, _, picks, scales = staged[0]
    width = rows.shape[-1]
    wide = far[0].shape[1]
    held = pl.BlockSpec(memory_space=pltpu.HBM)
    vmem = pl.BlockSpec(memory_space=pltpu.VMEM)
    return pl.pallas_call(
        lambda *refs: result_kernel(halves, *refs),
        out_shape=(jax.ShapeDtypeStruct((size, width), bf16),) * SET_BLOCKS,
        in_specs=[held] * 18,
        out_specs=(held,) * SET_BLOCKS,
        scratch_shapes=[
            pltpu.VMEM(rows.shape, bf16),
            pltpu.VMEM((2, rows.shape[1], 4 * wide), bf16),
            pltpu.VMEM(picks.shape, bf16),
            pltpu.VMEM(scales.shape, f32),
            pltpu.VMEM((2, 2 * width, wide), bf16),
            pltpu.VMEM((2, width, 4 * wide), bf16),
            pltpu.VMEM(rows.shape[1:], bf16),
            pltpu.VMEM((SET_BLOCKS, size, width), bf16),
            pltpu.SemaphoreType.DMA((24,)),
            pltpu.SemaphoreType.DMA((4, SET_BLOCKS)),
        ],
        compiler_params=pltpu.CompilerParams(vmem_limit_bytes=VMEM_LIMIT),
        cost_estimate=pl.CostEstimate(flops=8_000_000_000, bytes_accessed=24_000_000, transcendentals=0),
    )(*staged[0], *staged[1], *far, *downs)


def finish_kernel(order, first, second, third, fourth, out):
    _, width = first.shape
    wide = width // 4

    def columns(i, _):
        cols = pl.ds(pl.multiple_of(i * wide, wide), wide)
        rows = jnp.concatenate([piece[:, cols] for piece in (first, second, third, fourth)], axis=0)
        out[:, cols] = lax.dot_general(order[...], rows, TN, preferred_element_type=f32).astype(bf16)
        return 0

    lax.fori_loop(0, 4, columns, 0)


def finish(order, pieces):
    count = order.shape[0]
    width = pieces[0].shape[1]
    vmem = pl.BlockSpec(memory_space=pltpu.VMEM)
    return pl.pallas_call(
        finish_kernel,
        out_shape=jax.ShapeDtypeStruct((count, width), bf16),
        in_specs=[vmem] * 5,
        out_specs=vmem,
        compiler_params=pltpu.CompilerParams(vmem_limit_bytes=VMEM_LIMIT),
        cost_estimate=pl.CostEstimate(flops=2_000_000_000, bytes_accessed=5_000_000, transcendentals=0),
        name="finish",
    )(order, *pieces)


def padded(block, width):
    axes = ("z", "y", "c")
    count = 1
    for axis in axes:
        count *= lax.axis_size(axis)
    forward = [(i, i + 1) for i in range(count - 1)]
    backward = [(target, source) for source, target in forward]
    low = lax.ppermute(block[-width:], axes, forward)
    high = lax.ppermute(block[:width], axes, backward)
    return jnp.concatenate([low, block, high], axis=0)


def attention_kernel(bounds, sinks, queries, extended, out):
    heads = queries.shape[1] // HEAD_DIM
    total = bounds[1]
    span = 3 * WINDOW
    lines = heads * WINDOW
    row = iota((lines, span), 0)
    col = iota((lines, span), 1)
    away = col - lax.bitwise_and(row, WINDOW - 1)
    near = (away >= 0) & (away <= 2 * WINDOW)
    head = lax.shift_right_logical(iota((lines, 1), 0), 7)
    sink = jnp.zeros((lines, 1), f32)
    for h in range(heads):
        sink = jnp.where(head == h, sinks[h], sink)

    blocks = queries.shape[0] // WINDOW

    def one_block(index, _):
        block = lax.bitwise_and(index + bounds[2], blocks - 1)
        start = pl.multiple_of(block * WINDOW, WINDOW)
        asked = queries[pl.ds(start, WINDOW), :]
        stacked = jnp.concatenate([asked[:, h * HEAD_DIM : (h + 1) * HEAD_DIM] for h in range(heads)], axis=0)
        band = extended[pl.ds(start, span), :]
        keys, held = band[:, :HEAD_DIM], band[:, HEAD_DIM:]
        scores = lax.dot_general(stacked, keys, NT, preferred_element_type=f32) * HEAD_DIM ** (-0.5)
        place = bounds[0] + start - WINDOW + col
        masked = jnp.where(near & (place >= 0) & (place < total), scores, -1e30)
        largest = jnp.maximum(jnp.max(masked, axis=-1, keepdims=True), sink)
        raised = jnp.exp(masked - largest)
        denominator = jnp.sum(raised, axis=-1, keepdims=True) + jnp.exp(sink - largest)
        weights = (raised * (1.0 / denominator)).astype(bf16)
        made = jnp.dot(weights, held, preferred_element_type=f32).astype(bf16)
        pieces = [made[h * WINDOW : (h + 1) * WINDOW] for h in range(heads)]
        out[pl.ds(pl.multiple_of(index * WINDOW, WINDOW), WINDOW), :] = jnp.concatenate(pieces, axis=1)
        return 0

    lax.fori_loop(0, blocks, one_block, 0)


def attention(queries, extended, sink_logit, offset, seq_total, turn):
    smem = pl.BlockSpec(memory_space=pltpu.SMEM)
    vmem = pl.BlockSpec(memory_space=pltpu.VMEM)
    bounds = jnp.stack([offset, jnp.int32(seq_total), turn]).astype(jnp.int32)
    return pl.pallas_call(
        attention_kernel,
        out_shape=jax.ShapeDtypeStruct(queries.shape, bf16),
        in_specs=[smem, smem, vmem, vmem],
        out_specs=vmem,
        compiler_params=pltpu.CompilerParams(vmem_limit_bytes=VMEM_LIMIT // 2),
        cost_estimate=pl.CostEstimate(flops=6_000_000_000, bytes_accessed=1_500_000, transcendentals=1_600_000),
        name="attention",
    )(bounds, sink_logit, queries, extended)


def move(value, axis, shift):
    return lax.ppermute(value, axis, shifted(lax.axis_size(axis), shift))


def after(value, *others):
    return lax.optimization_barrier((value,) + others)[0]


def local(
    queries,
    key_rows,
    values,
    sink_logit,
    out_weight,
    out_gain,
    routed_tokens,
    expert_ids,
    route_weight,
    routed_gain,
    expert_gate,
    expert_up,
    expert_down,
):
    row_count = queries.shape[0]
    z, y, c, x = (lax.axis_index(axis) for axis in ("z", "y", "c", "x"))
    expert = (z * 4 + y) * 2 + c
    place = jnp.stack([z, expert, expert + 1 - 2 * c]).astype(jnp.int32)

    split = expert_up.shape[1] // 2
    part_a = jnp.concatenate((expert_gate[0], expert_up[0, :split]), axis=0)
    part_b = jnp.concatenate((expert_up[0, split:], expert_down[0]), axis=0)
    low_a = move(part_a, "x", 1)
    high_b = move(part_b, "x", -1)
    low_b = move(part_b, "x", 1)
    high_a = move(part_a, "x", -1)
    far_a = move(low_a, "x", 1)
    far_b = move(high_b, "x", -1)
    mine = (part_a, part_b, low_a, low_b, high_a, high_b, far_a, far_b)
    prepared = prepare(place, routed_tokens, expert_ids, route_weight, routed_gain)
    own, order = prepared[0], prepared[4]
    size = own.shape[0]
    out = {s: move(prepared[s], "z", s) for s in (1, 3, 2)}
    joined = jnp.concatenate((out[1], out[3]), axis=0)
    groups = {"0": own, "13": joined, "2": out[2]}
    blocks = {}
    for name, chunk in groups.items():
        near_low = move(chunk, "y", 1)
        near_high = move(chunk, "y", -1)
        beyond = move(near_low, "y", 1) if name == "13" else move(near_high, "y", -1)
        blocks[name] = (chunk, near_low, near_high, beyond)

    extended = padded(jnp.concatenate((key_rows, values), axis=1), WINDOW)
    attended = attention(queries, extended, sink_logit, expert * row_count, row_count * 32, 2 * x)
    quarter = row_count // 4
    theirs = tuple(move(v, "c", 1) for v in mine)

    staged_a = stage(place, blocks["13"] * 2, mine[:6] + theirs[:6])
    staged_b = stage(place, blocks["0"] + blocks["2"], mine[:6] + theirs[:6])

    far = mine[6:] + theirs[6:]
    downs = mine[1:6:2] + theirs[1:6:2]
    sets = ((2, 3), (1, 0))
    made = []
    for which, halves in enumerate(((1, 1), (0, 0))):
        parts = (staged_b, staged_a) if which == 0 else (staged_a, staged_b)
        made.append(results(parts, halves, far, downs, size))
    crossed = {0: attended[:quarter]}
    for shift in (1, 2, 3):
        crossed[shift] = move(attended[shift * quarter : (shift + 1) * quarter], "x", shift)
    late = after(out_weight, made[0][0])
    low = move(late, "x", 1)
    high = move(late, "x", -1)
    half = attended.shape[1] // 2
    across = jnp.concatenate((move(low[:half], "x", 1), move(high[half:], "x", -1)), axis=0)
    mixed = jnp.zeros((quarter, out_weight.shape[1]), f32)
    for shift, piece in ((0, out_weight), (1, low), (3, high), (2, across)):
        mixed = mixed + jnp.dot(crossed[shift], piece, preferred_element_type=f32)
    mixer_out = (
        mixed * lax.rsqrt(jnp.mean(mixed * mixed, axis=-1, keepdims=True) + epsilon) * out_gain
    ).astype(bf16)
    back = {}
    for which, pair in enumerate(sets):
        for index, s in enumerate(pair):
            way = 1 if index == 0 else -1
            p_own, p_low, p_high, p_far = made[which][4 * index : 4 * index + 4]
            straight, through = (p_low, p_high) if way == 1 else (p_high, p_low)
            began = move(p_far, "y", way)
            direct = move(straight, "y", -way)
            merged = (began.astype(f32) + through.astype(f32)).astype(bf16)
            ended = move(merged, "y", way)
            if s == 0:
                p_own = after(p_own, mixer_out)
            total = (p_own.astype(f32) + direct.astype(f32) + ended.astype(f32)).astype(bf16)
            back[s] = move(total, "z", -s) if s else total
    experts_out = finish(order, [back[s] for s in range(4)])

    return (mixer_out, experts_out)


def solution(mesh):
    split = Mesh(mesh.devices.reshape(4, 4, 2, 4), ("z", "y", "c", "x"))
    ep = ("z", "y", "c")
    placed = (
        P(ep, "x"),
        P(ep, "x"),
        P(ep, "x"),
        P("x"),
        P("x", None),
        P(),
        P(ep + ("x",), None),
        P(ep + ("x",), None),
        P(ep + ("x",), None),
        P(),
        P(ep, None, "x"),
        P(ep, None, "x"),
        P(ep, None, "x"),
    )

    return jax.shard_map(
        local,
        mesh=split,
        in_specs=placed,
        out_specs=(P(ep + ("x",), None), P(ep + ("x",), None)),
        check_vma=False,
    )
```

```python
import jax
import jax.numpy as jnp
from jax import lax
from jax.experimental import pallas as pl
from jax.experimental.pallas import tpu as pltpu
from jax.sharding import Mesh, PartitionSpec as P


HEAD_DIM = 64
WINDOW = 128
CAP = 64
GROUPS = 4
META = 128
SET_BLOCKS = 8

epsilon = 1e-06
f32 = jnp.float32
bf16 = jnp.bfloat16
NT = (((1,), (1,)), ((), ()))
TN = (((0,), (0,)), ((), ()))
VMEM_LIMIT = 60 * 1024 * 1024


def shifted(size, shift):
    return [(i, (i + shift) % size) for i in range(size)]


def iota(shape, dim, kind=jnp.int32):
    return lax.broadcasted_iota(jnp.int32, shape, dim).astype(kind)


def prep_kernel(place, tok, ids_t, weight_t, gain, first, second, third, fourth, order):
    count, width = tok.shape
    each = count // GROUPS
    inputs = tok[...].astype(f32)
    scale = lax.rsqrt(jnp.mean(inputs * inputs, axis=-1, keepdims=True) + epsilon)
    ids = ids_t[...]
    group = lax.shift_right_logical(ids[0:1, :], 3)
    relative = lax.bitwise_and(group - place[0] + GROUPS, GROUPS - 1)
    member = (iota((16, count), 0) == relative).astype(f32)
    before = (iota((count, count), 0) < iota((count, count), 1)).astype(f32).astype(bf16)
    earlier = jnp.dot(member.astype(bf16), before, preferred_element_type=f32)
    rank = jnp.sum(earlier * member, axis=0, keepdims=True)
    slot = (relative * each).astype(f32) + rank
    order[...] = (iota((count, count), 0, f32) == slot).astype(f32).astype(bf16)
    outs = (first, second, third, fourth)
    line = iota((META, count), 0)
    meta = jnp.where(line == 0, ids[0:1, :].astype(f32), 0.0)
    meta = jnp.where(line == 1, ids[1:2, :].astype(f32), meta)
    for k in range(2):
        rest = weight_t[k : k + 1, :]
        for part in range(3):
            piece = rest.astype(bf16).astype(f32)
            meta = jnp.where(line == 2 + 3 * k + part, piece, meta)
            rest = rest - piece
    tags = lax.dot_general(order[...], meta.astype(bf16), NT, preferred_element_type=f32).astype(bf16)
    for index, out in enumerate(outs):
        out[:, width:] = tags[index * each : (index + 1) * each]
    wide = width // 4

    def columns(i, _):
        cols = pl.ds(pl.multiple_of(i * wide, wide), wide)
        normed = (tok[:, cols].astype(f32) * scale * gain[:, cols]).astype(bf16)
        rows = jnp.dot(order[...], normed, preferred_element_type=f32).astype(bf16)
        for index, out in enumerate(outs):
            out[:, cols] = rows[index * each : (index + 1) * each]
        return 0

    lax.fori_loop(0, 4, columns, 0)


def prepare(place, tokens, ids, weights, gain):
    count, width = tokens.shape
    chunk = jax.ShapeDtypeStruct((count // GROUPS, width + META), bf16)
    vmem = pl.BlockSpec(memory_space=pltpu.VMEM)
    return pl.pallas_call(
        prep_kernel,
        out_shape=(chunk, chunk, chunk, chunk, jax.ShapeDtypeStruct((count, count), bf16)),
        in_specs=[pl.BlockSpec(memory_space=pltpu.SMEM)] + [vmem] * 4,
        out_specs=(vmem,) * 5,
        compiler_params=pltpu.CompilerParams(vmem_limit_bytes=VMEM_LIMIT),
        cost_estimate=pl.CostEstimate(flops=6_000_000_000, bytes_accessed=6_000_000, transcendentals=512),
        name="prep",
    )(place, tokens, ids.T, weights.T, gain.reshape(1, width))


def choices(tags, experts):
    blocks = len(tags)
    size = tags[0].shape[0]
    lines = [jnp.transpose(t.astype(f32)) for t in tags]
    hits = [[tuple((t[k : k + 1] == e).astype(f32) for k in range(2)) for t in lines] for e in experts]
    row = iota((2 * blocks, size), 0)
    counts = jnp.zeros((2 * blocks, size), f32)
    for e in range(2):
        for b in range(blocks):
            counts = jnp.where(row == e * blocks + b, hits[e][b][0] + hits[e][b][1], counts)
    before = (iota((size, size), 0) < iota((size, size), 1)).astype(f32).astype(bf16)
    earlier = jnp.dot(counts.astype(bf16), before, preferred_element_type=f32)
    place = iota((2 * CAP, size), 0, f32)
    found = []
    for pair in range(blocks // 2):
        picks = []
        weights = []
        for e in range(2):
            halves = []
            weight = jnp.zeros((2 * CAP, size), f32)
            for j in range(2):
                b = 2 * pair + j
                hit = hits[e][b]
                slot = earlier[e * blocks + b : e * blocks + b + 1] + float(CAP * j)
                one = jnp.where(place == slot, hit[0], 0.0)
                two = jnp.where(place == slot + hit[0], hit[1], 0.0)
                halves.append(one + two)
                t = lines[b]
                weight = weight + one * (t[2:3] + t[3:4] + t[4:5]) + two * (t[5:6] + t[6:7] + t[7:8])
            picks.append(jnp.concatenate(halves, axis=1))
            weights.append(jnp.sum(weight, axis=1, keepdims=True))
        found.append((jnp.concatenate(picks, axis=0).astype(bf16), jnp.concatenate(weights, axis=0)))
    return found


def stage_kernel(place, *refs):
    sources, weights = refs[:8], refs[8:20]
    rows_out, hidden_out, pick_out, scale_out = refs[20:24]
    tok, held, rows, units, pick_v, scale_v, tok_sem, held_sem, out_sem = refs[24:]
    width = rows.shape[-1]
    part, wide = weights[0].shape
    rest = 2 * width - part
    size = tok.shape[1]
    arrivals = []
    for b in range(SET_BLOCKS):
        source = sources[b]
        if source.shape[0] > size:
            source = source.at[pl.ds(b // 4 * size, size)]
        arrivals.append(pltpu.make_async_copy(source, tok.at[b], tok_sem.at[b]))
    fetches = []
    for i in range(6):
        fetches.append(
            (
                pltpu.make_async_copy(weights[2 * i], held.at[i, pl.ds(0, part)], held_sem.at[0, i]),
                pltpu.make_async_copy(
                    weights[2 * i + 1].at[pl.ds(0, rest)], held.at[i, pl.ds(part, rest)], held_sem.at[1, i]
                ),
            )
        )
    for copy in arrivals:
        copy.start()
    for copy in fetches[0]:
        copy.start()
    experts = (place[1].astype(f32), place[2].astype(f32))
    for copy in arrivals:
        copy.wait()
    for pair_of in fetches[1:]:
        for copy in pair_of:
            copy.start()
    for pair, (pick, scale) in enumerate(choices([tok[b, :, width:] for b in range(SET_BLOCKS)], experts)):
        pick_v[pair] = pick
        scale_v[pair] = jnp.broadcast_to(scale, scale_v.shape[1:])
        both = tok[2 * pair : 2 * pair + 2, :, :width].reshape(2 * size, width)
        chosen = jnp.dot(pick, both, preferred_element_type=f32).astype(bf16)
        for e in range(2):
            rows[e, 2 * CAP * pair : 2 * CAP * (pair + 1)] = chosen[2 * CAP * e : 2 * CAP * (e + 1)]
    sent = [
        pltpu.make_async_copy(rows, rows_out, out_sem.at[0]),
        pltpu.make_async_copy(pick_v, pick_out, out_sem.at[1]),
        pltpu.make_async_copy(scale_v, scale_out, out_sem.at[2]),
    ]
    for copy in sent:
        copy.start()

    def one_shard(i, _):
        e = i // 3
        shard = i - 3 * e
        pltpu.make_async_copy(weights[0], held.at[i, pl.ds(0, part)], held_sem.at[0, i]).wait()
        pltpu.make_async_copy(weights[1].at[pl.ds(0, rest)], held.at[i, pl.ds(part, rest)], held_sem.at[1, i]).wait()
        gate = jnp.dot(rows[e], held[i, :width], preferred_element_type=f32)
        up = jnp.dot(rows[e], held[i, width:], preferred_element_type=f32)
        columns = pl.ds(pl.multiple_of(shard * wide, wide), wide)
        units[e, :, columns] = (gate / (1.0 + jnp.exp(-gate)) * up).astype(bf16)
        return 0

    lax.fori_loop(0, 6, one_shard, 0)
    sent.append(pltpu.make_async_copy(units, hidden_out, out_sem.at[3]))
    sent[-1].start()
    for copy in sent:
        copy.wait()


def stage(place, blocks, weights):
    size = min(b.shape[0] for b in blocks)
    size = size if size < 256 else size // 2
    full = blocks[0].shape[1]
    width = full - META
    wide = weights[0].shape[1]
    rows = SET_BLOCKS * CAP
    shapes = (
        ((2, rows, width), bf16),
        ((2, rows, 3 * wide), bf16),
        ((SET_BLOCKS // 2, 4 * CAP, 2 * size), bf16),
        ((SET_BLOCKS // 2, 4 * CAP, 128), f32),
    )
    held = pl.BlockSpec(memory_space=pltpu.HBM)
    return pl.pallas_call(
        stage_kernel,
        out_shape=tuple(jax.ShapeDtypeStruct(*s) for s in shapes),
        in_specs=[pl.BlockSpec(memory_space=pltpu.SMEM)] + [held] * 20,
        out_specs=(held,) * 4,
        scratch_shapes=[
            pltpu.VMEM((SET_BLOCKS, size, full), bf16),
            pltpu.VMEM((6, 2 * width, wide), bf16),
        ]
        + [pltpu.VMEM(*s) for s in shapes]
        + [
            pltpu.SemaphoreType.DMA((SET_BLOCKS,)),
            pltpu.SemaphoreType.DMA((2, 6)),
            pltpu.SemaphoreType.DMA((4,)),
        ],
        compiler_params=pltpu.CompilerParams(vmem_limit_bytes=VMEM_LIMIT),
        cost_estimate=pl.CostEstimate(flops=10_000_000_000, bytes_accessed=24_000_000, transcendentals=0),
    )(place, *blocks, *weights)


def result_kernel(halves, *refs):
    staged, far, downs = (refs[:4], refs[4:8]), refs[8:12], refs[12:18]
    outs = refs[18:26]
    rows, units, pick_v, scale_v, held, down_v, made, spread_v, sem, out_sem = refs[26:]
    width = rows.shape[-1]
    part, wide = far[0].shape
    rest = 2 * width - part
    each = rows.shape[1] // 2
    first, second = [], []
    for e in range(2):
        for j in range(2):
            source = staged[j][0].at[e, pl.ds(halves[j] * each, each)]
            first.append(pltpu.make_async_copy(source, rows.at[e, pl.ds(j * each, each)], sem.at[4 * e + j]))
        first.append(pltpu.make_async_copy(far[2 * e], held.at[e, pl.ds(0, part)], sem.at[4 * e + 2]))
        first.append(pltpu.make_async_copy(far[2 * e + 1].at[pl.ds(0, rest)], held.at[e, pl.ds(part, rest)], sem.at[4 * e + 3]))
    for e in range(2):
        for j in range(2):
            source = staged[j][1].at[e, pl.ds(halves[j] * each, each)]
            target = units.at[e, pl.ds(j * each, each), pl.ds(0, 3 * wide)]
            second.append(pltpu.make_async_copy(source, target, sem.at[8 + 6 * e + j]))
        for shard in range(4):
            source = (far[2 * e + 1] if shard == 3 else downs[3 * e + shard]).at[pl.ds(rest, width)]
            target = down_v.at[e, :, pl.ds(shard * wide, wide)]
            second.append(pltpu.make_async_copy(source, target, sem.at[10 + 6 * e + shard]))
    third = []
    for j in range(2):
        pairs, place = pl.ds(2 * halves[j], 2), pl.ds(2 * j, 2)
        third.append(pltpu.make_async_copy(staged[j][2].at[pairs], pick_v.at[place], sem.at[20 + j]))
        third.append(pltpu.make_async_copy(staged[j][3].at[pairs], scale_v.at[place], sem.at[22 + j]))
    stages = [first[:4], first[4:], second[:6], second[6:] + third]

    def begin(group):
        for copy in stages[group]:
            copy.start()

    def arrive(group):
        for copy in stages[group]:
            copy.wait()

    def far_units(e):
        gate = jnp.dot(rows[e], held[e, :width], preferred_element_type=f32)
        up = jnp.dot(rows[e], held[e, width:], preferred_element_type=f32)
        units[e, :, 3 * wide :] = (gate / (1.0 + jnp.exp(-gate)) * up).astype(bf16)

    quarter = width // 4

    def project(e, cols):
        return lax.dot_general(units[e], down_v[e, cols, :], NT, preferred_element_type=f32).astype(bf16)

    begin(0)
    begin(1)
    arrive(0)
    begin(2)

    def both(e, _):
        @pl.when(e == 1)
        def _():
            arrive(1)
            begin(3)

        far_units(e)
        return 0

    lax.fori_loop(0, 2, both, 0)
    arrive(2)

    def first_expert(i, _):
        cols = pl.ds(pl.multiple_of(i * quarter, quarter), quarter)
        made[:, cols] = project(0, cols)
        return 0

    lax.fori_loop(0, 4, first_expert, 0)
    arrive(3)
    size = outs[0].shape[0]

    def leave(i, b):
        cols = pl.ds(pl.multiple_of(i * quarter, quarter), quarter)
        return pltpu.make_async_copy(spread_v.at[b, :, cols], outs[b].at[:, cols], out_sem.at[i, b])

    def columns(i, _):
        cols = pl.ds(pl.multiple_of(i * quarter, quarter), quarter)
        other = project(1, cols)
        for pair in range(SET_BLOCKS // 2):
            lines = slice(2 * CAP * pair, 2 * CAP * (pair + 1))
            result = jnp.concatenate([made[lines, cols], other[lines]], axis=0).astype(f32)
            scaled = (result * scale_v[pair, :, 0:1]).astype(bf16)
            spread = lax.dot_general(pick_v[pair], scaled, TN, preferred_element_type=f32).astype(bf16)
            spread_v[2 * pair, :, cols] = spread[:size]
            spread_v[2 * pair + 1, :, cols] = spread[size:]
        for b in range(SET_BLOCKS):
            leave(i, b).start()
        return 0

    lax.fori_loop(0, 4, columns, 0)

    def settle(i, _):
        for b in range(SET_BLOCKS):
            leave(i, b).wait()
        return 0

    lax.fori_loop(0, 4, settle, 0)


def results(staged, halves, far, downs, size):
    rows, _, picks, scales = staged[0]
    width = rows.shape[-1]
    wide = far[0].shape[1]
    held = pl.BlockSpec(memory_space=pltpu.HBM)
    vmem = pl.BlockSpec(memory_space=pltpu.VMEM)
    return pl.pallas_call(
        lambda *refs: result_kernel(halves, *refs),
        out_shape=(jax.ShapeDtypeStruct((size, width), bf16),) * SET_BLOCKS,
        in_specs=[held] * 18,
        out_specs=(held,) * SET_BLOCKS,
        scratch_shapes=[
            pltpu.VMEM(rows.shape, bf16),
            pltpu.VMEM((2, rows.shape[1], 4 * wide), bf16),
            pltpu.VMEM(picks.shape, bf16),
            pltpu.VMEM(scales.shape, f32),
            pltpu.VMEM((2, 2 * width, wide), bf16),
            pltpu.VMEM((2, width, 4 * wide), bf16),
            pltpu.VMEM(rows.shape[1:], bf16),
            pltpu.VMEM((SET_BLOCKS, size, width), bf16),
            pltpu.SemaphoreType.DMA((24,)),
            pltpu.SemaphoreType.DMA((4, SET_BLOCKS)),
        ],
        compiler_params=pltpu.CompilerParams(vmem_limit_bytes=VMEM_LIMIT),
        cost_estimate=pl.CostEstimate(flops=8_000_000_000, bytes_accessed=24_000_000, transcendentals=0),
    )(*staged[0], *staged[1], *far, *downs)


def turn_kernel(order, out):
    out[...] = jnp.transpose(order[...].astype(f32)).astype(bf16)


def turn(order):
    vmem = pl.BlockSpec(memory_space=pltpu.VMEM)
    return pl.pallas_call(
        turn_kernel,
        out_shape=jax.ShapeDtypeStruct(order.shape, bf16),
        in_specs=[vmem],
        out_specs=vmem,
        compiler_params=pltpu.CompilerParams(vmem_limit_bytes=VMEM_LIMIT // 2),
        cost_estimate=pl.CostEstimate(flops=1_000_000_000, bytes_accessed=1_000_000, transcendentals=0),
        name="turn",
    )(order)


def finish_kernel(order, first, second, third, fourth, out):
    _, width = first.shape
    wide = width // 4

    def columns(i, _):
        cols = pl.ds(pl.multiple_of(i * wide, wide), wide)
        rows = jnp.concatenate([piece[:, cols] for piece in (first, second, third, fourth)], axis=0)
        out[:, cols] = jnp.dot(order[...], rows, preferred_element_type=f32).astype(bf16)
        return 0

    lax.fori_loop(0, 4, columns, 0)


def finish(order, pieces):
    count = order.shape[0]
    width = pieces[0].shape[1]
    vmem = pl.BlockSpec(memory_space=pltpu.VMEM)
    return pl.pallas_call(
        finish_kernel,
        out_shape=jax.ShapeDtypeStruct((count, width), bf16),
        in_specs=[vmem] * 5,
        out_specs=vmem,
        compiler_params=pltpu.CompilerParams(vmem_limit_bytes=VMEM_LIMIT),
        cost_estimate=pl.CostEstimate(flops=2_000_000_000, bytes_accessed=5_000_000, transcendentals=0),
        name="finish",
    )(order, *pieces)


def padded(block, width):
    axes = ("z", "y", "c")
    count = 1
    for axis in axes:
        count *= lax.axis_size(axis)
    forward = [(i, i + 1) for i in range(count - 1)]
    backward = [(target, source) for source, target in forward]
    low = lax.ppermute(block[-width:], axes, forward)
    high = lax.ppermute(block[:width], axes, backward)
    return jnp.concatenate([low, block, high], axis=0)


def attention_kernel(bounds, sinks, queries, extended, out):
    heads = queries.shape[1] // HEAD_DIM
    total = bounds[1]
    span = 3 * WINDOW
    lines = heads * WINDOW
    row = iota((lines, span), 0)
    col = iota((lines, span), 1)
    away = col - lax.bitwise_and(row, WINDOW - 1)
    near = (away >= 0) & (away <= 2 * WINDOW)
    head = lax.shift_right_logical(iota((lines, 1), 0), 7)
    sink = jnp.zeros((lines, 1), f32)
    for h in range(heads):
        sink = jnp.where(head == h, sinks[h], sink)

    blocks = queries.shape[0] // WINDOW

    def one_block(index, _):
        block = lax.bitwise_and(index + bounds[2], blocks - 1)
        start = pl.multiple_of(block * WINDOW, WINDOW)
        asked = queries[pl.ds(start, WINDOW), :]
        stacked = jnp.concatenate([asked[:, h * HEAD_DIM : (h + 1) * HEAD_DIM] for h in range(heads)], axis=0)
        band = extended[pl.ds(start, span), :]
        keys, held = band[:, :HEAD_DIM], band[:, HEAD_DIM:]
        scores = lax.dot_general(stacked, keys, NT, preferred_element_type=f32) * HEAD_DIM ** (-0.5)
        place = bounds[0] + start - WINDOW + col
        masked = jnp.where(near & (place >= 0) & (place < total), scores, -1e30)
        largest = jnp.maximum(jnp.max(masked, axis=-1, keepdims=True), sink)
        raised = jnp.exp(masked - largest)
        denominator = jnp.sum(raised, axis=-1, keepdims=True) + jnp.exp(sink - largest)
        weights = (raised * (1.0 / denominator)).astype(bf16)
        made = jnp.dot(weights, held, preferred_element_type=f32).astype(bf16)
        pieces = [made[h * WINDOW : (h + 1) * WINDOW] for h in range(heads)]
        out[pl.ds(pl.multiple_of(index * WINDOW, WINDOW), WINDOW), :] = jnp.concatenate(pieces, axis=1)
        return 0

    lax.fori_loop(0, blocks, one_block, 0)


def attention(queries, extended, sink_logit, offset, seq_total, turn):
    smem = pl.BlockSpec(memory_space=pltpu.SMEM)
    vmem = pl.BlockSpec(memory_space=pltpu.VMEM)
    bounds = jnp.stack([offset, jnp.int32(seq_total), turn]).astype(jnp.int32)
    return pl.pallas_call(
        attention_kernel,
        out_shape=jax.ShapeDtypeStruct(queries.shape, bf16),
        in_specs=[smem, smem, vmem, vmem],
        out_specs=vmem,
        compiler_params=pltpu.CompilerParams(vmem_limit_bytes=VMEM_LIMIT // 2),
        cost_estimate=pl.CostEstimate(flops=6_000_000_000, bytes_accessed=1_500_000, transcendentals=1_600_000),
        name="attention",
    )(bounds, sink_logit, queries, extended)


def move(value, axis, shift):
    return lax.ppermute(value, axis, shifted(lax.axis_size(axis), shift))


def after(value, *others):
    return lax.optimization_barrier((value,) + others)[0]


def local(
    queries,
    key_rows,
    values,
    sink_logit,
    out_weight,
    out_gain,
    routed_tokens,
    expert_ids,
    route_weight,
    routed_gain,
    expert_gate,
    expert_up,
    expert_down,
):
    row_count = queries.shape[0]
    z, y, c, x = (lax.axis_index(axis) for axis in ("z", "y", "c", "x"))
    expert = (z * 4 + y) * 2 + c
    place = jnp.stack([z, expert, expert + 1 - 2 * c]).astype(jnp.int32)

    split = expert_up.shape[1] // 2
    part_a = jnp.concatenate((expert_gate[0], expert_up[0, :split]), axis=0)
    part_b = jnp.concatenate((expert_up[0, split:], expert_down[0]), axis=0)
    low_a = move(part_a, "x", 1)
    high_b = move(part_b, "x", -1)
    low_b = move(part_b, "x", 1)
    high_a = move(part_a, "x", -1)
    far_a = move(low_a, "x", 1)
    far_b = move(high_b, "x", -1)
    mine = (part_a, part_b, low_a, low_b, high_a, high_b, far_a, far_b)
    prepared = prepare(place, routed_tokens, expert_ids, route_weight, routed_gain)
    own, order = prepared[0], prepared[4]
    size = own.shape[0]
    out = {s: move(prepared[s], "z", s) for s in (1, 3, 2)}
    joined = jnp.concatenate((out[1], out[3]), axis=0)
    groups = {"0": own, "13": joined, "2": out[2]}
    blocks = {}
    for name, chunk in groups.items():
        near_low = move(chunk, "y", 1)
        near_high = move(chunk, "y", -1)
        beyond = move(near_low, "y", 1) if name == "13" else move(near_high, "y", -1)
        blocks[name] = (chunk, near_low, near_high, beyond)

    extended = padded(jnp.concatenate((key_rows, values), axis=1), WINDOW)
    attended = attention(queries, extended, sink_logit, expert * row_count, row_count * 32, 2 * x)
    quarter = row_count // 4
    theirs = tuple(move(v, "c", 1) for v in mine)

    staged_a = stage(place, blocks["13"] * 2, mine[:6] + theirs[:6])
    staged_b = stage(place, blocks["0"] + blocks["2"], mine[:6] + theirs[:6])

    far = mine[6:] + theirs[6:]
    downs = mine[1:6:2] + theirs[1:6:2]
    sets = ((2, 3), (1, 0))
    made = []
    for which, halves in enumerate(((1, 1), (0, 0))):
        parts = (staged_b, staged_a) if which == 0 else (staged_a, staged_b)
        made.append(results(parts, halves, far, downs, size))
    crossed = {0: attended[:quarter]}
    for shift in (1, 2, 3):
        crossed[shift] = move(attended[shift * quarter : (shift + 1) * quarter], "x", shift)
    late = after(out_weight, made[0][0])
    low = move(late, "x", 1)
    high = move(late, "x", -1)
    half = attended.shape[1] // 2
    across = jnp.concatenate((move(low[:half], "x", 1), move(high[half:], "x", -1)), axis=0)
    mixed = jnp.zeros((quarter, out_weight.shape[1]), f32)
    for shift, piece in ((0, out_weight), (1, low), (3, high), (2, across)):
        mixed = mixed + jnp.dot(crossed[shift], piece, preferred_element_type=f32)
    mixer_out = (
        mixed * lax.rsqrt(jnp.mean(mixed * mixed, axis=-1, keepdims=True) + epsilon) * out_gain
    ).astype(bf16)
    back = {}
    for which, pair in enumerate(sets):
        for index, s in enumerate(pair):
            way = 1 if index == 0 else -1
            p_own, p_low, p_high, p_far = made[which][4 * index : 4 * index + 4]
            straight, through = (p_low, p_high) if way == 1 else (p_high, p_low)
            began = move(p_far, "y", way)
            direct = move(straight, "y", -way)
            merged = (began.astype(f32) + through.astype(f32)).astype(bf16)
            ended = move(merged, "y", way)
            if s == 0:
                p_own = after(p_own, mixer_out)
            total = (p_own.astype(f32) + direct.astype(f32) + ended.astype(f32)).astype(bf16)
            back[s] = move(total, "z", -s) if s else total
    turned = turn(order)
    experts_out = finish(turned, [back[s] for s in range(4)])

    return (mixer_out, experts_out)


def solution(mesh):
    split = Mesh(mesh.devices.reshape(4, 4, 2, 4), ("z", "y", "c", "x"))
    ep = ("z", "y", "c")
    placed = (
        P(ep, "x"),
        P(ep, "x"),
        P(ep, "x"),
        P("x"),
        P("x", None),
        P(),
        P(ep + ("x",), None),
        P(ep + ("x",), None),
        P(ep + ("x",), None),
        P(),
        P(ep, None, "x"),
        P(ep, None, "x"),
        P(ep, None, "x"),
    )

    return jax.shard_map(
        local,
        mesh=split,
        in_specs=placed,
        out_specs=(P(ep + ("x",), None), P(ep + ("x",), None)),
        check_vma=False,
    )
```

```python
import jax
import jax.numpy as jnp
from jax import lax
from jax.experimental import pallas as pl
from jax.experimental.pallas import tpu as pltpu
from jax.sharding import Mesh, PartitionSpec as P


HEAD_DIM = 64
WINDOW = 128
CAP = 64
GROUPS = 4
META = 128
SET_BLOCKS = 8

epsilon = 1e-06
f32 = jnp.float32
bf16 = jnp.bfloat16
NT = (((1,), (1,)), ((), ()))
TN = (((0,), (0,)), ((), ()))
VMEM_LIMIT = 60 * 1024 * 1024


def shifted(size, shift):
    return [(i, (i + shift) % size) for i in range(size)]


def iota(shape, dim, kind=jnp.int32):
    return lax.broadcasted_iota(jnp.int32, shape, dim).astype(kind)


def prep_kernel(place, tok, ids_t, weight_t, gain, first, second, third, fourth, order):
    count, width = tok.shape
    each = count // GROUPS
    inputs = tok[...].astype(f32)
    scale = lax.rsqrt(jnp.mean(inputs * inputs, axis=-1, keepdims=True) + epsilon)
    ids = ids_t[...]
    group = lax.shift_right_logical(ids[0:1, :], 3)
    relative = lax.bitwise_and(group - place[0] + GROUPS, GROUPS - 1)
    member = (iota((16, count), 0) == relative).astype(f32)
    before = (iota((count, count), 0) < iota((count, count), 1)).astype(f32).astype(bf16)
    earlier = jnp.dot(member.astype(bf16), before, preferred_element_type=f32)
    rank = jnp.sum(earlier * member, axis=0, keepdims=True)
    slot = (relative * each).astype(f32) + rank
    order[...] = (iota((count, count), 0, f32) == slot).astype(f32).astype(bf16)
    outs = (first, second, third, fourth)
    line = iota((META, count), 0)
    meta = jnp.where(line == 0, ids[0:1, :].astype(f32), 0.0)
    meta = jnp.where(line == 1, ids[1:2, :].astype(f32), meta)
    for k in range(2):
        rest = weight_t[k : k + 1, :]
        for part in range(3):
            piece = rest.astype(bf16).astype(f32)
            meta = jnp.where(line == 2 + 3 * k + part, piece, meta)
            rest = rest - piece
    tags = lax.dot_general(order[...], meta.astype(bf16), NT, preferred_element_type=f32).astype(bf16)
    for index, out in enumerate(outs):
        out[:, width:] = tags[index * each : (index + 1) * each]
    wide = width // 4

    def columns(i, _):
        cols = pl.ds(pl.multiple_of(i * wide, wide), wide)
        normed = (tok[:, cols].astype(f32) * scale * gain[:, cols]).astype(bf16)
        rows = jnp.dot(order[...], normed, preferred_element_type=f32).astype(bf16)
        for index, out in enumerate(outs):
            out[:, cols] = rows[index * each : (index + 1) * each]
        return 0

    lax.fori_loop(0, 4, columns, 0)


def prepare(place, tokens, ids, weights, gain):
    count, width = tokens.shape
    chunk = jax.ShapeDtypeStruct((count // GROUPS, width + META), bf16)
    vmem = pl.BlockSpec(memory_space=pltpu.VMEM)
    return pl.pallas_call(
        prep_kernel,
        out_shape=(chunk, chunk, chunk, chunk, jax.ShapeDtypeStruct((count, count), bf16)),
        in_specs=[pl.BlockSpec(memory_space=pltpu.SMEM)] + [vmem] * 4,
        out_specs=(vmem,) * 5,
        compiler_params=pltpu.CompilerParams(vmem_limit_bytes=VMEM_LIMIT),
        cost_estimate=pl.CostEstimate(flops=6_000_000_000, bytes_accessed=6_000_000, transcendentals=512),
        name="prep",
    )(place, tokens, ids.T, weights.T, gain.reshape(1, width))


def choices(tags, experts):
    blocks = len(tags)
    size = tags[0].shape[0]
    lines = [jnp.transpose(t.astype(f32)) for t in tags]
    hits = [[tuple((t[k : k + 1] == e).astype(f32) for k in range(2)) for t in lines] for e in experts]
    row = iota((2 * blocks, size), 0)
    counts = jnp.zeros((2 * blocks, size), f32)
    for e in range(2):
        for b in range(blocks):
            counts = jnp.where(row == e * blocks + b, hits[e][b][0] + hits[e][b][1], counts)
    before = (iota((size, size), 0) < iota((size, size), 1)).astype(f32).astype(bf16)
    earlier = jnp.dot(counts.astype(bf16), before, preferred_element_type=f32)
    place = iota((2 * CAP, size), 0, f32)
    found = []
    for pair in range(blocks // 2):
        picks = []
        weights = []
        for e in range(2):
            halves = []
            weight = jnp.zeros((2 * CAP, size), f32)
            for j in range(2):
                b = 2 * pair + j
                hit = hits[e][b]
                slot = earlier[e * blocks + b : e * blocks + b + 1] + float(CAP * j)
                one = jnp.where(place == slot, hit[0], 0.0)
                two = jnp.where(place == slot + hit[0], hit[1], 0.0)
                halves.append(one + two)
                t = lines[b]
                weight = weight + one * (t[2:3] + t[3:4] + t[4:5]) + two * (t[5:6] + t[6:7] + t[7:8])
            picks.append(jnp.concatenate(halves, axis=1))
            weights.append(jnp.sum(weight, axis=1, keepdims=True))
        found.append((jnp.concatenate(picks, axis=0).astype(bf16), jnp.concatenate(weights, axis=0)))
    return found


def stage_kernel(place, *refs):
    sources, weights = refs[:8], refs[8:20]
    rows_out, hidden_out, pick_out, scale_out = refs[20:24]
    tok, held, rows, units, pick_v, scale_v, tok_sem, held_sem, out_sem = refs[24:]
    width = rows.shape[-1]
    part, wide = weights[0].shape
    rest = 2 * width - part
    size = tok.shape[1]
    arrivals = []
    for b in range(SET_BLOCKS):
        arrivals.append(pltpu.make_async_copy(sources[b], tok.at[b], tok_sem.at[b]))
    fetches = []
    for i in range(6):
        fetches.append(
            (
                pltpu.make_async_copy(weights[2 * i], held.at[i, pl.ds(0, part)], held_sem.at[0, i]),
                pltpu.make_async_copy(
                    weights[2 * i + 1].at[pl.ds(0, rest)], held.at[i, pl.ds(part, rest)], held_sem.at[1, i]
                ),
            )
        )
    for copy in arrivals:
        copy.start()
    for copy in fetches[0]:
        copy.start()
    experts = (place[1].astype(f32), place[2].astype(f32))
    for copy in arrivals:
        copy.wait()
    for pair_of in fetches[1:]:
        for copy in pair_of:
            copy.start()
    for pair, (pick, scale) in enumerate(choices([tok[b, :, width:] for b in range(SET_BLOCKS)], experts)):
        pick_v[pair] = pick
        scale_v[pair] = jnp.broadcast_to(scale, scale_v.shape[1:])
        both = tok[2 * pair : 2 * pair + 2, :, :width].reshape(2 * size, width)
        chosen = jnp.dot(pick, both, preferred_element_type=f32).astype(bf16)
        for e in range(2):
            rows[e, 2 * CAP * pair : 2 * CAP * (pair + 1)] = chosen[2 * CAP * e : 2 * CAP * (e + 1)]
    sent = [
        pltpu.make_async_copy(rows, rows_out, out_sem.at[0]),
        pltpu.make_async_copy(pick_v, pick_out, out_sem.at[1]),
        pltpu.make_async_copy(scale_v, scale_out, out_sem.at[2]),
    ]
    for copy in sent:
        copy.start()

    def one_shard(i, _):
        e = i // 3
        shard = i - 3 * e
        pltpu.make_async_copy(weights[0], held.at[i, pl.ds(0, part)], held_sem.at[0, i]).wait()
        pltpu.make_async_copy(weights[1].at[pl.ds(0, rest)], held.at[i, pl.ds(part, rest)], held_sem.at[1, i]).wait()
        gate = jnp.dot(rows[e], held[i, :width], preferred_element_type=f32)
        up = jnp.dot(rows[e], held[i, width:], preferred_element_type=f32)
        columns = pl.ds(pl.multiple_of(shard * wide, wide), wide)
        units[e, :, columns] = (gate / (1.0 + jnp.exp(-gate)) * up).astype(bf16)
        return 0

    lax.fori_loop(0, 6, one_shard, 0)
    sent.append(pltpu.make_async_copy(units, hidden_out, out_sem.at[3]))
    sent[-1].start()
    for copy in sent:
        copy.wait()


def stage(place, blocks, weights):
    size, full = blocks[0].shape
    width = full - META
    wide = weights[0].shape[1]
    rows = SET_BLOCKS * CAP
    shapes = (
        ((2, rows, width), bf16),
        ((2, rows, 3 * wide), bf16),
        ((SET_BLOCKS // 2, 4 * CAP, 2 * size), bf16),
        ((SET_BLOCKS // 2, 4 * CAP, 128), f32),
    )
    held = pl.BlockSpec(memory_space=pltpu.HBM)
    return pl.pallas_call(
        stage_kernel,
        out_shape=tuple(jax.ShapeDtypeStruct(*s) for s in shapes),
        in_specs=[pl.BlockSpec(memory_space=pltpu.SMEM)] + [held] * 20,
        out_specs=(held,) * 4,
        scratch_shapes=[
            pltpu.VMEM((SET_BLOCKS, size, full), bf16),
            pltpu.VMEM((6, 2 * width, wide), bf16),
        ]
        + [pltpu.VMEM(*s) for s in shapes]
        + [
            pltpu.SemaphoreType.DMA((SET_BLOCKS,)),
            pltpu.SemaphoreType.DMA((2, 6)),
            pltpu.SemaphoreType.DMA((4,)),
        ],
        compiler_params=pltpu.CompilerParams(vmem_limit_bytes=VMEM_LIMIT),
        cost_estimate=pl.CostEstimate(flops=10_000_000_000, bytes_accessed=24_000_000, transcendentals=0),
    )(place, *blocks, *weights)


def result_kernel(halves, *refs):
    staged, far, downs = (refs[:4], refs[4:8]), refs[8:12], refs[12:18]
    outs = refs[18:26]
    rows, units, pick_v, scale_v, held, down_v, made, spread_v, sem, out_sem = refs[26:]
    width = rows.shape[-1]
    part, wide = far[0].shape
    rest = 2 * width - part
    each = rows.shape[1] // 2
    first, second = [], []
    for e in range(2):
        for j in range(2):
            source = staged[j][0].at[e, pl.ds(halves[j] * each, each)]
            first.append(pltpu.make_async_copy(source, rows.at[e, pl.ds(j * each, each)], sem.at[4 * e + j]))
        first.append(pltpu.make_async_copy(far[2 * e], held.at[e, pl.ds(0, part)], sem.at[4 * e + 2]))
        first.append(pltpu.make_async_copy(far[2 * e + 1].at[pl.ds(0, rest)], held.at[e, pl.ds(part, rest)], sem.at[4 * e + 3]))
    for e in range(2):
        for j in range(2):
            source = staged[j][1].at[e, pl.ds(halves[j] * each, each)]
            target = units.at[e, pl.ds(j * each, each), pl.ds(0, 3 * wide)]
            second.append(pltpu.make_async_copy(source, target, sem.at[8 + 6 * e + j]))
        for shard in range(4):
            source = (far[2 * e + 1] if shard == 3 else downs[3 * e + shard]).at[pl.ds(rest, width)]
            target = down_v.at[e, :, pl.ds(shard * wide, wide)]
            second.append(pltpu.make_async_copy(source, target, sem.at[10 + 6 * e + shard]))
    third = []
    for j in range(2):
        pairs, place = pl.ds(2 * halves[j], 2), pl.ds(2 * j, 2)
        third.append(pltpu.make_async_copy(staged[j][2].at[pairs], pick_v.at[place], sem.at[20 + j]))
        third.append(pltpu.make_async_copy(staged[j][3].at[pairs], scale_v.at[place], sem.at[22 + j]))
    stages = [first[:4], first[4:], second[:6], second[6:] + third]

    def begin(group):
        for copy in stages[group]:
            copy.start()

    def arrive(group):
        for copy in stages[group]:
            copy.wait()

    def far_units(e):
        gate = jnp.dot(rows[e], held[e, :width], preferred_element_type=f32)
        up = jnp.dot(rows[e], held[e, width:], preferred_element_type=f32)
        units[e, :, 3 * wide :] = (gate / (1.0 + jnp.exp(-gate)) * up).astype(bf16)

    quarter = width // 4

    def project(e, cols):
        return lax.dot_general(units[e], down_v[e, cols, :], NT, preferred_element_type=f32).astype(bf16)

    begin(0)
    begin(1)
    arrive(0)
    begin(2)

    def both(e, _):
        @pl.when(e == 1)
        def _():
            arrive(1)
            begin(3)

        far_units(e)
        return 0

    lax.fori_loop(0, 2, both, 0)
    arrive(2)

    def first_expert(i, _):
        cols = pl.ds(pl.multiple_of(i * quarter, quarter), quarter)
        made[:, cols] = project(0, cols)
        return 0

    lax.fori_loop(0, 4, first_expert, 0)
    arrive(3)
    size = outs[0].shape[0]

    def leave(i, b):
        cols = pl.ds(pl.multiple_of(i * quarter, quarter), quarter)
        return pltpu.make_async_copy(spread_v.at[b, :, cols], outs[b].at[:, cols], out_sem.at[i, b])

    def columns(i, _):
        cols = pl.ds(pl.multiple_of(i * quarter, quarter), quarter)
        other = project(1, cols)
        for pair in range(SET_BLOCKS // 2):
            lines = slice(2 * CAP * pair, 2 * CAP * (pair + 1))
            result = jnp.concatenate([made[lines, cols], other[lines]], axis=0).astype(f32)
            scaled = (result * scale_v[pair, :, 0:1]).astype(bf16)
            spread = lax.dot_general(pick_v[pair], scaled, TN, preferred_element_type=f32).astype(bf16)
            spread_v[2 * pair, :, cols] = spread[:size]
            spread_v[2 * pair + 1, :, cols] = spread[size:]
        for b in range(SET_BLOCKS):
            leave(i, b).start()
        return 0

    lax.fori_loop(0, 4, columns, 0)

    def settle(i, _):
        for b in range(SET_BLOCKS):
            leave(i, b).wait()
        return 0

    lax.fori_loop(0, 4, settle, 0)


def results(staged, halves, far, downs, size):
    rows, _, picks, scales = staged[0]
    width = rows.shape[-1]
    wide = far[0].shape[1]
    held = pl.BlockSpec(memory_space=pltpu.HBM)
    vmem = pl.BlockSpec(memory_space=pltpu.VMEM)
    return pl.pallas_call(
        lambda *refs: result_kernel(halves, *refs),
        out_shape=(jax.ShapeDtypeStruct((size, width), bf16),) * SET_BLOCKS,
        in_specs=[held] * 18,
        out_specs=(held,) * SET_BLOCKS,
        scratch_shapes=[
            pltpu.VMEM(rows.shape, bf16),
            pltpu.VMEM((2, rows.shape[1], 4 * wide), bf16),
            pltpu.VMEM(picks.shape, bf16),
            pltpu.VMEM(scales.shape, f32),
            pltpu.VMEM((2, 2 * width, wide), bf16),
            pltpu.VMEM((2, width, 4 * wide), bf16),
            pltpu.VMEM(rows.shape[1:], bf16),
            pltpu.VMEM((SET_BLOCKS, size, width), bf16),
            pltpu.SemaphoreType.DMA((24,)),
            pltpu.SemaphoreType.DMA((4, SET_BLOCKS)),
        ],
        compiler_params=pltpu.CompilerParams(vmem_limit_bytes=VMEM_LIMIT),
        cost_estimate=pl.CostEstimate(flops=8_000_000_000, bytes_accessed=24_000_000, transcendentals=0),
    )(*staged[0], *staged[1], *far, *downs)


def turn_kernel(order, out):
    out[...] = jnp.transpose(order[...].astype(f32)).astype(bf16)


def turn(order):
    vmem = pl.BlockSpec(memory_space=pltpu.VMEM)
    return pl.pallas_call(
        turn_kernel,
        out_shape=jax.ShapeDtypeStruct(order.shape, bf16),
        in_specs=[vmem],
        out_specs=vmem,
        compiler_params=pltpu.CompilerParams(vmem_limit_bytes=VMEM_LIMIT // 2),
        cost_estimate=pl.CostEstimate(flops=1_000_000_000, bytes_accessed=1_000_000, transcendentals=0),
        name="turn",
    )(order)


def finish_kernel(order, first, second, third, fourth, out):
    _, width = first.shape
    wide = width // 4

    def columns(i, _):
        cols = pl.ds(pl.multiple_of(i * wide, wide), wide)
        rows = jnp.concatenate([piece[:, cols] for piece in (first, second, third, fourth)], axis=0)
        out[:, cols] = jnp.dot(order[...], rows, preferred_element_type=f32).astype(bf16)
        return 0

    lax.fori_loop(0, 4, columns, 0)


def finish(order, pieces):
    count = order.shape[0]
    width = pieces[0].shape[1]
    vmem = pl.BlockSpec(memory_space=pltpu.VMEM)
    return pl.pallas_call(
        finish_kernel,
        out_shape=jax.ShapeDtypeStruct((count, width), bf16),
        in_specs=[vmem] * 5,
        out_specs=vmem,
        compiler_params=pltpu.CompilerParams(vmem_limit_bytes=VMEM_LIMIT),
        cost_estimate=pl.CostEstimate(flops=2_000_000_000, bytes_accessed=5_000_000, transcendentals=0),
        name="finish",
    )(order, *pieces)


def padded(block, width):
    axes = ("z", "y", "c")
    count = 1
    for axis in axes:
        count *= lax.axis_size(axis)
    forward = [(i, i + 1) for i in range(count - 1)]
    backward = [(target, source) for source, target in forward]
    low = lax.ppermute(block[-width:], axes, forward)
    high = lax.ppermute(block[:width], axes, backward)
    return jnp.concatenate([low, block, high], axis=0)


def attention_kernel(bounds, sinks, queries, extended, out):
    heads = queries.shape[1] // HEAD_DIM
    total = bounds[1]
    span = 3 * WINDOW
    lines = heads * WINDOW
    row = iota((lines, span), 0)
    col = iota((lines, span), 1)
    away = col - lax.bitwise_and(row, WINDOW - 1)
    near = (away >= 0) & (away <= 2 * WINDOW)
    head = lax.shift_right_logical(iota((lines, 1), 0), 7)
    sink = jnp.zeros((lines, 1), f32)
    for h in range(heads):
        sink = jnp.where(head == h, sinks[h], sink)

    blocks = queries.shape[0] // WINDOW

    def one_block(index, _):
        block = lax.bitwise_and(index + bounds[2], blocks - 1)
        start = pl.multiple_of(block * WINDOW, WINDOW)
        asked = queries[pl.ds(start, WINDOW), :]
        stacked = jnp.concatenate([asked[:, h * HEAD_DIM : (h + 1) * HEAD_DIM] for h in range(heads)], axis=0)
        band = extended[pl.ds(start, span), :]
        keys, held = band[:, :HEAD_DIM], band[:, HEAD_DIM:]
        scores = lax.dot_general(stacked, keys, NT, preferred_element_type=f32) * HEAD_DIM ** (-0.5)
        place = bounds[0] + start - WINDOW + col
        masked = jnp.where(near & (place >= 0) & (place < total), scores, -1e30)
        largest = jnp.maximum(jnp.max(masked, axis=-1, keepdims=True), sink)
        raised = jnp.exp(masked - largest)
        denominator = jnp.sum(raised, axis=-1, keepdims=True) + jnp.exp(sink - largest)
        weights = (raised * (1.0 / denominator)).astype(bf16)
        made = jnp.dot(weights, held, preferred_element_type=f32).astype(bf16)
        pieces = [made[h * WINDOW : (h + 1) * WINDOW] for h in range(heads)]
        out[pl.ds(pl.multiple_of(index * WINDOW, WINDOW), WINDOW), :] = jnp.concatenate(pieces, axis=1)
        return 0

    lax.fori_loop(0, blocks, one_block, 0)


def attention(queries, extended, sink_logit, offset, seq_total, turn):
    smem = pl.BlockSpec(memory_space=pltpu.SMEM)
    vmem = pl.BlockSpec(memory_space=pltpu.VMEM)
    bounds = jnp.stack([offset, jnp.int32(seq_total), turn]).astype(jnp.int32)
    return pl.pallas_call(
        attention_kernel,
        out_shape=jax.ShapeDtypeStruct(queries.shape, bf16),
        in_specs=[smem, smem, vmem, vmem],
        out_specs=vmem,
        compiler_params=pltpu.CompilerParams(vmem_limit_bytes=VMEM_LIMIT // 2),
        cost_estimate=pl.CostEstimate(flops=6_000_000_000, bytes_accessed=1_500_000, transcendentals=1_600_000),
        name="attention",
    )(bounds, sink_logit, queries, extended)


def move(value, axis, shift):
    return lax.ppermute(value, axis, shifted(lax.axis_size(axis), shift))


def after(value, *others):
    return lax.optimization_barrier((value,) + others)[0]


def local(
    queries,
    key_rows,
    values,
    sink_logit,
    out_weight,
    out_gain,
    routed_tokens,
    expert_ids,
    route_weight,
    routed_gain,
    expert_gate,
    expert_up,
    expert_down,
):
    row_count = queries.shape[0]
    z, y, c, x = (lax.axis_index(axis) for axis in ("z", "y", "c", "x"))
    expert = (z * 4 + y) * 2 + c
    place = jnp.stack([z, expert, expert + 1 - 2 * c]).astype(jnp.int32)

    split = expert_up.shape[1] // 2
    part_a = jnp.concatenate((expert_gate[0], expert_up[0, :split]), axis=0)
    part_b = jnp.concatenate((expert_up[0, split:], expert_down[0]), axis=0)
    low_a = move(part_a, "x", 1)
    high_b = move(part_b, "x", -1)
    low_b = move(part_b, "x", 1)
    high_a = move(part_a, "x", -1)
    far_a = move(low_a, "x", 1)
    far_b = move(high_b, "x", -1)
    mine = (part_a, part_b, low_a, low_b, high_a, high_b, far_a, far_b)
    prepared = prepare(place, routed_tokens, expert_ids, route_weight, routed_gain)
    own, order = prepared[0], prepared[4]
    size = own.shape[0]
    out = {s: move(prepared[s], "z", s) for s in (1, 3, 2)}
    groups = {0: own, 1: out[1], 3: out[3], 2: out[2]}
    blocks = {}
    for name, chunk in groups.items():
        near_low = move(chunk, "y", 1)
        near_high = move(chunk, "y", -1)
        beyond = move(near_low, "y", 1) if name in (1, 3) else move(near_high, "y", -1)
        blocks[name] = (chunk, near_low, near_high, beyond)

    extended = padded(jnp.concatenate((key_rows, values), axis=1), WINDOW)
    attended = attention(queries, extended, sink_logit, expert * row_count, row_count * 32, 2 * x)
    quarter = row_count // 4
    theirs = tuple(move(v, "c", 1) for v in mine)

    staged_a = stage(place, blocks[1] + blocks[3], mine[:6] + theirs[:6])
    staged_b = stage(place, blocks[0] + blocks[2], mine[:6] + theirs[:6])

    far = mine[6:] + theirs[6:]
    downs = mine[1:6:2] + theirs[1:6:2]
    sets = ((2, 3), (1, 0))
    made = []
    for which, halves in enumerate(((1, 1), (0, 0))):
        parts = (staged_b, staged_a) if which == 0 else (staged_a, staged_b)
        made.append(results(parts, halves, far, downs, size))
    crossed = {0: attended[:quarter]}
    for shift in (1, 2, 3):
        crossed[shift] = move(attended[shift * quarter : (shift + 1) * quarter], "x", shift)
    late = after(out_weight, made[0][0])
    low = move(late, "x", 1)
    high = move(late, "x", -1)
    half = attended.shape[1] // 2
    across = jnp.concatenate((move(low[:half], "x", 1), move(high[half:], "x", -1)), axis=0)
    mixed = jnp.zeros((quarter, out_weight.shape[1]), f32)
    for shift, piece in ((0, out_weight), (1, low), (3, high), (2, across)):
        mixed = mixed + jnp.dot(crossed[shift], piece, preferred_element_type=f32)
    mixer_out = (
        mixed * lax.rsqrt(jnp.mean(mixed * mixed, axis=-1, keepdims=True) + epsilon) * out_gain
    ).astype(bf16)
    back = {}
    for which, pair in enumerate(sets):
        for index, s in enumerate(pair):
            way = 1 if index == 0 else -1
            p_own, p_low, p_high, p_far = made[which][4 * index : 4 * index + 4]
            straight, through = (p_low, p_high) if way == 1 else (p_high, p_low)
            began = move(p_far, "y", way)
            direct = move(straight, "y", -way)
            merged = (began.astype(f32) + through.astype(f32)).astype(bf16)
            ended = move(merged, "y", way)
            if s == 0:
                p_own = after(p_own, mixer_out)
            total = (p_own.astype(f32) + direct.astype(f32) + ended.astype(f32)).astype(bf16)
            back[s] = move(total, "z", -s) if s else total
    turned = turn(order)
    experts_out = finish(turned, [back[s] for s in range(4)])

    return (mixer_out, experts_out)


def solution(mesh):
    split = Mesh(mesh.devices.reshape(4, 4, 2, 4), ("z", "y", "c", "x"))
    ep = ("z", "y", "c")
    placed = (
        P(ep, "x"),
        P(ep, "x"),
        P(ep, "x"),
        P("x"),
        P("x", None),
        P(),
        P(ep + ("x",), None),
        P(ep + ("x",), None),
        P(ep + ("x",), None),
        P(),
        P(ep, None, "x"),
        P(ep, None, "x"),
        P(ep, None, "x"),
    )

    return jax.shard_map(
        local,
        mesh=split,
        in_specs=placed,
        out_specs=(P(ep + ("x",), None), P(ep + ("x",), None)),
        check_vma=False,
    )
```

```python
import jax
import jax.numpy as jnp
from jax import lax
from jax.experimental import pallas as pl
from jax.experimental.pallas import tpu as pltpu
from jax.sharding import Mesh, PartitionSpec as P


HEAD_DIM = 64
WINDOW = 128
CAP = 64
GROUPS = 4
META = 128
SET_BLOCKS = 8

epsilon = 1e-06
f32 = jnp.float32
bf16 = jnp.bfloat16
NT = (((1,), (1,)), ((), ()))
TN = (((0,), (0,)), ((), ()))
VMEM_LIMIT = 60 * 1024 * 1024


def shifted(size, shift):
    return [(i, (i + shift) % size) for i in range(size)]


def iota(shape, dim, kind=jnp.int32):
    return lax.broadcasted_iota(jnp.int32, shape, dim).astype(kind)


def prep_kernel(place, tok, ids_t, weight_t, gain, first, second, third, fourth, order):
    count, width = tok.shape
    each = count // GROUPS
    inputs = tok[...].astype(f32)
    scale = lax.rsqrt(jnp.mean(inputs * inputs, axis=-1, keepdims=True) + epsilon)
    ids = ids_t[...]
    group = lax.shift_right_logical(ids[0:1, :], 3)
    relative = lax.bitwise_and(group - place[0] + GROUPS, GROUPS - 1)
    member = (iota((16, count), 0) == relative).astype(f32)
    before = (iota((count, count), 0) < iota((count, count), 1)).astype(f32).astype(bf16)
    earlier = jnp.dot(member.astype(bf16), before, preferred_element_type=f32)
    rank = jnp.sum(earlier * member, axis=0, keepdims=True)
    slot = (relative * each).astype(f32) + rank
    order[...] = (iota((count, count), 0, f32) == slot).astype(f32).astype(bf16)
    outs = (first, second, third, fourth)
    line = iota((META, count), 0)
    meta = jnp.where(line == 0, ids[0:1, :].astype(f32), 0.0)
    meta = jnp.where(line == 1, ids[1:2, :].astype(f32), meta)
    for k in range(2):
        rest = weight_t[k : k + 1, :]
        for part in range(3):
            piece = rest.astype(bf16).astype(f32)
            meta = jnp.where(line == 2 + 3 * k + part, piece, meta)
            rest = rest - piece
    tags = lax.dot_general(order[...], meta.astype(bf16), NT, preferred_element_type=f32).astype(bf16)
    for index, out in enumerate(outs):
        out[:, width:] = tags[index * each : (index + 1) * each]
    wide = width // 4

    def columns(i, _):
        cols = pl.ds(pl.multiple_of(i * wide, wide), wide)
        normed = (tok[:, cols].astype(f32) * scale * gain[:, cols]).astype(bf16)
        rows = jnp.dot(order[...], normed, preferred_element_type=f32).astype(bf16)
        for index, out in enumerate(outs):
            out[:, cols] = rows[index * each : (index + 1) * each]
        return 0

    lax.fori_loop(0, 4, columns, 0)


def prepare(place, tokens, ids, weights, gain):
    count, width = tokens.shape
    chunk = jax.ShapeDtypeStruct((count // GROUPS, width + META), bf16)
    vmem = pl.BlockSpec(memory_space=pltpu.VMEM)
    return pl.pallas_call(
        prep_kernel,
        out_shape=(chunk, chunk, chunk, chunk, jax.ShapeDtypeStruct((count, count), bf16)),
        in_specs=[pl.BlockSpec(memory_space=pltpu.SMEM)] + [vmem] * 4,
        out_specs=(vmem,) * 5,
        compiler_params=pltpu.CompilerParams(vmem_limit_bytes=VMEM_LIMIT),
        cost_estimate=pl.CostEstimate(flops=6_000_000_000, bytes_accessed=6_000_000, transcendentals=512),
        name="prep",
    )(place, tokens, ids.T, weights.T, gain.reshape(1, width))


def choices(tags, experts):
    blocks = len(tags)
    size = tags[0].shape[0]
    lines = [jnp.transpose(t.astype(f32)) for t in tags]
    hits = [[tuple((t[k : k + 1] == e).astype(f32) for k in range(2)) for t in lines] for e in experts]
    row = iota((2 * blocks, size), 0)
    counts = jnp.zeros((2 * blocks, size), f32)
    for e in range(2):
        for b in range(blocks):
            counts = jnp.where(row == e * blocks + b, hits[e][b][0] + hits[e][b][1], counts)
    before = (iota((size, size), 0) < iota((size, size), 1)).astype(f32).astype(bf16)
    earlier = jnp.dot(counts.astype(bf16), before, preferred_element_type=f32)
    place = iota((2 * CAP, size), 0, f32)
    found = []
    for pair in range(blocks // 2):
        picks = []
        weights = []
        for e in range(2):
            halves = []
            weight = jnp.zeros((2 * CAP, size), f32)
            for j in range(2):
                b = 2 * pair + j
                hit = hits[e][b]
                slot = earlier[e * blocks + b : e * blocks + b + 1] + float(CAP * j)
                one = jnp.where(place == slot, hit[0], 0.0)
                two = jnp.where(place == slot + hit[0], hit[1], 0.0)
                halves.append(one + two)
                t = lines[b]
                weight = weight + one * (t[2:3] + t[3:4] + t[4:5]) + two * (t[5:6] + t[6:7] + t[7:8])
            picks.append(jnp.concatenate(halves, axis=1))
            weights.append(jnp.sum(weight, axis=1, keepdims=True))
        found.append((jnp.concatenate(picks, axis=0).astype(bf16), jnp.concatenate(weights, axis=0)))
    return found


def stage_kernel(place, *refs):
    sources, weights = refs[:8], refs[8:20]
    rows_out, hidden_out, pick_out, scale_out = refs[20:24]
    tok, held, rows, units, pick_v, scale_v, tok_sem, held_sem, out_sem = refs[24:]
    width = rows.shape[-1]
    part, wide = weights[0].shape
    rest = 2 * width - part
    size = tok.shape[1]
    arrivals = []
    for b in range(SET_BLOCKS):
        arrivals.append(pltpu.make_async_copy(sources[b], tok.at[b], tok_sem.at[b]))
    fetches = []
    for i in range(6):
        fetches.append(
            (
                pltpu.make_async_copy(weights[2 * i], held.at[i, pl.ds(0, part)], held_sem.at[0, i]),
                pltpu.make_async_copy(
                    weights[2 * i + 1].at[pl.ds(0, rest)], held.at[i, pl.ds(part, rest)], held_sem.at[1, i]
                ),
            )
        )
    for copy in arrivals:
        copy.start()
    for copy in fetches[0]:
        copy.start()
    experts = (place[1].astype(f32), place[2].astype(f32))
    for copy in arrivals:
        copy.wait()
    for pair_of in fetches[1:]:
        for copy in pair_of:
            copy.start()
    for pair, (pick, scale) in enumerate(choices([tok[b, :, width:] for b in range(SET_BLOCKS)], experts)):
        pick_v[pair] = pick
        scale_v[pair] = jnp.broadcast_to(scale, scale_v.shape[1:])
        both = tok[2 * pair : 2 * pair + 2, :, :width].reshape(2 * size, width)
        chosen = jnp.dot(pick, both, preferred_element_type=f32).astype(bf16)
        for e in range(2):
            rows[e, 2 * CAP * pair : 2 * CAP * (pair + 1)] = chosen[2 * CAP * e : 2 * CAP * (e + 1)]
    sent = [
        pltpu.make_async_copy(rows, rows_out, out_sem.at[0]),
        pltpu.make_async_copy(pick_v, pick_out, out_sem.at[1]),
        pltpu.make_async_copy(scale_v, scale_out, out_sem.at[2]),
    ]
    for copy in sent:
        copy.start()

    def one_shard(i, _):
        e = i // 3
        shard = i - 3 * e
        pltpu.make_async_copy(weights[0], held.at[i, pl.ds(0, part)], held_sem.at[0, i]).wait()
        pltpu.make_async_copy(weights[1].at[pl.ds(0, rest)], held.at[i, pl.ds(part, rest)], held_sem.at[1, i]).wait()
        gate = jnp.dot(rows[e], held[i, :width], preferred_element_type=f32)
        up = jnp.dot(rows[e], held[i, width:], preferred_element_type=f32)
        columns = pl.ds(pl.multiple_of(shard * wide, wide), wide)
        units[e, :, columns] = (gate / (1.0 + jnp.exp(-gate)) * up).astype(bf16)
        return 0

    lax.fori_loop(0, 6, one_shard, 0)
    sent.append(pltpu.make_async_copy(units, hidden_out, out_sem.at[3]))
    sent[-1].start()
    for copy in sent:
        copy.wait()


def stage(place, blocks, weights):
    size, full = blocks[0].shape
    width = full - META
    wide = weights[0].shape[1]
    rows = SET_BLOCKS * CAP
    shapes = (
        ((2, rows, width), bf16),
        ((2, rows, 3 * wide), bf16),
        ((SET_BLOCKS // 2, 4 * CAP, 2 * size), bf16),
        ((SET_BLOCKS // 2, 4 * CAP, 128), f32),
    )
    held = pl.BlockSpec(memory_space=pltpu.HBM)
    return pl.pallas_call(
        stage_kernel,
        out_shape=tuple(jax.ShapeDtypeStruct(*s) for s in shapes),
        in_specs=[pl.BlockSpec(memory_space=pltpu.SMEM)] + [held] * 20,
        out_specs=(held,) * 4,
        scratch_shapes=[
            pltpu.VMEM((SET_BLOCKS, size, full), bf16),
            pltpu.VMEM((6, 2 * width, wide), bf16),
        ]
        + [pltpu.VMEM(*s) for s in shapes]
        + [
            pltpu.SemaphoreType.DMA((SET_BLOCKS,)),
            pltpu.SemaphoreType.DMA((2, 6)),
            pltpu.SemaphoreType.DMA((4,)),
        ],
        compiler_params=pltpu.CompilerParams(vmem_limit_bytes=VMEM_LIMIT),
        cost_estimate=pl.CostEstimate(flops=10_000_000_000, bytes_accessed=24_000_000, transcendentals=0),
    )(place, *blocks, *weights)


def result_kernel(halves, *refs):
    staged, far, downs = (refs[:4], refs[4:8]), refs[8:12], refs[12:18]
    outs = refs[18:26]
    rows, units, pick_v, scale_v, held, down_v, made, spread_v, sem, out_sem = refs[26:]
    width = rows.shape[-1]
    part, wide = far[0].shape
    rest = 2 * width - part
    each = rows.shape[1] // 2
    first, second = [], []
    for e in range(2):
        for j in range(2):
            source = staged[j][0].at[e, pl.ds(halves[j] * each, each)]
            first.append(pltpu.make_async_copy(source, rows.at[e, pl.ds(j * each, each)], sem.at[4 * e + j]))
        first.append(pltpu.make_async_copy(far[2 * e], held.at[e, pl.ds(0, part)], sem.at[4 * e + 2]))
        first.append(pltpu.make_async_copy(far[2 * e + 1].at[pl.ds(0, rest)], held.at[e, pl.ds(part, rest)], sem.at[4 * e + 3]))
    for e in range(2):
        for j in range(2):
            source = staged[j][1].at[e, pl.ds(halves[j] * each, each)]
            target = units.at[e, pl.ds(j * each, each), pl.ds(0, 3 * wide)]
            second.append(pltpu.make_async_copy(source, target, sem.at[8 + 6 * e + j]))
        for shard in range(4):
            source = (far[2 * e + 1] if shard == 3 else downs[3 * e + shard]).at[pl.ds(rest, width)]
            target = down_v.at[e, :, pl.ds(shard * wide, wide)]
            second.append(pltpu.make_async_copy(source, target, sem.at[10 + 6 * e + shard]))
    third = []
    for j in range(2):
        pairs, place = pl.ds(2 * halves[j], 2), pl.ds(2 * j, 2)
        third.append(pltpu.make_async_copy(staged[j][2].at[pairs], pick_v.at[place], sem.at[20 + j]))
        third.append(pltpu.make_async_copy(staged[j][3].at[pairs], scale_v.at[place], sem.at[22 + j]))
    stages = [first[:4], first[4:], second[:6], second[6:] + third]

    def begin(group):
        for copy in stages[group]:
            copy.start()

    def arrive(group):
        for copy in stages[group]:
            copy.wait()

    def far_units(e):
        gate = jnp.dot(rows[e], held[e, :width], preferred_element_type=f32)
        up = jnp.dot(rows[e], held[e, width:], preferred_element_type=f32)
        units[e, :, 3 * wide :] = (gate / (1.0 + jnp.exp(-gate)) * up).astype(bf16)

    quarter = width // 4

    def project(e, cols):
        return lax.dot_general(units[e], down_v[e, cols, :], NT, preferred_element_type=f32).astype(bf16)

    begin(0)
    begin(1)
    arrive(0)
    begin(2)

    def both(e, _):
        @pl.when(e == 1)
        def _():
            arrive(1)
            begin(3)

        far_units(e)
        return 0

    lax.fori_loop(0, 2, both, 0)
    arrive(2)

    def first_expert(i, _):
        cols = pl.ds(pl.multiple_of(i * quarter, quarter), quarter)
        made[:, cols] = project(0, cols)
        return 0

    lax.fori_loop(0, 4, first_expert, 0)
    arrive(3)
    size = outs[0].shape[0]

    def leave(i, b):
        cols = pl.ds(pl.multiple_of(i * quarter, quarter), quarter)
        return pltpu.make_async_copy(spread_v.at[b, :, cols], outs[b].at[:, cols], out_sem.at[i, b])

    def columns(i, _):
        cols = pl.ds(pl.multiple_of(i * quarter, quarter), quarter)
        other = project(1, cols)
        for pair in range(SET_BLOCKS // 2):
            lines = slice(2 * CAP * pair, 2 * CAP * (pair + 1))
            result = jnp.concatenate([made[lines, cols], other[lines]], axis=0).astype(f32)
            scaled = (result * scale_v[pair, :, 0:1]).astype(bf16)
            spread = lax.dot_general(pick_v[pair], scaled, TN, preferred_element_type=f32).astype(bf16)
            spread_v[2 * pair, :, cols] = spread[:size]
            spread_v[2 * pair + 1, :, cols] = spread[size:]
        for b in range(SET_BLOCKS):
            leave(i, b).start()
        return 0

    lax.fori_loop(0, 4, columns, 0)

    def settle(i, _):
        for b in range(SET_BLOCKS):
            leave(i, b).wait()
        return 0

    lax.fori_loop(0, 4, settle, 0)


def results(staged, halves, far, downs, size):
    rows, _, picks, scales = staged[0]
    width = rows.shape[-1]
    wide = far[0].shape[1]
    held = pl.BlockSpec(memory_space=pltpu.HBM)
    vmem = pl.BlockSpec(memory_space=pltpu.VMEM)
    return pl.pallas_call(
        lambda *refs: result_kernel(halves, *refs),
        out_shape=(jax.ShapeDtypeStruct((size, width), bf16),) * SET_BLOCKS,
        in_specs=[held] * 18,
        out_specs=(held,) * SET_BLOCKS,
        scratch_shapes=[
            pltpu.VMEM(rows.shape, bf16),
            pltpu.VMEM((2, rows.shape[1], 4 * wide), bf16),
            pltpu.VMEM(picks.shape, bf16),
            pltpu.VMEM(scales.shape, f32),
            pltpu.VMEM((2, 2 * width, wide), bf16),
            pltpu.VMEM((2, width, 4 * wide), bf16),
            pltpu.VMEM(rows.shape[1:], bf16),
            pltpu.VMEM((SET_BLOCKS, size, width), bf16),
            pltpu.SemaphoreType.DMA((24,)),
            pltpu.SemaphoreType.DMA((4, SET_BLOCKS)),
        ],
        compiler_params=pltpu.CompilerParams(vmem_limit_bytes=VMEM_LIMIT),
        cost_estimate=pl.CostEstimate(flops=8_000_000_000, bytes_accessed=24_000_000, transcendentals=0),
    )(*staged[0], *staged[1], *far, *downs)


def turn_kernel(order, out):
    out[...] = jnp.transpose(order[...].astype(f32)).astype(bf16)


def turn(order):
    vmem = pl.BlockSpec(memory_space=pltpu.VMEM)
    return pl.pallas_call(
        turn_kernel,
        out_shape=jax.ShapeDtypeStruct(order.shape, bf16),
        in_specs=[vmem],
        out_specs=vmem,
        compiler_params=pltpu.CompilerParams(vmem_limit_bytes=VMEM_LIMIT // 2),
        cost_estimate=pl.CostEstimate(flops=1_000_000_000, bytes_accessed=1_000_000, transcendentals=0),
        name="turn",
    )(order)


def finish_kernel(order, first, second, third, fourth, out):
    rows = jnp.concatenate([piece[...] for piece in (first, second, third, fourth)], axis=0)
    out[...] = jnp.dot(order[...], rows, preferred_element_type=f32).astype(bf16)


def finish(order, pieces):
    count = order.shape[0]
    each, width = pieces[0].shape
    wide = width // 4
    return pl.pallas_call(
        finish_kernel,
        grid=(4,),
        out_shape=jax.ShapeDtypeStruct((count, width), bf16),
        in_specs=[pl.BlockSpec((count, count), lambda i: (0, 0))] + [pl.BlockSpec((each, wide), lambda i: (0, i))] * 4,
        out_specs=pl.BlockSpec((count, wide), lambda i: (0, i)),
        compiler_params=pltpu.CompilerParams(vmem_limit_bytes=VMEM_LIMIT),
        cost_estimate=pl.CostEstimate(flops=2_000_000_000, bytes_accessed=5_000_000, transcendentals=0),
        name="finish",
    )(order, *pieces)


def padded(block, width):
    axes = ("z", "y", "c")
    count = 1
    for axis in axes:
        count *= lax.axis_size(axis)
    forward = [(i, i + 1) for i in range(count - 1)]
    backward = [(target, source) for source, target in forward]
    low = lax.ppermute(block[-width:], axes, forward)
    high = lax.ppermute(block[:width], axes, backward)
    return jnp.concatenate([low, block, high], axis=0)


def attention_kernel(bounds, sinks, queries, extended, out):
    heads = queries.shape[1] // HEAD_DIM
    total = bounds[1]
    span = 3 * WINDOW
    lines = heads * WINDOW
    row = iota((lines, span), 0)
    col = iota((lines, span), 1)
    away = col - lax.bitwise_and(row, WINDOW - 1)
    near = (away >= 0) & (away <= 2 * WINDOW)
    head = lax.shift_right_logical(iota((lines, 1), 0), 7)
    sink = jnp.zeros((lines, 1), f32)
    for h in range(heads):
        sink = jnp.where(head == h, sinks[h], sink)

    blocks = queries.shape[0] // WINDOW

    def one_block(index, _):
        block = lax.bitwise_and(index + bounds[2], blocks - 1)
        start = pl.multiple_of(block * WINDOW, WINDOW)
        asked = queries[pl.ds(start, WINDOW), :]
        stacked = jnp.concatenate([asked[:, h * HEAD_DIM : (h + 1) * HEAD_DIM] for h in range(heads)], axis=0)
        band = extended[pl.ds(start, span), :]
        keys, held = band[:, :HEAD_DIM], band[:, HEAD_DIM:]
        scores = lax.dot_general(stacked, keys, NT, preferred_element_type=f32) * HEAD_DIM ** (-0.5)
        place = bounds[0] + start - WINDOW + col
        masked = jnp.where(near & (place >= 0) & (place < total), scores, -1e30)
        largest = jnp.maximum(jnp.max(masked, axis=-1, keepdims=True), sink)
        raised = jnp.exp(masked - largest)
        denominator = jnp.sum(raised, axis=-1, keepdims=True) + jnp.exp(sink - largest)
        weights = (raised * (1.0 / denominator)).astype(bf16)
        made = jnp.dot(weights, held, preferred_element_type=f32).astype(bf16)
        pieces = [made[h * WINDOW : (h + 1) * WINDOW] for h in range(heads)]
        out[pl.ds(pl.multiple_of(index * WINDOW, WINDOW), WINDOW), :] = jnp.concatenate(pieces, axis=1)
        return 0

    lax.fori_loop(0, blocks, one_block, 0)


def attention(queries, extended, sink_logit, offset, seq_total, turn):
    smem = pl.BlockSpec(memory_space=pltpu.SMEM)
    vmem = pl.BlockSpec(memory_space=pltpu.VMEM)
    bounds = jnp.stack([offset, jnp.int32(seq_total), turn]).astype(jnp.int32)
    return pl.pallas_call(
        attention_kernel,
        out_shape=jax.ShapeDtypeStruct(queries.shape, bf16),
        in_specs=[smem, smem, vmem, vmem],
        out_specs=vmem,
        compiler_params=pltpu.CompilerParams(vmem_limit_bytes=VMEM_LIMIT // 2),
        cost_estimate=pl.CostEstimate(flops=6_000_000_000, bytes_accessed=1_500_000, transcendentals=1_600_000),
        name="attention",
    )(bounds, sink_logit, queries, extended)


def move(value, axis, shift):
    return lax.ppermute(value, axis, shifted(lax.axis_size(axis), shift))


def after(value, *others):
    return lax.optimization_barrier((value,) + others)[0]


def local(
    queries,
    key_rows,
    values,
    sink_logit,
    out_weight,
    out_gain,
    routed_tokens,
    expert_ids,
    route_weight,
    routed_gain,
    expert_gate,
    expert_up,
    expert_down,
):
    row_count = queries.shape[0]
    z, y, c, x = (lax.axis_index(axis) for axis in ("z", "y", "c", "x"))
    expert = (z * 4 + y) * 2 + c
    place = jnp.stack([z, expert, expert + 1 - 2 * c]).astype(jnp.int32)

    split = expert_up.shape[1] // 2
    part_a = jnp.concatenate((expert_gate[0], expert_up[0, :split]), axis=0)
    part_b = jnp.concatenate((expert_up[0, split:], expert_down[0]), axis=0)
    low_a = move(part_a, "x", 1)
    high_b = move(part_b, "x", -1)
    low_b = move(part_b, "x", 1)
    high_a = move(part_a, "x", -1)
    far_a = move(low_a, "x", 1)
    far_b = move(high_b, "x", -1)
    mine = (part_a, part_b, low_a, low_b, high_a, high_b, far_a, far_b)
    prepared = prepare(place, routed_tokens, expert_ids, route_weight, routed_gain)
    own, order = prepared[0], prepared[4]
    size = own.shape[0]
    out = {s: move(prepared[s], "z", s) for s in (1, 3, 2)}
    groups = {0: own, 1: out[1], 3: out[3], 2: out[2]}
    blocks = {}
    for name, chunk in groups.items():
        near_low = move(chunk, "y", 1)
        near_high = move(chunk, "y", -1)
        beyond = move(near_low, "y", 1) if name in (1, 3) else move(near_high, "y", -1)
        blocks[name] = (chunk, near_low, near_high, beyond)

    extended = padded(jnp.concatenate((key_rows, values), axis=1), WINDOW)
    attended = attention(queries, extended, sink_logit, expert * row_count, row_count * 32, 2 * x)
    quarter = row_count // 4
    theirs = tuple(move(v, "c", 1) for v in mine)

    staged_a = stage(place, blocks[1] + blocks[3], mine[:6] + theirs[:6])
    staged_b = stage(place, blocks[0] + blocks[2], mine[:6] + theirs[:6])

    far = mine[6:] + theirs[6:]
    downs = mine[1:6:2] + theirs[1:6:2]
    sets = ((2, 3), (1, 0))
    made = []
    for which, halves in enumerate(((1, 1), (0, 0))):
        parts = (staged_b, staged_a) if which == 0 else (staged_a, staged_b)
        made.append(results(parts, halves, far, downs, size))
    crossed = {0: attended[:quarter]}
    for shift in (1, 2, 3):
        crossed[shift] = move(attended[shift * quarter : (shift + 1) * quarter], "x", shift)
    late = after(out_weight, made[0][0])
    low = move(late, "x", 1)
    high = move(late, "x", -1)
    half = attended.shape[1] // 2
    across = jnp.concatenate((move(low[:half], "x", 1), move(high[half:], "x", -1)), axis=0)
    mixed = jnp.zeros((quarter, out_weight.shape[1]), f32)
    for shift, piece in ((0, out_weight), (1, low), (3, high), (2, across)):
        mixed = mixed + jnp.dot(crossed[shift], piece, preferred_element_type=f32)
    mixer_out = (
        mixed * lax.rsqrt(jnp.mean(mixed * mixed, axis=-1, keepdims=True) + epsilon) * out_gain
    ).astype(bf16)
    back = {}
    for which, pair in enumerate(sets):
        for index, s in enumerate(pair):
            way = 1 if index == 0 else -1
            p_own, p_low, p_high, p_far = made[which][4 * index : 4 * index + 4]
            straight, through = (p_low, p_high) if way == 1 else (p_high, p_low)
            began = move(p_far, "y", way)
            direct = move(straight, "y", -way)
            merged = (began.astype(f32) + through.astype(f32)).astype(bf16)
            ended = move(merged, "y", way)
            if s == 0:
                p_own = after(p_own, mixer_out)
            total = (p_own.astype(f32) + direct.astype(f32) + ended.astype(f32)).astype(bf16)
            back[s] = move(total, "z", -s) if s else total
    turned = turn(order)
    experts_out = finish(turned, [back[s] for s in range(4)])

    return (mixer_out, experts_out)


def solution(mesh):
    split = Mesh(mesh.devices.reshape(4, 4, 2, 4), ("z", "y", "c", "x"))
    ep = ("z", "y", "c")
    placed = (
        P(ep, "x"),
        P(ep, "x"),
        P(ep, "x"),
        P("x"),
        P("x", None),
        P(),
        P(ep + ("x",), None),
        P(ep + ("x",), None),
        P(ep + ("x",), None),
        P(),
        P(ep, None, "x"),
        P(ep, None, "x"),
        P(ep, None, "x"),
    )

    return jax.shard_map(
        local,
        mesh=split,
        in_specs=placed,
        out_specs=(P(ep + ("x",), None), P(ep + ("x",), None)),
        check_vma=False,
    )
```
